32 devices in a mesh: sp: 8 (over z, y), tp: 4 (over x, core).
Axes of the slice: x: 2, y: 2, z: 4, core: 2. Of those that a mesh axis runs over, the one named last changes fastest.
Arguments:
- tokens: bfloat16 [2048, 4096], P('sp'), may hold values from -64 to 64
- norm_gain: float32 [4096], replicated, may hold values from 0.1 to 1.9
- w_query: bfloat16 [4096, 2048], P('sp', 'tp'), may hold values from -1.09375 to 1.09375
- w_key: bfloat16 [4096, 512], P('sp', 'tp'), may hold values from -0.09375 to 0.09375
- w_value: bfloat16 [4096, 512], P('sp', 'tp'), may hold values from -0.09375 to 0.09375
- w_glu: bfloat16 [4096, 2048], P('sp', 'tp'), may hold values from -0.09375 to 0.09375
- w_gate: bfloat16 [4096, 2048], P('sp', 'tp'), may hold values from -0.09375 to 0.09375
- sink_logit: float32 [32], P('tp'), may hold values from 2 to 6
- conv_taps: bfloat16 [31, 2048], P(None, 'tp'), may hold values from -12.9315817 to 12.9315817
- conv_gain: float32 [2048], P('tp'), may hold values from 0.1 to 1.9
- out_attn: bfloat16 [2048, 4096], P('sp', 'tp'), may hold values from -0.5 to 0.5
- out_conv: bfloat16 [2048, 4096], P('sp', 'tp'), may hold values from -0.125 to 0.125
Outputs:
- mixed: bfloat16 [2048, 4096], P('sp', 'tp')
The draws below stay inside these ranges and needn't reach their ends.
All inputs are finite; a program needn't handle non-finite values.
Results may differ from the reference program's by a relative error of at most 0.008.
The reference program's roundings to bfloat16 on the way count: a program that leaves them out, or rounds other values in their place, can miss the bound.
Values may be sent and summed in bfloat16 or wider, within the bound.
A program may use at most 64 MiB of HBM per device.

```python
import math
import jax
import jax.numpy as jnp
from jax import lax

D = 4096
HEADS = 32
HEAD = 64
KV = 8
CONV = 2048
KSIZE = 31
WINDOW = 128
TOKENS = 2048


def draw_tokens(key, part):
    subkeys = jax.random.split(key, 3)
    row_scale = jnp.exp(jax.random.uniform(subkeys[0], (TOKENS, 1), jnp.float32, 0.0, math.log(4.0)))
    col_scale = jnp.exp(jax.random.uniform(subkeys[1], (1, D), jnp.float32, 0.0, math.log(4.0)))
    raw_draw = jnp.clip(jax.random.normal(subkeys[2], (TOKENS, D), jnp.float32), -4.0, 4.0)
    return (raw_draw * row_scale * col_scale).astype(jnp.bfloat16)


def draw_w_query(key, part):
    spread = D ** (-0.5)
    raw_draw = jnp.clip(jax.random.normal(key, (D, HEADS * HEAD), jnp.float32), -4.0, 4.0)
    return (raw_draw * spread).astype(jnp.bfloat16)


def draw_conv_taps(key, part):
    subkeys = jax.random.split(key, 2)
    channel = jnp.arange(CONV, dtype=jnp.float32)[None, :] / CONV
    jitter = jnp.exp(jax.random.uniform(subkeys[0], (1, CONV), jnp.float32, math.log(0.7), math.log(1.4)))
    rising = 10.0 ** channel
    raw_draw = jnp.clip(jax.random.normal(subkeys[1], (KSIZE, CONV), jnp.float32), -4.0, 4.0)
    return (raw_draw * rising * jitter * KSIZE ** (-0.5)).astype(jnp.bfloat16)


def steps_of(rng, shape, shards, smallest, largest):
    level = 1.0
    for dim, blocks in shards:
        heights = jax.random.uniform(jax.random.fold_in(jax.random.fold_in(rng, 6), dim), (blocks,), jnp.float32, smallest / len(shards), largest / len(shards))
        level = level * jnp.repeat(jnp.exp(heights), shape[dim] // blocks).reshape((-1,) + (1,) * (len(shape) - 1 - dim))
    return level


def scatter_about(stream_key, shape, width, limit, pieces=(), held_as=jnp.bfloat16):
    gain = steps_of(stream_key, shape, pieces, -0.22, 0.18) if pieces else 1.0
    array = jax.random.normal(stream_key, shape, jnp.float32) * width * gain
    return jnp.minimum(jnp.maximum(array, -limit), limit).astype(held_as)


def setup_inputs(seed: int = 0) -> dict:
    key_of = jax.random.split(jax.random.key(seed), 13)
    tokens = draw_tokens(jax.random.fold_in(key_of[12], 71), 0)
    norm_gain = jnp.clip(1.0 + 0.18 * jax.random.normal(key_of[1], (D,), jnp.float32), 0.1, 1.9)
    w_query = draw_w_query(jax.random.fold_in(key_of[12], 71), 0)
    w_key = scatter_about(key_of[3], (D, KV * HEAD), D ** -0.5, 0.09375, ((0, 8), (1, 4)))
    w_value = scatter_about(key_of[4], (D, KV * HEAD), D ** -0.5, 0.09375, ((0, 8), (1, 4)))
    w_glu = scatter_about(key_of[5], (D, CONV), D ** -0.5, 0.09375, ((0, 8), (1, 4)))
    w_gate = scatter_about(key_of[6], (D, CONV), D ** -0.5, 0.09375, ((0, 8), (1, 4)))
    sink_logit = jnp.clip(2.0 + 4.0 * jax.random.uniform(key_of[7], (HEADS,), jnp.float32) ** steps_of(key_of[7], (HEADS,), ((0, 4),), -0.2, 0.2), 2.0, 6.0)
    conv_taps = draw_conv_taps(jax.random.fold_in(key_of[12], 71), 0)
    conv_gain = jnp.clip(1.0 + 0.18 * jax.random.normal(key_of[9], (CONV,), jnp.float32), 0.1, 1.9)
    out_attn = scatter_about(key_of[10], (HEADS * HEAD, D), (HEADS * HEAD // 16) ** -0.5, 0.5, ((0, 8), (1, 4)))
    out_conv = scatter_about(key_of[11], (CONV, D), CONV ** -0.5, 0.125, ((0, 8), (1, 4)))
    return {"tokens": tokens, "norm_gain": norm_gain, "w_query": w_query, "w_key": w_key, "w_value": w_value, "w_glu": w_glu, "w_gate": w_gate, "sink_logit": sink_logit, "conv_taps": conv_taps, "conv_gain": conv_gain, "out_attn": out_attn, "out_conv": out_conv}


def rotate_heads(values, positions):
    half_width = values.shape[-1] // 2
    frequency = 10000.0 ** (-jnp.arange(half_width, dtype=jnp.float32) * 2.0 / values.shape[-1])
    angles = positions.astype(jnp.float32)[:, None] * frequency[None, :]
    cosine = jnp.cos(angles)[:, None, :]
    sine_part = jnp.sin(angles)[:, None, :]
    first_half = values[..., :half_width]
    second_half = values[..., half_width:]
    return jnp.concatenate([first_half * cosine - second_half * sine_part, second_half * cosine + first_half * sine_part], axis=-1)

def window_attention(operands):
    queries, keys_rot, values_bf, sinks = operands
    total_rows, group_size, head_dimension = queries.shape
    block_count = total_rows // WINDOW
    query_block_rows = queries.reshape(block_count, WINDOW, group_size, head_dimension).astype(jnp.float32)
    key_blocks = keys_rot.reshape(block_count, WINDOW, head_dimension).astype(jnp.float32)
    value_blocks = values_bf.reshape(block_count, WINDOW, head_dimension).astype(jnp.float32)
    empty_block = jnp.zeros((1, WINDOW, head_dimension), jnp.float32)
    key_pair_rows = jnp.concatenate([jnp.concatenate([empty_block, key_blocks[:-1]], axis=0), key_blocks], axis=1)
    value_pair_rows = jnp.concatenate([jnp.concatenate([empty_block, value_blocks[:-1]], axis=0), value_blocks], axis=1)
    score_matrix = jnp.einsum('schn,svn->shcv', query_block_rows, key_pair_rows) * (1.0 / math.sqrt(head_dimension))
    block_ids = jnp.arange(block_count, dtype=jnp.int32)[:, None, None]
    query_pos = block_ids * WINDOW + jnp.arange(WINDOW, dtype=jnp.int32)[None, :, None]
    key_pos = (block_ids - 1) * WINDOW + jnp.arange(2 * WINDOW, dtype=jnp.int32)[None, None, :]
    distance = query_pos - key_pos
    allowed = (distance >= 0) & (distance < WINDOW) & (key_pos >= 0)
    score_matrix = jnp.where(allowed[:, None], score_matrix, -1e+30)
    sink_col = sinks.astype(jnp.float32)[None, :, None, None]
    highest = jnp.maximum(lax.optimization_barrier(jnp.max(score_matrix, axis=-1, keepdims=True)), sink_col)
    weights_exp = jnp.exp(score_matrix - highest)
    denom_total = lax.optimization_barrier(jnp.sum(weights_exp, axis=-1, keepdims=True)) + jnp.exp(sink_col - highest)
    weights_bfloat_half = (weights_exp / denom_total).astype(jnp.bfloat16)
    attended_values = jnp.einsum('jxcp,jpi->jcxi', weights_bfloat_half.astype(jnp.float32), value_pair_rows).astype(jnp.bfloat16)
    return attended_values.reshape(total_rows, group_size, head_dimension)

def reference(tokens, norm_gain, w_query, w_key, w_value, w_glu, w_gate, sink_logit, conv_taps, conv_gain, out_attn, out_conv):
    total_rows = tokens.shape[0]
    tokens_f = tokens.astype(jnp.float32)
    normed = (tokens_f * lax.rsqrt(lax.optimization_barrier(jnp.mean(tokens_f * tokens_f, axis=1, keepdims=True)) + 1e-06) * norm_gain.astype(jnp.float32)).astype(jnp.bfloat16)
    positions = jnp.arange(total_rows, dtype=jnp.int32)
    queries = rotate_heads(jnp.dot(normed, w_query, preferred_element_type=jnp.float32).reshape(total_rows, HEADS, HEAD), positions).astype(jnp.bfloat16)
    keys_rot = rotate_heads(jnp.dot(normed, w_key, preferred_element_type=jnp.float32).reshape(total_rows, KV, HEAD), positions).astype(jnp.bfloat16)
    values_bf = jnp.dot(normed, w_value, preferred_element_type=jnp.float32).astype(jnp.bfloat16).reshape(total_rows, KV, HEAD)
    group_size = HEADS // KV
    query_heads = jnp.transpose(queries.reshape(total_rows, KV, group_size, HEAD), (1, 0, 2, 3))
    key_heads = jnp.transpose(keys_rot, (1, 0, 2))
    value_heads = jnp.transpose(values_bf, (1, 0, 2))
    sink_heads = sink_logit.reshape(KV, group_size)
    attended_values = lax.map(window_attention, (query_heads, key_heads, value_heads, sink_heads))
    attended_values = jnp.transpose(attended_values, (1, 0, 2, 3)).reshape(total_rows, HEADS * HEAD)
    glu_part = jnp.dot(normed, w_glu, preferred_element_type=jnp.float32)
    gate_part = jnp.dot(normed, w_gate, preferred_element_type=jnp.float32)
    gated = (glu_part * jax.nn.sigmoid(gate_part)).astype(jnp.bfloat16)
    extended = jnp.concatenate([jnp.zeros((KSIZE - 1, CONV), jnp.float32), gated.astype(jnp.float32)], axis=0)
    filtered = lax.conv_general_dilated(extended[None], conv_taps.astype(jnp.float32)[:, None, :], (1,), 'VALID', dimension_numbers=('NWC', 'WIO', 'NWC'), feature_group_count=CONV, precision=lax.Precision.HIGHEST)[0]
    mean_value = lax.optimization_barrier(jnp.sum(filtered, axis=1)) / CONV
    variance = lax.optimization_barrier(jnp.sum(filtered * filtered, axis=1)) / CONV - mean_value * mean_value
    scaled = (filtered - mean_value[:, None]) * lax.rsqrt(variance + 1e-05)[:, None] * conv_gain.astype(jnp.float32)
    conv_out = jax.nn.silu(scaled).astype(jnp.bfloat16)
    mixed = jnp.dot(attended_values, out_attn, preferred_element_type=jnp.float32) + jnp.dot(conv_out, out_conv, preferred_element_type=jnp.float32)
    return mixed.astype(jnp.bfloat16)
```

```python
import functools
import math

import jax
import jax.numpy as jnp
from jax import lax
from jax.experimental import pallas as pl
from jax.experimental.pallas import tpu as pltpu
from jax.sharding import PartitionSpec as P

HEADS = 32
HEAD = 64
KV = 8
CONV = 2048
KSIZE = 31
WINDOW = 128


def passed_along(block, axis, distance):
    devices = range(lax.axis_size(axis))
    route = [(i - distance, i) for i in devices if i - distance in devices]
    return lax.ppermute(block, axis, route)


def rotate_heads(values, positions):
    half_width = values.shape[-1] // 2
    frequency = 10000.0 ** (-jnp.arange(half_width, dtype=jnp.float32) * 2.0 / values.shape[-1])
    angles = positions.astype(jnp.float32)[:, None] * frequency[None, :]
    cosine = jnp.cos(angles)[:, None, :]
    sine_part = jnp.sin(angles)[:, None, :]
    first_half = values[..., :half_width]
    second_half = values[..., half_width:]
    return jnp.concatenate(
        [
            first_half * cosine - second_half * sine_part,
            second_half * cosine + first_half * sine_part,
        ],
        axis=-1,
    )


def ring_gather_kernel(n, count, *refs):
    shards, wholes = refs[:count], refs[count : 2 * count]
    bounce = refs[2 * count : 3 * count]
    in_sem, out_sem, send_sem, recv_sem = refs[3 * count :]
    me = lax.axis_index("sp")
    half = n // 2
    odd = lax.rem(me, 2)
    place = (1 - odd) * lax.div(me, 2) + odd * (n - 1 - lax.div(me, 2))

    def device_at(position):
        spot = lax.rem(position + 2 * n, n)
        back = lax.div(spot, half)
        return (1 - back) * 2 * spot + back * (2 * (n - 1 - spot) + 1)

    ahead, behind = device_at(place + 1), device_at(place - 1)
    barrier = pltpu.get_barrier_semaphore()
    for neighbour in (ahead, behind):
        pl.semaphore_signal(
            barrier, inc=1, device_id={"sp": neighbour}, device_id_type=pl.DeviceIdType.MESH
        )
    pl.semaphore_wait(barrier, 2)

    def block(array, owner, way):
        rows = shards[array].shape[0]
        part = rows // 2
        start = pl.multiple_of(owner * rows + way * part, part)
        return wholes[array].at[pl.ds(start, part)]

    def hop(array, step, way):
        owner = device_at(place - step) if way == 0 else device_at(place + step)
        part = shards[array].shape[0] // 2
        target = block(array, owner, way)
        source = shards[array].at[pl.ds(way * part, part)] if step == 0 else target
        return pltpu.make_async_remote_copy(
            src_ref=source,
            dst_ref=target,
            send_sem=send_sem.at[way, step, array],
            recv_sem=recv_sem.at[way, step, array],
            device_id={"sp": ahead if way == 0 else behind},
            device_id_type=pl.DeviceIdType.MESH,
        )

    def arrival(array, step, way):
        owner = device_at(place - step - 1) if way == 0 else device_at(place + step + 1)
        target = block(array, owner, way)
        return pltpu.make_async_remote_copy(
            src_ref=target,
            dst_ref=target,
            send_sem=send_sem.at[way, step, array],
            recv_sem=recv_sem.at[way, step, array],
            device_id={"sp": ahead if way == 0 else behind},
            device_id_type=pl.DeviceIdType.MESH,
        )

    for array in range(count):
        for way in range(2):
            hop(array, 0, way).start()
    loads = [
        pltpu.make_async_copy(shards[a], bounce[a], in_sem.at[a]) for a in range(count)
    ]
    for load in loads:
        load.start()
    stores = []
    for a in range(count):
        loads[a].wait()
        rows = shards[a].shape[0]
        mine = wholes[a].at[pl.ds(pl.multiple_of(me * rows, rows), rows)]
        stores.append(pltpu.make_async_copy(bounce[a], mine, out_sem.at[a]))
        stores[a].start()
    for step in range(1, n - 1):
        for array in range(count):
            for way in range(2):
                arrival(array, step - 1, way).wait_recv()
                hop(array, step, way).start()
    for array in range(count):
        for way in range(2):
            arrival(array, n - 2, way).wait_recv()
    for step in range(n - 1):
        for array in range(count):
            for way in range(2):
                hop(array, step, way).wait_send()
    for store in stores:
        store.wait()


def ring_gather(arrays, collective_id):
    n = lax.axis_size("sp")
    count = len(arrays)
    return pl.pallas_call(
        functools.partial(ring_gather_kernel, n, count),
        out_shape=[
            jax.ShapeDtypeStruct((n * a.shape[0],) + a.shape[1:], a.dtype) for a in arrays
        ],
        in_specs=[pl.BlockSpec(memory_space=pl.ANY)] * count,
        out_specs=[pl.BlockSpec(memory_space=pl.ANY)] * count,
        scratch_shapes=[pltpu.VMEM(a.shape, a.dtype) for a in arrays]
        + [
            pltpu.SemaphoreType.DMA((count,)),
            pltpu.SemaphoreType.DMA((count,)),
            pltpu.SemaphoreType.DMA((2, n - 1, count)),
            pltpu.SemaphoreType.DMA((2, n - 1, count)),
        ],
        compiler_params=pltpu.CompilerParams(
            collective_id=collective_id, has_side_effects=True
        ),
    )(*arrays)


def gathered_per_device(
    tokens,
    norm_gain,
    w_query,
    w_key,
    w_value,
    w_glu,
    w_gate,
    sink_logit,
    conv_taps,
    conv_gain,
    out_attn,
    out_conv,
):
    row_count = tokens.shape[0]
    offset_rows = lax.axis_index("sp") * row_count
    positions = offset_rows + jnp.arange(row_count, dtype=jnp.int32)
    tokens_f = tokens.astype(jnp.float32)
    normed = (
        tokens_f
        * lax.rsqrt(jnp.mean(tokens_f * tokens_f, axis=1, keepdims=True) + 1e-06)
        * norm_gain
    ).astype(jnp.bfloat16)
    local_heads = w_query.shape[1] // HEAD
    local_kv = w_key.shape[1] // HEAD
    group_size = HEADS // KV
    kv_width = local_kv * HEAD
    *pieces, attn_rows, conv_rows = ring_gather(
        (w_query, w_key, w_value, w_glu, w_gate, out_attn, out_conv), 0
    )
    query_acc, key_acc, value_acc, glu_acc, gate_acc = tuple(
        (
            jnp.dot(normed, weight_piece, preferred_element_type=jnp.float32)
            for weight_piece in pieces
        )
    )
    queries = rotate_heads(query_acc.reshape(row_count, local_heads, HEAD), positions).astype(
        jnp.bfloat16
    )
    keys_rot = rotate_heads(key_acc.reshape(row_count, local_kv, HEAD), positions).astype(
        jnp.bfloat16
    )
    keys_rot = keys_rot.reshape(row_count, kv_width)
    values_bf = value_acc.astype(jnp.bfloat16)
    kv_tail = jnp.concatenate(
        [keys_rot[row_count - WINDOW :], values_bf[row_count - WINDOW :]], axis=1
    )
    kv_rim = passed_along(kv_tail, "sp", 1)
    gated = (glu_acc * jax.nn.sigmoid(gate_acc)).astype(jnp.bfloat16)
    conv_tail = gated[row_count - (KSIZE - 1) :]
    conv_rim = passed_along(conv_tail, "sp", 1)
    block_count = row_count // WINDOW
    keys_all = jnp.concatenate([kv_rim[:, :kv_width], keys_rot], axis=0).reshape(
        block_count + 1, WINDOW, local_kv, HEAD
    )
    vals_all = jnp.concatenate([kv_rim[:, kv_width:], values_bf], axis=0).reshape(
        block_count + 1, WINDOW, local_kv, HEAD
    )
    key_blocks = jnp.concatenate([keys_all[:-1], keys_all[1:]], axis=1)
    value_blocks = jnp.concatenate([vals_all[:-1], vals_all[1:]], axis=1)
    query_block_rows = queries.reshape(block_count, WINDOW, local_kv, group_size, HEAD)
    score_matrix = jnp.einsum(
        "bqhgd,bkhd->bhgqk", query_block_rows, key_blocks, preferred_element_type=jnp.float32
    ) * (1.0 / math.sqrt(HEAD))
    block_ids = jnp.arange(block_count, dtype=jnp.int32)[:, None, None]
    query_pos = (
        offset_rows + block_ids * WINDOW + jnp.arange(WINDOW, dtype=jnp.int32)[None, :, None]
    )
    key_pos = (
        offset_rows
        + (block_ids - 1) * WINDOW
        + jnp.arange(2 * WINDOW, dtype=jnp.int32)[None, None, :]
    )
    distance = query_pos - key_pos
    allowed = (distance >= 0) & (distance < WINDOW) & (key_pos >= 0)
    score_matrix = jnp.where(allowed[:, None, None], score_matrix, -1e30)
    sink_local = sink_logit.reshape(local_kv, group_size)[None, :, :, None, None]
    highest = jnp.maximum(jnp.max(score_matrix, axis=-1, keepdims=True), sink_local)
    weights_exp = jnp.exp(score_matrix - highest)
    denom_total = jnp.sum(weights_exp, axis=-1, keepdims=True) + jnp.exp(sink_local - highest)
    weights_bfloat_half = (weights_exp / denom_total).astype(jnp.bfloat16)
    attended_values = jnp.einsum(
        "bhgqk,bkhd->bqhgd", weights_bfloat_half, value_blocks, preferred_element_type=jnp.float32
    ).astype(jnp.bfloat16)
    attended_values = attended_values.reshape(row_count, local_heads * HEAD)
    extended = jnp.concatenate([conv_rim, gated], axis=0).astype(jnp.float32)
    filtered = lax.conv_general_dilated(
        extended[None],
        conv_taps.astype(jnp.float32)[:, None, :],
        (1,),
        "VALID",
        dimension_numbers=("NWC", "WIO", "NWC"),
        feature_group_count=extended.shape[1],
        precision=lax.Precision.HIGHEST,
    )[0]
    channel_sum, channel_square = lax.psum(
        (jnp.sum(filtered, axis=1), jnp.sum(filtered * filtered, axis=1)), "tp"
    )
    mean_value = channel_sum / CONV
    variance = channel_square / CONV - mean_value * mean_value
    scaled = (filtered - mean_value[:, None]) * lax.rsqrt(variance + 1e-05)[:, None] * conv_gain
    conv_out = jax.nn.silu(scaled).astype(jnp.bfloat16)
    pieces = (
        lax.all_gather(attended_values, "tp", axis=1, tiled=True),
        lax.all_gather(conv_out, "tp", axis=1, tiled=True),
    )
    mixed = jnp.dot(pieces[0], attn_rows, preferred_element_type=jnp.float32) + jnp.dot(
        pieces[1], conv_rows, preferred_element_type=jnp.float32
    )
    return mixed.astype(jnp.bfloat16)


MESH = pl.DeviceIdType.MESH
A_CHUNKS = 2


def remote(src, dst, sems, index, target, send_index=None):
    send_sem, recv_sem = sems
    return pltpu.make_async_remote_copy(
        src_ref=src,
        dst_ref=dst,
        send_sem=send_sem.at[index if send_index is None else send_index],
        recv_sem=recv_sem.at[index],
        device_id=target,
        device_id_type=MESH,
    )


def greet(targets):
    barrier = pltpu.get_barrier_semaphore()
    for target in targets:
        pl.semaphore_signal(barrier, inc=1, device_id=target, device_id_type=MESH)
    pl.semaphore_wait(barrier, len(targets))


def spread_kernel(
    planes,
    normed,
    w_query,
    w_glu,
    w_gate,
    w_kv,
    out_attn,
    out_conv,
    rows_all,
    w_all,
    out_other,
    stage,
    bounce,
    local_sem,
    a_send,
    a_recv,
    ax_send,
    ax_recv,
    ac_send,
    ac_recv,
    w1_send,
    w1_recv,
    w2_send,
    w2_recv,
    w3_send,
    w3_recv,
    kc_send,
    kc_recv,
    o_send,
    o_recv,
):
    s, t = lax.axis_index("sp"), lax.axis_index("tp")
    z, y, x, c = s // 2, s % 2, t // 2, t % 2
    block = normed.shape[0]
    piece = block // planes
    step = piece // A_CHUNKS
    depth = w_query.shape[0]
    width = w_query.shape[1] // planes
    three = 3 * width
    half = depth // 2

    def at(zz, yy, tt):
        return {"sp": zz * 2 + yy, "tp": tt}

    across_y = at(z, 1 - y, t)
    across_x = at(z, y, (1 - x) * 2 + c)
    diagonal = at(z, y, (1 - x) * 2 + (1 - c))
    partner = at(z, y, x * 2 + (1 - c))
    others = [lax.rem(z + k, planes) for k in range(1, planes)]
    greet([across_y, across_x, diagonal, partner] + [at(zz, y, t) for zz in others])

    def rows_of(zz, tt, chunk):
        start = pl.multiple_of(zz * block + tt * piece + chunk * step, step)
        return rows_all.at[pl.ds(start, step)]

    def chain(way, distance, chunk):
        from_z = z - distance if way == 0 else z + distance
        to_z = z + 1 if way == 0 else z - 1
        target = rows_of(from_z, t, chunk)
        if distance == 0:
            start = pl.multiple_of(t * piece + chunk * step, step)
            source = normed.at[pl.ds(start, step)]
        else:
            source = target
        index = (way * planes + distance) * A_CHUNKS + chunk
        return remote(source, target, (a_send, a_recv), index, at(to_z, y, t))

    def chain_arrival(way, distance, chunk):
        from_z = z - distance if way == 0 else z + distance
        index = (way * planes + distance - 1) * A_CHUNKS + chunk
        return remote(rows_of(from_z, t, chunk), rows_of(from_z, t, chunk), (a_send, a_recv), index, across_x)

    def can_send(way, distance):
        if way == 0:
            return jnp.logical_and(z - distance >= 0, z + 1 < planes)
        return jnp.logical_and(z + distance < planes, z - 1 >= 0)

    def exists(way, distance):
        return z - distance >= 0 if way == 0 else z + distance < planes

    def sideways(way, distance, chunk):
        from_z = z - distance if way == 0 else z + distance
        ref = rows_of(from_z, t, chunk)
        index = (way * planes + distance) * A_CHUNKS + chunk
        return remote(ref, ref, (ax_send, ax_recv), index, across_x)

    def sideways_arrival(way, distance, chunk):
        from_z = z - distance if way == 0 else z + distance
        ref = rows_of(from_z, (1 - x) * 2 + c, chunk)
        index = (way * planes + distance) * A_CHUNKS + chunk
        return remote(ref, ref, (ax_send, ax_recv), index, across_x)

    def to_partner(way, distance, chunk, far):
        from_z = z - distance if way == 0 else z + distance
        tt = (1 - x) * 2 + c if far else t
        ref = rows_of(from_z, tt, chunk)
        index = ((way * planes + distance) * A_CHUNKS + chunk) * 2 + far
        return remote(ref, ref, (ac_send, ac_recv), index, partner)

    def partner_arrival(way, distance, chunk, far):
        from_z = z - distance if way == 0 else z + distance
        tt = (1 - x) * 2 + (1 - c) if far else x * 2 + (1 - c)
        ref = rows_of(from_z, tt, chunk)
        index = ((way * planes + distance) * A_CHUNKS + chunk) * 2 + far
        return remote(ref, ref, (ac_send, ac_recv), index, partner)

    def home(zz, yy):
        return pl.multiple_of((zz * 2 + yy) * depth, depth)

    def wide(ref, start):
        return ref.at[pl.ds(start, depth), pl.ds(0, three)]

    def narrow(ref, start, cc):
        return ref.at[pl.ds(pl.multiple_of(start + cc * half, half), half), pl.ds(three, width)]

    def w_sources(tt):
        cols = pl.ds(pl.multiple_of(tt * width, width), width)
        return [w_query.at[:, cols], w_glu.at[:, cols], w_gate.at[:, cols], w_kv.at[tt]]

    def w_targets(ref, start, cc):
        rows = pl.ds(start, depth)
        return [ref.at[rows, pl.ds(g * width, width)] for g in range(3)] + [narrow(ref, start, cc)]

    def first(kind, target, tt, src_t, ref, start):
        return [
            remote(a, b, (w1_send, w1_recv), kind * 4 + i, target)
            for i, (a, b) in enumerate(zip(w_sources(tt), w_targets(ref, start, tt % 2)))
        ]

    def first_all(kind, target, tt, what):
        @pl.when(t == z)
        def _():
            for copy in first(kind, target, tt, t, w_all, home(z, y)):
                what(copy)

        @pl.when(t != z)
        def _():
            for copy in first(kind, target, tt, t, stage, pl.multiple_of(t * depth, depth)):
                what(copy)

    def first_arrival(kind, src_t):
        @pl.when(src_t == z)
        def _():
            for i, ref in enumerate(w_targets(w_all, home(z, y), c)):
                remote(ref, ref, (w1_send, w1_recv), kind * 4 + i, across_x).wait_recv()

        @pl.when(src_t != z)
        def _():
            for i, ref in enumerate(w_targets(stage, pl.multiple_of(src_t * depth, depth), c)):
                remote(ref, ref, (w1_send, w1_recv), kind * 4 + i, across_x).wait_recv()

    def second_local():
        return [
            remote(a, b, (w2_send, w2_recv), z * 4 + i, at(t, y, t), t * 4 + i)
            for i, (a, b) in enumerate(zip(w_sources(t), w_targets(w_all, home(z, y), c)))
        ]

    def second_staged(src_t):
        start = pl.multiple_of(src_t * depth, depth)
        return [
            remote(a, b, (w2_send, w2_recv), z * 4 + i, at(src_t, y, t), src_t * 4 + i)
            for a, b, i in (
                (wide(stage, start), wide(w_all, home(z, y)), 0),
                (narrow(stage, start, c), narrow(w_all, home(z, y), c), 3),
            )
        ]

    def second_arrival(from_z):
        ref_start = home(from_z, y)

        @pl.when(t == z)
        def _():
            for i, ref in enumerate(w_targets(w_all, ref_start, c)):
                remote(ref, ref, (w2_send, w2_recv), from_z * 4 + i, across_x).wait_recv()

        @pl.when(t != z)
        def _():
            for ref, index in (
                (wide(w_all, ref_start), from_z * 4),
                (narrow(w_all, ref_start, c), from_z * 4 + 3),
            ):
                remote(ref, ref, (w2_send, w2_recv), index, across_x).wait_recv()

    def third(from_z):
        start = home(from_z, y)
        return [
            remote(wide(w_all, start), wide(w_all, start), (w3_send, w3_recv), from_z * 2, across_y),
            remote(narrow(w_all, start, c), narrow(w_all, start, c), (w3_send, w3_recv), from_z * 2 + 1, across_y),
        ]

    def third_arrival(from_z):
        start = home(from_z, 1 - y)
        for ref, index in (
            (narrow(w_all, start, c), from_z * 2 + 1),
            (wide(w_all, start), from_z * 2),
        ):
            remote(ref, ref, (w3_send, w3_recv), index, across_y).wait_recv()

    def to_share(from_z, own):
        ref = narrow(w_all, home(from_z, y if own else 1 - y), c)
        return remote(ref, ref, (kc_send, kc_recv), from_z * 2 + own, partner)

    def share_arrival(from_z, own):
        ref = narrow(w_all, home(from_z, y if own else 1 - y), 1 - c)
        return remote(ref, ref, (kc_send, kc_recv), from_z * 2 + own, partner)

    outs = [
        remote(out_attn, out_other.at[0], (o_send, o_recv), 0, across_y),
        remote(out_conv, out_other.at[1], (o_send, o_recv), 1, across_y),
    ]

    own_rows = pltpu.make_async_copy(
        normed, rows_all.at[pl.ds(pl.multiple_of(z * block, block), block)], local_sem.at[0]
    )
    own_rows.start()

    for chunk in range(A_CHUNKS):
        for way in range(2):
            @pl.when(can_send(way, 0))
            def _():
                chain(way, 0, chunk).start()
    tx, td, tp = (1 - x) * 2 + c, (1 - x) * 2 + (1 - c), x * 2 + (1 - c)
    first_all(2, partner, tp, lambda copy: copy.start())
    first_all(0, across_x, tx, lambda copy: copy.start())
    first_all(1, diagonal, td, lambda copy: copy.start())
    for copy in outs:
        copy.start()

    @pl.when(t != z)
    def _():
        for copy in second_local():
            copy.start()

    def loads():
        return [
            pltpu.make_async_copy(a, b, local_sem.at[1 + i])
            for i, (a, b) in enumerate(zip(w_sources(t), [bounce.at[:, pl.ds(g * width, width)] for g in range(3)] + [bounce.at[pl.ds(0, half), pl.ds(three, width)]]))
        ]

    def stores():
        return [
            pltpu.make_async_copy(a, b, local_sem.at[1 + i])
            for i, (a, b) in enumerate(zip([bounce.at[:, pl.ds(g * width, width)] for g in range(3)] + [bounce.at[pl.ds(0, half), pl.ds(three, width)]], w_targets(w_all, home(z, y), c)))
        ]

    @pl.when(t == z)
    def _():
        for copy in loads():
            copy.start()
        for copy in loads():
            copy.wait()
        for copy in stores():
            copy.start()
        for copy in stores():
            copy.wait()

    def pass_on(src_t):
        @pl.when(src_t != z)
        def _():
            for copy in second_staged(src_t):
                copy.start()

    def chain_step(distance):
        for chunk in range(A_CHUNKS):
            for way in range(2):
                @pl.when(exists(way, distance))
                def _():
                    chain_arrival(way, distance, chunk).wait_recv()

                    @pl.when(can_send(way, distance))
                    def _():
                        chain(way, distance, chunk).start()

                    sideways(way, distance, chunk).start()
                    to_partner(way, distance, chunk, 0).start()

    def sideways_step(distance):
        for chunk in range(A_CHUNKS):
            for way in range(2):
                @pl.when(exists(way, distance))
                def _():
                    sideways_arrival(way, distance, chunk).wait_recv()
                    to_partner(way, distance, chunk, 1).start()

    def settle(from_z):
        for copy in third(from_z):
            copy.start()
        to_share(from_z, 1).start()

    first_arrival(2, tp)
    pass_on(tp)
    chain_step(1)
    first_arrival(0, tx)
    pass_on(tx)
    first_arrival(1, td)
    pass_on(td)
    settle(z)

    def plane_step(distance):
        for way in range(2):
            from_z = z - distance if way == 0 else z + distance

            @pl.when(exists(way, distance))
            def _():
                second_arrival(from_z)
                settle(from_z)

    plane_step(1)
    chain_step(2)
    sideways_step(1)
    plane_step(2)
    chain_step(3)
    plane_step(3)
    sideways_step(2)
    sideways_step(3)
    for k in range(planes):
        from_z = lax.rem(z + k, planes)
        third_arrival(from_z)
        to_share(from_z, 0).start()
    for copy in outs:
        copy.wait_recv()
    for distance in range(1, planes):
        for chunk in range(A_CHUNKS):
            for way in range(2):
                @pl.when(exists(way, distance))
                def _():
                    for far in range(2):
                        partner_arrival(way, distance, chunk, far).wait_recv()
    for k in range(planes):
        from_z = lax.rem(z + k, planes)
        for own in range(2):
            share_arrival(from_z, own).wait_recv()

    own_rows.wait()
    for copy in outs:
        copy.wait_send()
    first_all(2, partner, tp, lambda copy: copy.wait_send())
    first_all(0, across_x, tx, lambda copy: copy.wait_send())
    first_all(1, diagonal, td, lambda copy: copy.wait_send())

    @pl.when(t != z)
    def _():
        for copy in second_local():
            copy.wait_send()

    for src_t in (tp, tx, td):
        @pl.when(src_t != z)
        def _():
            for copy in second_staged(src_t):
                copy.wait_send()

    for k in range(planes):
        from_z = lax.rem(z + k, planes)
        for copy in third(from_z):
            copy.wait_send()
        for own in range(2):
            to_share(from_z, own).wait_send()
    for distance in range(planes):
        for chunk in range(A_CHUNKS):
            for way in range(2):
                @pl.when(can_send(way, distance))
                def _():
                    chain(way, distance, chunk).wait_send()

                if distance:
                    @pl.when(exists(way, distance))
                    def _():
                        sideways(way, distance, chunk).wait_send()
                        for far in range(2):
                            to_partner(way, distance, chunk, far).wait_send()


def spread(normed, w_query, w_glu, w_gate, w_kv, out_attn, out_conv, planes):
    depth, cols = w_query.shape
    width = cols // planes
    any_spec = pl.BlockSpec(memory_space=pl.ANY)
    count = 2 * planes * A_CHUNKS
    pairs = [count, count, 2 * count, 12, 4 * planes, 2 * planes, 2 * planes, 2]
    sems = []
    for n in pairs:
        sems += [pltpu.SemaphoreType.DMA((n,)), pltpu.SemaphoreType.DMA((n,))]
    return pl.pallas_call(
        functools.partial(spread_kernel, planes),
        out_shape=[
            jax.ShapeDtypeStruct((planes * normed.shape[0], normed.shape[1]), jnp.bfloat16),
            jax.ShapeDtypeStruct((2 * planes * depth, 4 * width), jnp.bfloat16),
            jax.ShapeDtypeStruct((2,) + out_attn.shape, jnp.bfloat16),
            jax.ShapeDtypeStruct((planes * depth, 4 * width), jnp.bfloat16),
        ],
        in_specs=[pl.BlockSpec(memory_space=pltpu.VMEM)] + [any_spec] * 6,
        out_specs=[any_spec] * 4,
        scratch_shapes=[
            pltpu.VMEM((depth, 4 * width), jnp.bfloat16),
            pltpu.SemaphoreType.DMA((8,)),
        ]
        + sems,
        compiler_params=pltpu.CompilerParams(collective_id=0, has_side_effects=True),
    )(normed, w_query, w_glu, w_gate, w_kv, out_attn, out_conv)


OUT_CHUNKS = 2


def merge_kernel(
    planes,
    channels,
    att,
    filtered,
    stats,
    gain,
    out_attn,
    out_conv,
    out_other,
    mixed,
    act,
    weights,
    stats_all,
    in_up,
    in_down,
    outgoing,
    local_sem,
    s_send,
    s_recv,
    x_send,
    x_recv,
    c_send,
    c_recv,
    r_send,
    r_recv,
):
    s, t = lax.axis_index("sp"), lax.axis_index("tp")
    z, y, x, c = s // 2, s % 2, t // 2, t % 2
    width = att.shape[1]
    rows = att.shape[0]
    block = rows // planes
    group = out_attn.shape[0]
    part = planes * width

    def at(zz, yy, tt):
        return {"sp": zz * 2 + yy, "tp": tt}

    size = planes * planes
    mine = z * planes + t
    peers = [lax.rem(mine + k, size) for k in range(1, size)]
    greet([at(g // planes, y, g % planes) for g in peers])
    tx, tp = (1 - x) * 2 + c, x * 2 + (1 - c)
    td = (1 - x) * 2 + (1 - c)

    loads = [
        pltpu.make_async_copy(
            a, weights.at[pl.ds(pl.multiple_of(base + yy * group, group), group)], local_sem.at[i]
        )
        for i, (a, base, yy) in enumerate(
            (
                (out_attn, 0, y),
                (out_other.at[0], 0, 1 - y),
                (out_conv, part, y),
                (out_other.at[1], part, 1 - y),
            )
        )
    ]
    for load in loads:
        load.start()

    def stat(k):
        g = peers[k]
        return pltpu.make_async_remote_copy(
            src_ref=stats,
            dst_ref=stats_all.at[mine],
            send_sem=s_send.at[k],
            recv_sem=s_recv.at[mine],
            device_id=at(g // planes, y, g % planes),
            device_id_type=MESH,
        )

    for k in range(size - 1):
        stat(k).start()

    def columns(kind, tt):
        return pl.ds(pl.multiple_of(kind * part + tt * width, width), width)

    def region(kind, r, tt):
        return act.at[pl.ds(r * block, block), columns(kind, tt)]

    def source(kind, r):
        return att.at[pl.ds(r * block, block)] if kind == 0 else region(1, r, t)

    def cross(kind, r):
        return remote(source(kind, r), region(kind, r, t), (x_send, x_recv), kind * planes + r, at(z, y, tx))

    def cross_arrival(kind, r):
        return remote(region(kind, r, tx), region(kind, r, tx), (x_send, x_recv), kind * planes + r, at(z, y, tx))

    def hand(kind, r, far):
        src = region(kind, r, tx) if far else source(kind, r)
        dst = region(kind, r, tx) if far else region(kind, r, t)
        return remote(src, dst, (c_send, c_recv), (kind * planes + r) * 2 + far, at(z, y, tp))

    def hand_arrival(kind, r, far):
        ref = region(kind, r, td if far else tp)
        return remote(ref, ref, (c_send, c_recv), (kind * planes + r) * 2 + far, at(z, y, tp))

    for r in range(planes):
        cross(0, r).start()
        hand(0, r, 0).start()
    act[:, columns(0, t)] = att[...]
    stats_all[mine] = stats[...]
    for g in peers:
        ref = stats_all.at[g]
        pltpu.make_async_remote_copy(
            src_ref=ref,
            dst_ref=ref,
            send_sem=s_send.at[0],
            recv_sem=s_recv.at[g],
            device_id=at(z, y, tp),
            device_id_type=MESH,
        ).wait_recv()
    total = stats_all[0]
    for g in range(1, size):
        total = total + stats_all[g]
    tiles = total.shape[0] // 2
    mean = total[:tiles] / channels
    variance = total[tiles:] / channels - mean * mean
    rate = lax.rsqrt(variance + 1e-05)
    lanes = total.shape[1]
    per = block // lanes
    for r in range(planes):
        for k in range(r * per, (r + 1) * per):
            mean_col = jnp.transpose(jnp.broadcast_to(mean[k : k + 1], (lanes, lanes)))
            rate_col = jnp.transpose(jnp.broadcast_to(rate[k : k + 1], (lanes, lanes)))
            scaled = (filtered[k * lanes : (k + 1) * lanes] - mean_col[:, :width]) * rate_col[:, :width] * gain[...]
            act[k * lanes : (k + 1) * lanes, columns(1, t)] = (scaled / (1.0 + jnp.exp(-scaled))).astype(act.dtype)
        cross(1, r).start()
        hand(1, r, 0).start()
    for kind in range(2):
        for r in range(planes):
            cross_arrival(kind, r).wait_recv()
            hand(kind, r, 1).start()
    for load in loads:
        load.wait()
    for kind in range(2):
        for r in range(planes):
            for far in range(2):
                hand_arrival(kind, r, far).wait_recv()

    step = block // OUT_CHUNKS

    def partial(r, h, tile, wide):
        start = pl.multiple_of(r * block + h * step, step)
        cols = pl.ds(pl.multiple_of(tile * wide, wide), wide)
        return jnp.dot(act[pl.ds(start, step), :], weights[:, cols], preferred_element_type=jnp.float32), cols

    columns_out = mixed.shape[1]
    wide = min(256, columns_out)
    tiles_out = columns_out // wide

    def travel(way, r, h):
        rows_h = pl.ds(h * step, step)
        index = (way * planes + r) * OUT_CHUNKS + h
        into = in_up if way == 0 else in_down
        return remote(
            outgoing.at[r, rows_h],
            into.at[r, rows_h],
            (r_send, r_recv),
            index,
            at(z + 1 if way == 0 else z - 1, y, t),
        )

    def travelled(way, r, h):
        rows_h = pl.ds(h * step, step)
        index = (way * planes + r) * OUT_CHUNKS + h
        into = (in_up if way == 0 else in_down).at[r, rows_h]
        return remote(into, into, (r_send, r_recv), index, at(z, y, tp))

    for distance in range(planes - 1, 0, -1):
        for h in range(OUT_CHUNKS):
            rows_h = pl.ds(h * step, step)
            for way in range(2):
                r = z + distance if way == 0 else z - distance
                there = r < planes if way == 0 else r >= 0
                more = z > 0 if way == 0 else z < planes - 1
                into = in_up if way == 0 else in_down

                @pl.when(jnp.logical_and(there, jnp.logical_not(more)))
                def _():
                    @pl.loop(0, tiles_out)
                    def _(tile):
                        value, cols = partial(r, h, tile, wide)
                        outgoing[r, rows_h, cols] = value.astype(outgoing.dtype)

                    travel(way, r, h).start()

                @pl.when(jnp.logical_and(there, more))
                def _():
                    travelled(way, r, h).wait_recv()

                    @pl.loop(0, tiles_out)
                    def _(tile):
                        value, cols = partial(r, h, tile, wide)
                        outgoing[r, rows_h, cols] = (
                            value + into[r, rows_h, cols].astype(jnp.float32)
                        ).astype(outgoing.dtype)

                    travel(way, r, h).start()

    for h in range(OUT_CHUNKS):
        rows_h = pl.ds(h * step, step)

        @pl.when(z > 0)
        def _():
            travelled(0, z, h).wait_recv()

        @pl.when(z < planes - 1)
        def _():
            travelled(1, z, h).wait_recv()

        @pl.loop(0, tiles_out)
        def _(tile):
            value, cols = partial(z, h, tile, wide)
            below = in_up[z, rows_h, cols].astype(jnp.float32)
            above = in_down[z, rows_h, cols].astype(jnp.float32)
            value = value + jnp.where(z > 0, below, 0.0) + jnp.where(z < planes - 1, above, 0.0)
            mixed[rows_h, cols] = value.astype(mixed.dtype)

    for k in range(size - 1):
        stat(k).wait_send()
    for kind in range(2):
        for r in range(planes):
            cross(kind, r).wait_send()
            for far in range(2):
                hand(kind, r, far).wait_send()
    for distance in range(1, planes):
        for h in range(OUT_CHUNKS):
            for way in range(2):
                r = z + distance if way == 0 else z - distance

                @pl.when(r < planes if way == 0 else r >= 0)
                def _():
                    travel(way, r, h).wait_send()


def merge(att, filtered, stats, gain, out_attn, out_conv, out_other, planes, channels):
    rows, width = att.shape
    block = rows // planes
    any_spec = pl.BlockSpec(memory_space=pl.ANY)
    vmem = pl.BlockSpec(memory_space=pltpu.VMEM)
    cols = out_attn.shape[1]
    size = planes * planes
    dma = pltpu.SemaphoreType.DMA
    return pl.pallas_call(
        functools.partial(merge_kernel, planes, channels),
        out_shape=jax.ShapeDtypeStruct((block, cols), jnp.bfloat16),
        in_specs=[vmem] * 4 + [any_spec] * 3,
        out_specs=vmem,
        scratch_shapes=[
            pltpu.VMEM((rows, 2 * planes * width), jnp.bfloat16),
            pltpu.VMEM((2 * planes * width, cols), jnp.bfloat16),
            pltpu.VMEM((size,) + stats.shape, jnp.float32),
            pltpu.VMEM((planes, block, cols), jnp.bfloat16),
            pltpu.VMEM((planes, block, cols), jnp.bfloat16),
            pltpu.VMEM((planes, block, cols), jnp.bfloat16),
            dma((4,)),
            dma((size,)),
            dma((size,)),
            dma((2 * planes,)),
            dma((2 * planes,)),
            dma((4 * planes,)),
            dma((4 * planes,)),
            dma((2 * planes * OUT_CHUNKS,)),
            dma((2 * planes * OUT_CHUNKS,)),
        ],
        compiler_params=pltpu.CompilerParams(collective_id=1, has_side_effects=True),
    )(att, filtered, stats, gain, out_attn, out_conv, out_other)


def spread_per_device(
    tokens,
    norm_gain,
    w_query,
    w_key,
    w_value,
    w_glu,
    w_gate,
    sink_logit,
    conv_taps,
    conv_gain,
    out_attn,
    out_conv,
):
    planes = lax.axis_size("tp")
    block = tokens.shape[0]
    rows = planes * block
    s, t = lax.axis_index("sp"), lax.axis_index("tp")
    z, y = s // 2, s % 2
    tokens_f = tokens.astype(jnp.float32)
    normed = (
        tokens_f
        * lax.rsqrt(jnp.mean(tokens_f * tokens_f, axis=1, keepdims=True) + 1e-06)
        * norm_gain
    ).astype(jnp.bfloat16)
    depth = w_key.shape[0]
    kv = jnp.concatenate(
        [w_key.reshape(2, depth // 2, 2, HEAD), w_value.reshape(2, depth // 2, 2, HEAD)], axis=-1
    )
    w_kv = jnp.transpose(kv, (2, 0, 1, 3)).reshape(planes, depth // 2, 2 * HEAD)
    rows_all, w_all, out_other, _ = spread(
        normed, w_query, w_glu, w_gate, w_kv, out_attn, out_conv, planes
    )
    width = w_query.shape[1] // planes
    heads = width // HEAD
    acc = jnp.dot(rows_all, w_all, preferred_element_type=jnp.float32)
    positions = (
        (2 * jnp.arange(planes, dtype=jnp.int32) + y)[:, None] * block
        + jnp.arange(block, dtype=jnp.int32)[None, :]
    )
    flat_positions = positions.reshape(rows)
    queries = rotate_heads(acc[:, :width].reshape(rows, heads, HEAD), flat_positions).astype(
        jnp.bfloat16
    )
    keys_rot = rotate_heads(
        acc[:, 3 * width : 3 * width + HEAD].reshape(rows, 1, HEAD), flat_positions
    ).astype(jnp.bfloat16)
    keys_rot = keys_rot.reshape(planes, block, HEAD)
    values_bf = acc[:, 3 * width + HEAD :].astype(jnp.bfloat16).reshape(planes, block, HEAD)
    gated = (acc[:, width : 2 * width] * jax.nn.sigmoid(acc[:, 2 * width : 3 * width])).astype(
        jnp.bfloat16
    )
    gated = gated.reshape(planes, block, width)
    kv_tail = jnp.concatenate([keys_rot, values_bf], axis=2)[:, block - WINDOW :]
    tails = jnp.concatenate([kv_tail, gated[:, block - (KSIZE - 1) :]], axis=1)
    flips = [(i, i ^ 1) for i in range(lax.axis_size("sp"))]
    came = lax.ppermute(tails, "sp", flips)
    earlier = jnp.concatenate([jnp.zeros_like(came[:1]), came[:-1]], axis=0)
    rim = jnp.where(y == 1, came, earlier)
    blocks = block // WINDOW
    keys_all = jnp.concatenate([rim[:, :WINDOW, :HEAD], keys_rot], axis=1).reshape(
        planes, blocks + 1, WINDOW, HEAD
    )
    vals_all = jnp.concatenate([rim[:, :WINDOW, HEAD:], values_bf], axis=1).reshape(
        planes, blocks + 1, WINDOW, HEAD
    )
    key_blocks = jnp.concatenate([keys_all[:, :-1], keys_all[:, 1:]], axis=2).reshape(
        planes * blocks, 2 * WINDOW, HEAD
    )
    value_blocks = jnp.concatenate([vals_all[:, :-1], vals_all[:, 1:]], axis=2).reshape(
        planes * blocks, 2 * WINDOW, HEAD
    )
    query_blocks = queries.reshape(planes * blocks, WINDOW, heads, HEAD)
    scores = jnp.einsum(
        "bqgd,bkd->bgqk", query_blocks, key_blocks, preferred_element_type=jnp.float32
    ) * (1.0 / math.sqrt(HEAD))
    starts = positions[:, ::WINDOW].reshape(planes * blocks)[:, None, None]
    query_pos = starts + jnp.arange(WINDOW, dtype=jnp.int32)[None, :, None]
    key_pos = starts - WINDOW + jnp.arange(2 * WINDOW, dtype=jnp.int32)[None, None, :]
    distance = query_pos - key_pos
    allowed = (distance >= 0) & (distance < WINDOW) & (key_pos >= 0)
    scores = jnp.where(allowed[:, None], scores, -1e30)
    sink_all = lax.all_gather(sink_logit, "tp", tiled=True)
    sinks = lax.dynamic_slice(sink_all, (z * planes * heads + t * heads,), (heads,))
    sinks = sinks[None, :, None, None]
    highest = jnp.maximum(jnp.max(scores, axis=-1, keepdims=True), sinks)
    weights_exp = jnp.exp(scores - highest)
    denom = jnp.sum(weights_exp, axis=-1, keepdims=True) + jnp.exp(sinks - highest)
    probs = (weights_exp / denom).astype(jnp.bfloat16)
    attended = jnp.einsum(
        "bgqk,bkd->bqgd", probs, value_blocks, preferred_element_type=jnp.float32
    ).astype(jnp.bfloat16)
    attended = attended.reshape(rows, width)
    extended = jnp.concatenate([rim[:, WINDOW:], gated], axis=1).astype(jnp.float32)
    small = jnp.concatenate([conv_taps.astype(jnp.float32), conv_gain[None]], axis=0)
    small = lax.all_gather(small, "tp", axis=1, tiled=True)
    small = lax.dynamic_slice(small, (0, (z * planes + t) * width), (KSIZE + 1, width))
    filtered = lax.conv_general_dilated(
        extended,
        small[:KSIZE, None, :],
        (1,),
        "VALID",
        dimension_numbers=("NWC", "WIO", "NWC"),
        feature_group_count=width,
        precision=lax.Precision.HIGHEST,
    ).reshape(rows, width)
    stats = jnp.concatenate(
        [jnp.sum(filtered, axis=1).reshape(-1, 128), jnp.sum(filtered * filtered, axis=1).reshape(-1, 128)]
    )
    return merge(
        attended, filtered, stats, small[KSIZE:], out_attn, out_conv, out_other, planes, CONV
    )


def solution(mesh):
    planes, others = mesh.shape["tp"], mesh.shape["sp"]
    fits = others == 2 * planes and planes % 2 == 0 and HEADS % (planes * planes) == 0
    return jax.shard_map(
        spread_per_device if fits else gathered_per_device,
        mesh=mesh,
        in_specs=(
            P("sp", None),
            P(),
            P("sp", "tp"),
            P("sp", "tp"),
            P("sp", "tp"),
            P("sp", "tp"),
            P("sp", "tp"),
            P("tp"),
            P(None, "tp"),
            P("tp"),
            P("sp", "tp"),
            P("sp", "tp"),
        ),
        out_specs=P("sp", "tp"),
        check_vma=False,
    )
```

```python
import functools
import math

import jax
import jax.numpy as jnp
from jax import lax
from jax.experimental import pallas as pl
from jax.experimental.pallas import tpu as pltpu
from jax.sharding import PartitionSpec as P

HEADS = 32
HEAD = 64
KV = 8
CONV = 2048
KSIZE = 31
WINDOW = 128


def passed_along(block, axis, distance):
    devices = range(lax.axis_size(axis))
    route = [(i - distance, i) for i in devices if i - distance in devices]
    return lax.ppermute(block, axis, route)


def rotate_heads(values, positions):
    half_width = values.shape[-1] // 2
    frequency = 10000.0 ** (-jnp.arange(half_width, dtype=jnp.float32) * 2.0 / values.shape[-1])
    angles = positions.astype(jnp.float32)[:, None] * frequency[None, :]
    cosine = jnp.cos(angles)[:, None, :]
    sine_part = jnp.sin(angles)[:, None, :]
    first_half = values[..., :half_width]
    second_half = values[..., half_width:]
    return jnp.concatenate(
        [
            first_half * cosine - second_half * sine_part,
            second_half * cosine + first_half * sine_part,
        ],
        axis=-1,
    )


def ring_gather_kernel(n, count, *refs):
    shards, wholes = refs[:count], refs[count : 2 * count]
    bounce = refs[2 * count : 3 * count]
    in_sem, out_sem, send_sem, recv_sem = refs[3 * count :]
    me = lax.axis_index("sp")
    half = n // 2
    odd = lax.rem(me, 2)
    place = (1 - odd) * lax.div(me, 2) + odd * (n - 1 - lax.div(me, 2))

    def device_at(position):
        spot = lax.rem(position + 2 * n, n)
        back = lax.div(spot, half)
        return (1 - back) * 2 * spot + back * (2 * (n - 1 - spot) + 1)

    ahead, behind = device_at(place + 1), device_at(place - 1)
    barrier = pltpu.get_barrier_semaphore()
    for neighbour in (ahead, behind):
        pl.semaphore_signal(
            barrier, inc=1, device_id={"sp": neighbour}, device_id_type=pl.DeviceIdType.MESH
        )
    pl.semaphore_wait(barrier, 2)

    def block(array, owner, way):
        rows = shards[array].shape[0]
        part = rows // 2
        start = pl.multiple_of(owner * rows + way * part, part)
        return wholes[array].at[pl.ds(start, part)]

    def hop(array, step, way):
        owner = device_at(place - step) if way == 0 else device_at(place + step)
        part = shards[array].shape[0] // 2
        target = block(array, owner, way)
        source = shards[array].at[pl.ds(way * part, part)] if step == 0 else target
        return pltpu.make_async_remote_copy(
            src_ref=source,
            dst_ref=target,
            send_sem=send_sem.at[way, step, array],
            recv_sem=recv_sem.at[way, step, array],
            device_id={"sp": ahead if way == 0 else behind},
            device_id_type=pl.DeviceIdType.MESH,
        )

    def arrival(array, step, way):
        owner = device_at(place - step - 1) if way == 0 else device_at(place + step + 1)
        target = block(array, owner, way)
        return pltpu.make_async_remote_copy(
            src_ref=target,
            dst_ref=target,
            send_sem=send_sem.at[way, step, array],
            recv_sem=recv_sem.at[way, step, array],
            device_id={"sp": ahead if way == 0 else behind},
            device_id_type=pl.DeviceIdType.MESH,
        )

    for array in range(count):
        for way in range(2):
            hop(array, 0, way).start()
    loads = [
        pltpu.make_async_copy(shards[a], bounce[a], in_sem.at[a]) for a in range(count)
    ]
    for load in loads:
        load.start()
    stores = []
    for a in range(count):
        loads[a].wait()
        rows = shards[a].shape[0]
        mine = wholes[a].at[pl.ds(pl.multiple_of(me * rows, rows), rows)]
        stores.append(pltpu.make_async_copy(bounce[a], mine, out_sem.at[a]))
        stores[a].start()
    for step in range(1, n - 1):
        for array in range(count):
            for way in range(2):
                arrival(array, step - 1, way).wait_recv()
                hop(array, step, way).start()
    for array in range(count):
        for way in range(2):
            arrival(array, n - 2, way).wait_recv()
    for step in range(n - 1):
        for array in range(count):
            for way in range(2):
                hop(array, step, way).wait_send()
    for store in stores:
        store.wait()


def ring_gather(arrays, collective_id):
    n = lax.axis_size("sp")
    count = len(arrays)
    return pl.pallas_call(
        functools.partial(ring_gather_kernel, n, count),
        out_shape=[
            jax.ShapeDtypeStruct((n * a.shape[0],) + a.shape[1:], a.dtype) for a in arrays
        ],
        in_specs=[pl.BlockSpec(memory_space=pl.ANY)] * count,
        out_specs=[pl.BlockSpec(memory_space=pl.ANY)] * count,
        scratch_shapes=[pltpu.VMEM(a.shape, a.dtype) for a in arrays]
        + [
            pltpu.SemaphoreType.DMA((count,)),
            pltpu.SemaphoreType.DMA((count,)),
            pltpu.SemaphoreType.DMA((2, n - 1, count)),
            pltpu.SemaphoreType.DMA((2, n - 1, count)),
        ],
        compiler_params=pltpu.CompilerParams(
            collective_id=collective_id, has_side_effects=True
        ),
    )(*arrays)


def gathered_per_device(
    tokens,
    norm_gain,
    w_query,
    w_key,
    w_value,
    w_glu,
    w_gate,
    sink_logit,
    conv_taps,
    conv_gain,
    out_attn,
    out_conv,
):
    row_count = tokens.shape[0]
    offset_rows = lax.axis_index("sp") * row_count
    positions = offset_rows + jnp.arange(row_count, dtype=jnp.int32)
    tokens_f = tokens.astype(jnp.float32)
    normed = (
        tokens_f
        * lax.rsqrt(jnp.mean(tokens_f * tokens_f, axis=1, keepdims=True) + 1e-06)
        * norm_gain
    ).astype(jnp.bfloat16)
    local_heads = w_query.shape[1] // HEAD
    local_kv = w_key.shape[1] // HEAD
    group_size = HEADS // KV
    kv_width = local_kv * HEAD
    *pieces, attn_rows, conv_rows = ring_gather(
        (w_query, w_key, w_value, w_glu, w_gate, out_attn, out_conv), 0
    )
    query_acc, key_acc, value_acc, glu_acc, gate_acc = tuple(
        (
            jnp.dot(normed, weight_piece, preferred_element_type=jnp.float32)
            for weight_piece in pieces
        )
    )
    queries = rotate_heads(query_acc.reshape(row_count, local_heads, HEAD), positions).astype(
        jnp.bfloat16
    )
    keys_rot = rotate_heads(key_acc.reshape(row_count, local_kv, HEAD), positions).astype(
        jnp.bfloat16
    )
    keys_rot = keys_rot.reshape(row_count, kv_width)
    values_bf = value_acc.astype(jnp.bfloat16)
    kv_tail = jnp.concatenate(
        [keys_rot[row_count - WINDOW :], values_bf[row_count - WINDOW :]], axis=1
    )
    kv_rim = passed_along(kv_tail, "sp", 1)
    gated = (glu_acc * jax.nn.sigmoid(gate_acc)).astype(jnp.bfloat16)
    conv_tail = gated[row_count - (KSIZE - 1) :]
    conv_rim = passed_along(conv_tail, "sp", 1)
    block_count = row_count // WINDOW
    keys_all = jnp.concatenate([kv_rim[:, :kv_width], keys_rot], axis=0).reshape(
        block_count + 1, WINDOW, local_kv, HEAD
    )
    vals_all = jnp.concatenate([kv_rim[:, kv_width:], values_bf], axis=0).reshape(
        block_count + 1, WINDOW, local_kv, HEAD
    )
    key_blocks = jnp.concatenate([keys_all[:-1], keys_all[1:]], axis=1)
    value_blocks = jnp.concatenate([vals_all[:-1], vals_all[1:]], axis=1)
    query_block_rows = queries.reshape(block_count, WINDOW, local_kv, group_size, HEAD)
    score_matrix = jnp.einsum(
        "bqhgd,bkhd->bhgqk", query_block_rows, key_blocks, preferred_element_type=jnp.float32
    ) * (1.0 / math.sqrt(HEAD))
    block_ids = jnp.arange(block_count, dtype=jnp.int32)[:, None, None]
    query_pos = (
        offset_rows + block_ids * WINDOW + jnp.arange(WINDOW, dtype=jnp.int32)[None, :, None]
    )
    key_pos = (
        offset_rows
        + (block_ids - 1) * WINDOW
        + jnp.arange(2 * WINDOW, dtype=jnp.int32)[None, None, :]
    )
    distance = query_pos - key_pos
    allowed = (distance >= 0) & (distance < WINDOW) & (key_pos >= 0)
    score_matrix = jnp.where(allowed[:, None, None], score_matrix, -1e30)
    sink_local = sink_logit.reshape(local_kv, group_size)[None, :, :, None, None]
    highest = jnp.maximum(jnp.max(score_matrix, axis=-1, keepdims=True), sink_local)
    weights_exp = jnp.exp(score_matrix - highest)
    denom_total = jnp.sum(weights_exp, axis=-1, keepdims=True) + jnp.exp(sink_local - highest)
    weights_bfloat_half = (weights_exp / denom_total).astype(jnp.bfloat16)
    attended_values = jnp.einsum(
        "bhgqk,bkhd->bqhgd", weights_bfloat_half, value_blocks, preferred_element_type=jnp.float32
    ).astype(jnp.bfloat16)
    attended_values = attended_values.reshape(row_count, local_heads * HEAD)
    extended = jnp.concatenate([conv_rim, gated], axis=0).astype(jnp.float32)
    filtered = lax.conv_general_dilated(
        extended[None],
        conv_taps.astype(jnp.float32)[:, None, :],
        (1,),
        "VALID",
        dimension_numbers=("NWC", "WIO", "NWC"),
        feature_group_count=extended.shape[1],
        precision=lax.Precision.HIGHEST,
    )[0]
    channel_sum, channel_square = lax.psum(
        (jnp.sum(filtered, axis=1), jnp.sum(filtered * filtered, axis=1)), "tp"
    )
    mean_value = channel_sum / CONV
    variance = channel_square / CONV - mean_value * mean_value
    scaled = (filtered - mean_value[:, None]) * lax.rsqrt(variance + 1e-05)[:, None] * conv_gain
    conv_out = jax.nn.silu(scaled).astype(jnp.bfloat16)
    pieces = (
        lax.all_gather(attended_values, "tp", axis=1, tiled=True),
        lax.all_gather(conv_out, "tp", axis=1, tiled=True),
    )
    mixed = jnp.dot(pieces[0], attn_rows, preferred_element_type=jnp.float32) + jnp.dot(
        pieces[1], conv_rows, preferred_element_type=jnp.float32
    )
    return mixed.astype(jnp.bfloat16)


MESH = pl.DeviceIdType.MESH
A_CHUNKS = 2
OUT_CHUNKS = 2
LANES = 128


def remote(src, dst, sems, index, target, send_index=None):
    send_sem, recv_sem = sems
    return pltpu.make_async_remote_copy(
        src_ref=src,
        dst_ref=dst,
        send_sem=send_sem.at[index if send_index is None else send_index],
        recv_sem=recv_sem.at[index],
        device_id=target,
        device_id_type=MESH,
    )


def layer_kernel(planes, channels, *refs):
    (tokens, norm_gain, freq, w_key, w_value, taps, conv_gain, sink) = refs[:8]
    (w_query, w_glu, w_gate, out_attn, out_conv) = refs[8:13]
    mixed = refs[13]
    (rows_all, w_all, stage, w_kv, small_src, small) = refs[14:20]
    (acc, cosine, sine, q_b, kv_b, kv_rim, gated, gated_rim, extended, filtered) = refs[20:30]
    (act, weights, stats, stats_all, moments, in_up, in_down, outgoing) = refs[30:38]
    local_sem = refs[38]
    pairs = [(refs[39 + 2 * i], refs[40 + 2 * i]) for i in range((len(refs) - 39) // 2)]
    (a_sem, ax_sem, ac_sem, w1_sem, w2_sem, w3_sem, kc_sem, o_sem, small_sem) = pairs[:9]
    (halo_sem, s_sem, x_sem, c_sem, r_sem) = pairs[9:14]

    s, t = lax.axis_index("sp"), lax.axis_index("tp")
    z, y, x, c = s // 2, s % 2, t // 2, t % 2
    block = tokens.shape[0]
    rows = planes * block
    piece = block // planes
    step = piece // A_CHUNKS
    depth = w_query.shape[0]
    width = w_query.shape[1] // planes
    three = 3 * width
    half = depth // 2
    heads = width // HEAD
    group = out_attn.shape[0]
    part = planes * width
    size = planes * planes
    f32 = jnp.float32

    def at(zz, yy, tt):
        return {"sp": zz * 2 + yy, "tp": tt}

    tx, td, tp = (1 - x) * 2 + c, (1 - x) * 2 + (1 - c), x * 2 + (1 - c)
    across_y, across_x = at(z, 1 - y, t), at(z, y, tx)
    diagonal, partner = at(z, y, td), at(z, y, tp)
    mine = z * planes + t
    peers = [lax.rem(mine + k, size) for k in range(1, size)]

    barrier = pltpu.get_barrier_semaphore()
    for target in [across_y] + [at(g // planes, y, g % planes) for g in peers]:
        pl.semaphore_signal(barrier, inc=1, device_id=target, device_id_type=MESH)

    def normalise(start, count):
        @pl.loop(0, count // 16)
        def _(i):
            here = pl.multiple_of(start + i * 16, 16)
            value = tokens[pl.ds(here, 16), :].astype(f32)
            scale = lax.rsqrt(jnp.mean(value * value, axis=1, keepdims=True) + 1e-06)
            there = pl.multiple_of(z * block + here, 16)
            rows_all[pl.ds(there, 16), :] = (value * scale * norm_gain[...]).astype(rows_all.dtype)

    normalise(t * piece, piece)

    lane = lax.broadcasted_iota(jnp.int32, (half, 2 * HEAD), 1)
    for cc in range(2):
        key = w_key[cc * half : (cc + 1) * half, :].astype(f32)
        value = w_value[cc * half : (cc + 1) * half, :].astype(f32)
        w_kv[cc] = jnp.where(lane < HEAD, key, pltpu.roll(value, HEAD, 1)).astype(w_kv.dtype)
        w_kv[2 + cc] = jnp.where(lane < HEAD, pltpu.roll(key, HEAD, 1), value).astype(w_kv.dtype)
    small_src[...] = jnp.zeros_like(small_src)
    for tt in range(planes):
        cols = slice(tt * width, (tt + 1) * width)
        small_src[tt, 0:KSIZE, :] = taps[:, cols].astype(f32)
        small_src[tt, 32:33, :] = conv_gain[:, cols]
        small_src[tt, 33:34, 0 : sink.shape[1]] = sink[...]
    pl.semaphore_wait(barrier, size)

    def rows_of(zz, tt, chunk):
        start = pl.multiple_of(zz * block + tt * piece + chunk * step, step)
        return rows_all.at[pl.ds(start, step)]

    def origin(way, distance):
        return z - distance if way == 0 else z + distance

    def chain(way, distance, chunk):
        ref = rows_of(origin(way, distance), t, chunk)
        index = (way * planes + distance) * A_CHUNKS + chunk
        return remote(ref, ref, a_sem, index, at(z + 1 if way == 0 else z - 1, y, t))

    def chain_arrival(way, distance, chunk):
        ref = rows_of(origin(way, distance), t, chunk)
        index = (way * planes + distance - 1) * A_CHUNKS + chunk
        return remote(ref, ref, a_sem, index, across_x)

    def can_send(way, distance):
        if way == 0:
            return jnp.logical_and(z - distance >= 0, z + 1 < planes)
        return jnp.logical_and(z + distance < planes, z - 1 >= 0)

    def exists(way, distance):
        return z - distance >= 0 if way == 0 else z + distance < planes

    def sideways(way, distance, chunk, arrival=False):
        ref = rows_of(origin(way, distance), tx if arrival else t, chunk)
        index = (way * planes + distance) * A_CHUNKS + chunk
        return remote(ref, ref, ax_sem, index, across_x)

    def to_partner(way, distance, chunk, far, arrival=False):
        tt = (td if far else tp) if arrival else (tx if far else t)
        ref = rows_of(origin(way, distance), tt, chunk)
        index = ((way * planes + distance) * A_CHUNKS + chunk) * 2 + far
        return remote(ref, ref, ac_sem, index, partner)

    def home(zz, yy):
        return pl.multiple_of((zz * 2 + yy) * depth, depth)

    def wide(ref, start):
        return ref.at[pl.ds(start, depth), pl.ds(0, three)]

    def narrow(ref, start, cc):
        return ref.at[pl.ds(pl.multiple_of(start + cc * half, half), half), pl.ds(three, width)]

    def w_sources(tt):
        cols = pl.ds(pl.multiple_of(tt * width, width), width)
        return [w_query.at[:, cols], w_glu.at[:, cols], w_gate.at[:, cols], w_kv.at[tt]]

    def w_targets(ref, start, cc):
        here = pl.ds(start, depth)
        return [ref.at[here, pl.ds(g * width, width)] for g in range(3)] + [narrow(ref, start, cc)]

    def first_all(kind, target, tt, what):
        for here, ref, start in (
            (t == z, w_all, home(z, y)),
            (t != z, stage, pl.multiple_of(t * depth, depth)),
        ):
            @pl.when(here)
            def _():
                for i, (a, b) in enumerate(zip(w_sources(tt), w_targets(ref, start, tt % 2))):
                    what(remote(a, b, w1_sem, kind * 4 + i, target))

    def first_arrival(kind, src_t):
        for here, ref, start in (
            (src_t == z, w_all, home(z, y)),
            (src_t != z, stage, pl.multiple_of(src_t * depth, depth)),
        ):
            @pl.when(here)
            def _():
                for i, b in enumerate(w_targets(ref, start, c)):
                    remote(b, b, w1_sem, kind * 4 + i, across_x).wait_recv()

    def second_local():
        return [
            remote(a, b, w2_sem, z * 4 + i, at(t, y, t), t * 4 + i)
            for i, (a, b) in enumerate(zip(w_sources(t), w_targets(w_all, home(z, y), c)))
        ]

    def second_staged(src_t):
        start = pl.multiple_of(src_t * depth, depth)
        return [
            remote(a, b, w2_sem, z * 4 + i, at(src_t, y, t), src_t * 4 + i)
            for a, b, i in (
                (wide(stage, start), wide(w_all, home(z, y)), 0),
                (narrow(stage, start, c), narrow(w_all, home(z, y), c), 3),
            )
        ]

    def second_arrival(from_z):
        start = home(from_z, y)

        @pl.when(t == z)
        def _():
            for i, ref in enumerate(w_targets(w_all, start, c)):
                remote(ref, ref, w2_sem, from_z * 4 + i, across_x).wait_recv()

        @pl.when(t != z)
        def _():
            for ref, i in ((wide(w_all, start), 0), (narrow(w_all, start, c), 3)):
                remote(ref, ref, w2_sem, from_z * 4 + i, across_x).wait_recv()

    def third(from_z, arrival=False):
        start = home(from_z, 1 - y if arrival else y)
        return [
            remote(ref, ref, w3_sem, from_z * 2 + i, across_y)
            for i, ref in enumerate((narrow(w_all, start, c), wide(w_all, start)))
        ]

    def to_share(from_z, own, arrival=False):
        ref = narrow(w_all, home(from_z, y if own else 1 - y), 1 - c if arrival else c)
        return remote(ref, ref, kc_sem, from_z * 2 + own, partner)

    def out_copies(yy):
        low = pl.multiple_of(yy * group, group)
        high = pl.multiple_of(part + yy * group, group)
        return [weights.at[pl.ds(low, group)], weights.at[pl.ds(high, group)]]

    outs = [
        remote(a, b, o_sem, i, across_y)
        for i, (a, b) in enumerate(zip((out_attn, out_conv), out_copies(y)))
    ]
    out_loads = [
        pltpu.make_async_copy(a, b, local_sem.at[4 + i])
        for i, (a, b) in enumerate(zip((out_attn, out_conv), out_copies(y)))
    ]
    own_loads = [
        pltpu.make_async_copy(a, b, local_sem.at[i])
        for i, (a, b) in enumerate(zip(w_sources(t)[:3], w_targets(w_all, home(z, y), c)))
    ]

    for chunk in range(A_CHUNKS):
        for way in range(2):
            @pl.when(can_send(way, 0))
            def _():
                chain(way, 0, chunk).start()
    small_to = [(partner, tp, 0), (across_x, tx, 1), (diagonal, td, 2)]

    def small_copy(target, tt, i):
        return pltpu.make_async_remote_copy(
            src_ref=small_src.at[tt],
            dst_ref=small,
            send_sem=small_sem[0].at[i],
            recv_sem=small_sem[1].at[0],
            device_id=target,
            device_id_type=MESH,
        )

    @pl.when(t == z)
    def _():
        for args in small_to:
            small_copy(*args).start()
        small[...] = small_src[t]

    first_all(2, partner, tp, lambda copy: copy.start())
    first_all(0, across_x, tx, lambda copy: copy.start())
    first_all(1, diagonal, td, lambda copy: copy.start())
    for copy in outs:
        copy.start()
    for copy in out_loads:
        copy.start()

    @pl.when(t == z)
    def _():
        for copy in own_loads:
            copy.start()
        start = pl.multiple_of(home(z, y) + c * half, half)
        w_all[pl.ds(start, half), three : three + width] = w_kv[t]
        for copy in own_loads:
            copy.wait()

    def toward(target, way):
        return target > z if way == 0 else target < z

    def send_second(way):
        @pl.when(toward(t, way))
        def _():
            for copy in second_local():
                copy.start()

        for src_t in (tp, tx, td):
            @pl.when(toward(src_t, way))
            def _():
                for copy in second_staged(src_t):
                    copy.start()

    def first_arrivals():
        first_arrival(2, tp)
        first_arrival(0, tx)
        first_arrival(1, td)

    def chain_step(distance):
        for chunk in range(A_CHUNKS):
            for way in range(2):
                @pl.when(exists(way, distance))
                def _():
                    chain_arrival(way, distance, chunk).wait_recv()

                    @pl.when(can_send(way, distance))
                    def _():
                        chain(way, distance, chunk).start()

                    sideways(way, distance, chunk).start()
                    to_partner(way, distance, chunk, 0).start()

    def sideways_step(distance):
        for chunk in range(A_CHUNKS):
            for way in range(2):
                @pl.when(exists(way, distance))
                def _():
                    sideways(way, distance, chunk, True).wait_recv()
                    to_partner(way, distance, chunk, 1).start()

    def settle(from_z):
        to_share(from_z, 1).start()
        for copy in third(from_z):
            copy.start()

    def plane_step(distance):
        for way in range(2):
            @pl.when(exists(way, distance))
            def _():
                second_arrival(origin(way, distance))
                settle(origin(way, distance))

    ends = jnp.logical_or(z == 0, z == planes - 1)

    @pl.when(ends)
    def _():
        first_arrivals()
        for way in range(2):
            send_second(way)

    for k in range(1, planes):
        normalise(lax.rem(t + k, planes) * piece, piece)
    for distance in range(1, planes - 1):
        chain_step(distance)
        if distance == 1:
            @pl.when(jnp.logical_not(ends))
            def _():
                first_arrivals()

            settle(z)
        for way in range(2):
            @pl.when(jnp.logical_and(jnp.logical_not(ends), z == (distance if way == 0 else planes - 1 - distance)))
            def _():
                send_second(way)

    row = lax.broadcasted_iota(jnp.int32, (block, LANES), 0)
    for zz in range(planes):
        angle = ((2 * zz + y) * block + row).astype(f32) * freq[...]
        here = slice(zz * block, (zz + 1) * block)
        cosine[here, :] = jnp.cos(angle)
        sine[here, :] = jnp.sin(angle)

    chain_step(planes - 1)
    plane_step(1)
    sideways_step(1)
    plane_step(2)
    for distance in range(2, planes):
        sideways_step(distance)
    for distance in range(3, planes):
        plane_step(distance)
    for distance in range(1, planes):
        for chunk in range(A_CHUNKS):
            for way in range(2):
                @pl.when(exists(way, distance))
                def _():
                    for far in range(2):
                        to_partner(way, distance, chunk, far, True).wait_recv()

    ahead = 1 - 2 * (z // (planes // 2))
    tall = rows // 2

    def multiply(from_z, yy, fresh):
        start = home(from_z, yy)
        cols = pl.ds(start, depth)

        @pl.loop(0, 2)
        def _(i):
            here = pl.ds(pl.multiple_of(i * tall, tall), tall)
            value = jnp.dot(rows_all[here, cols], w_all[cols, :], preferred_element_type=f32)
            if fresh:
                acc[here, :] = value
            else:
                acc[here, :] += value

    to_share(z, 1, True).wait_recv()
    multiply(z, y, True)

    @pl.loop(1, planes)
    def _(k):
        from_z = lax.rem(z + k * ahead + planes, planes)
        to_share(from_z, 1, True).wait_recv()
        multiply(from_z, y, False)

    @pl.loop(0, planes)
    def _(k):
        from_z = lax.rem(z + k * ahead + planes, planes)
        narrow_copy, wide_copy = third(from_z, True)
        narrow_copy.wait_recv()
        to_share(from_z, 0).start()
        wide_copy.wait_recv()
        to_share(from_z, 0, True).wait_recv()
        multiply(from_z, 1 - y, False)

    lane = lax.broadcasted_iota(jnp.int32, (block, LANES), 1)
    low = lax.rem(lane, HEAD) < HEAD // 2

    def turned(value, here):
        other = jnp.where(low, -pltpu.roll(value, LANES - HEAD // 2, 1), pltpu.roll(value, HEAD // 2, 1))
        return value * cosine[here, :] + other * sine[here, :]

    def halo(kind, zz):
        if kind == 0:
            ref = kv_b.at[pl.ds((zz + 1) * block - WINDOW, WINDOW)]
            return remote(ref, kv_rim.at[zz + y], halo_sem, zz, across_y)
        ref = gated.at[pl.ds((zz + 1) * block - 32, 32)]
        return remote(ref, gated_rim.at[zz + y], halo_sem, planes + zz, across_y)

    def halo_arrival(kind, zz):
        ref = (kv_rim if kind == 0 else gated_rim).at[zz + 1 - y]
        return remote(ref, ref, halo_sem, kind * planes + zz, across_y)

    for zz in range(planes):
        here = slice(zz * block, (zz + 1) * block)
        value = acc[here, three:]
        kv_b[here, :] = jnp.where(lane < HEAD, turned(value, here), value).astype(kv_b.dtype)
        halo(0, zz).start()
    for zz in range(planes):
        here = slice(zz * block, (zz + 1) * block)
        gate = acc[here, 2 * width : three]
        value = (acc[here, width : 2 * width] * (1.0 / (1.0 + jnp.exp(-gate)))).astype(gated.dtype)
        gated[here, :] = value
        extended[zz, 32:, :] = value.astype(f32)
        halo(1, zz).start()

    @pl.when(y == 0)
    def _():
        kv_rim[0] = jnp.zeros_like(kv_rim[0])
        gated_rim[0] = jnp.zeros_like(gated_rim[0])

    for zz in range(planes):
        here = slice(zz * block, (zz + 1) * block)
        q_b[here, :] = (turned(acc[here, :width], here) * (1.0 / math.sqrt(HEAD))).astype(q_b.dtype)

    @pl.when(t != z)
    def _():
        small_copy(partner, tp, 0).wait_recv()

    lane_q = lax.broadcasted_iota(jnp.int32, (WINDOW, LANES), 1)
    lane_k = lax.broadcasted_iota(jnp.int32, (2 * WINDOW, LANES), 1)
    row_s = lax.rem(lax.broadcasted_iota(jnp.int32, (heads * WINDOW, 2 * WINDOW), 0), WINDOW)
    col_s = lax.broadcasted_iota(jnp.int32, (heads * WINDOW, 2 * WINDOW), 1)
    distance_s = row_s + WINDOW - col_s
    inside = jnp.logical_and(distance_s >= 0, distance_s < WINDOW)
    sink_row = small[33:34, :]
    lane_1 = lax.broadcasted_iota(jnp.int32, (1, LANES), 1)
    sinks = [
        jnp.sum(jnp.where(lane_1 == t * heads + h, sink_row, 0.0), axis=1, keepdims=True)
        for h in range(heads)
    ]
    sink_col = jnp.concatenate([jnp.broadcast_to(v, (WINDOW, 1)) for v in sinks], axis=0)

    def attend(first_row, keys, mask):
        query = q_b[pl.ds(first_row, WINDOW), :]
        keys_f = keys.astype(f32)
        swapped = pltpu.roll(keys_f, HEAD, 1)
        key_two = jnp.where(lane_k < HEAD, keys_f, swapped).astype(jnp.bfloat16)
        value_two = jnp.where(lane_k < HEAD, swapped, keys_f).astype(jnp.bfloat16)
        zero = jnp.zeros_like(query)
        stacked = jnp.concatenate(
            [jnp.where(lane_q // HEAD == h, query, zero) for h in range(heads)], axis=0
        )
        scores = lax.dot_general(
            stacked, key_two, (((1,), (1,)), ((), ())), preferred_element_type=f32
        )
        scores = jnp.where(mask, scores, -1e30)
        top = jnp.maximum(jnp.max(scores, axis=1, keepdims=True), sink_col)
        grown = jnp.exp(scores - top)
        total = jnp.sum(grown, axis=1, keepdims=True) + jnp.exp(sink_col - top)
        probs = (grown / total).astype(jnp.bfloat16)
        mixed_values = jnp.dot(probs, value_two, preferred_element_type=f32)
        result = mixed_values[:WINDOW]
        for h in range(1, heads):
            result = jnp.where(lane_q // HEAD == h, mixed_values[h * WINDOW : (h + 1) * WINDOW], result)
        act[pl.ds(first_row, WINDOW), columns(0, t)] = result.astype(act.dtype)

    def columns(kind, tt):
        return pl.ds(pl.multiple_of(kind * part + tt * width, width), width)

    blocks = block // WINDOW

    @pl.loop(0, planes)
    def _(zz):
        for b in range(1, blocks):
            start = pl.multiple_of(zz * block + b * WINDOW, WINDOW)
            before = pl.multiple_of(zz * block + (b - 1) * WINDOW, WINDOW)
            attend(start, kv_b[pl.ds(before, 2 * WINDOW), :], inside)

    for zz in range(planes):
        if zz < planes - 1:
            halo_arrival(1, zz).wait_recv()

        @pl.when(y == 1)
        def _():
            if zz == planes - 1:
                halo_arrival(1, zz).wait_recv()

    for zz in range(planes):
        extended[zz, 0:32, :] = gated_rim[zz].astype(f32)
    strip = 64

    @pl.loop(0, planes)
    def _(zz):
        @pl.loop(0, block // strip)
        def _(i):
            base = pl.multiple_of(i * strip, strip)
            window = extended[zz, pl.ds(base, strip + 32), :]
            total = window[2 : 2 + strip] * small[0:1, :]
            for k in range(1, KSIZE):
                total = total + window[2 + k : 2 + k + strip] * small[k : k + 1, :]
            filtered[pl.ds(pl.multiple_of(zz * block + base, strip), strip), :] = total

    tiles = rows // LANES
    for k in range(tiles):
        value = filtered[k * LANES : (k + 1) * LANES, :]
        total = jnp.sum(value, axis=1, keepdims=True)
        square = jnp.sum(value * value, axis=1, keepdims=True)
        stats[k : k + 1, :] = jnp.transpose(jnp.broadcast_to(total, (LANES, LANES)))[0:1]
        stats[tiles + k : tiles + k + 1, :] = jnp.transpose(jnp.broadcast_to(square, (LANES, LANES)))[0:1]

    def stat(k):
        g = peers[k]
        return pltpu.make_async_remote_copy(
            src_ref=stats,
            dst_ref=stats_all.at[mine],
            send_sem=s_sem[0].at[k],
            recv_sem=s_sem[1].at[mine],
            device_id=at(g // planes, y, g % planes),
            device_id_type=MESH,
        )

    for k in range(size - 1):
        stat(k).start()
    stats_all[mine] = stats[...]

    for zz in range(planes):
        if zz < planes - 1:
            halo_arrival(0, zz).wait_recv()

        @pl.when(y == 1)
        def _():
            if zz == planes - 1:
                halo_arrival(0, zz).wait_recv()

    @pl.loop(0, planes)
    def _(zz):
        start = pl.multiple_of(zz * block, block)
        keys = jnp.concatenate([kv_rim[zz], kv_b[pl.ds(start, WINDOW), :]], axis=0)
        began = jnp.logical_or(zz * 2 + y > 0, col_s >= WINDOW)
        attend(start, keys, jnp.logical_and(inside, began))

    def region(kind, r, tt):
        start = pl.multiple_of(r * block, block)
        return act.at[pl.ds(start, block), columns(kind, tt)]

    def cross(kind, r, arrival=False):
        ref = region(kind, r, tx if arrival else t)
        return remote(ref, ref, x_sem, kind * planes + r, across_x)

    def hand(kind, r, far, arrival=False):
        tt = (td if far else tp) if arrival else (tx if far else t)
        ref = region(kind, r, tt)
        return remote(ref, ref, c_sem, (kind * planes + r) * 2 + far, partner)

    near = z // (planes // 2)
    order = [(1 - near) * (planes - 1 - j) + near * j for j in range(planes)]
    for r in order:
        cross(0, r).start()
        hand(0, r, 0).start()
    for g in peers:
        ref = stats_all.at[g]
        pltpu.make_async_remote_copy(
            src_ref=ref,
            dst_ref=ref,
            send_sem=s_sem[0].at[0],
            recv_sem=s_sem[1].at[g],
            device_id=partner,
            device_id_type=MESH,
        ).wait_recv()
    total = stats_all[0]
    for g in range(1, size):
        total = total + stats_all[g]
    mean = total[:tiles] / channels
    variance = total[tiles:] / channels - mean * mean
    moments[0] = mean
    moments[1] = lax.rsqrt(variance + 1e-05)
    per = block // LANES

    def normed_out(r):
        for k in range(per):
            tile = r * per + k
            mean_col = jnp.transpose(jnp.broadcast_to(moments[0, pl.ds(tile, 1), :], (LANES, LANES)))
            rate_col = jnp.transpose(jnp.broadcast_to(moments[1, pl.ds(tile, 1), :], (LANES, LANES)))
            here = pl.ds(pl.multiple_of(tile * LANES, LANES), LANES)
            scaled = (filtered[here, :] - mean_col) * rate_col * small[32:33, :]
            act[here, columns(1, t)] = (scaled / (1.0 + jnp.exp(-scaled))).astype(act.dtype)

    for r in order:
        normed_out(r)
        cross(1, r).start()
        hand(1, r, 0).start()
    for copy in out_loads:
        copy.wait()
    for copy in outs:
        copy.wait_recv()
    for kind in range(2):
        for r in order:
            cross(kind, r, True).wait_recv()
            hand(kind, r, 1).start()
    for kind in range(2):
        for r in order:
            for far in range(2):
                hand(kind, r, far, True).wait_recv()

    out_step = block // OUT_CHUNKS
    columns_out = mixed.shape[1]
    tile_out = min(256, columns_out)

    def partial(r, h, tile):
        start = pl.multiple_of(r * block + h * out_step, out_step)
        cols = pl.ds(pl.multiple_of(tile * tile_out, tile_out), tile_out)
        value = jnp.dot(act[pl.ds(start, out_step), :], weights[:, cols], preferred_element_type=f32)
        return value, cols

    def travel(way, r, h, arrival=False):
        rows_h = pl.ds(h * out_step, out_step)
        into = (in_up if way == 0 else in_down).at[r, rows_h]
        index = (way * planes + r) * OUT_CHUNKS + h
        source = into if arrival else outgoing.at[r, rows_h]
        return remote(source, into, r_sem, index, across_y if arrival else at(z + 1 if way == 0 else z - 1, y, t))

    for distance in range(planes - 1, 0, -1):
        for h in range(OUT_CHUNKS):
            rows_h = pl.ds(h * out_step, out_step)
            for way in range(2):
                r = z + distance if way == 0 else z - distance
                there = r < planes if way == 0 else r >= 0
                more = z > 0 if way == 0 else z < planes - 1
                into = in_up if way == 0 else in_down

                @pl.when(jnp.logical_and(there, jnp.logical_not(more)))
                def _():
                    @pl.loop(0, columns_out // tile_out)
                    def _(tile):
                        value, cols = partial(r, h, tile)
                        outgoing[r, rows_h, cols] = value.astype(outgoing.dtype)

                    travel(way, r, h).start()

                @pl.when(jnp.logical_and(there, more))
                def _():
                    travel(way, r, h, True).wait_recv()

                    @pl.loop(0, columns_out // tile_out)
                    def _(tile):
                        value, cols = partial(r, h, tile)
                        outgoing[r, rows_h, cols] = (value + into[r, rows_h, cols].astype(f32)).astype(
                            outgoing.dtype
                        )

                    travel(way, r, h).start()

    for h in range(OUT_CHUNKS):
        rows_h = pl.ds(h * out_step, out_step)

        @pl.when(z > 0)
        def _():
            travel(0, z, h, True).wait_recv()

        @pl.when(z < planes - 1)
        def _():
            travel(1, z, h, True).wait_recv()

        @pl.loop(0, columns_out // tile_out)
        def _(tile):
            value, cols = partial(z, h, tile)
            below = in_up[z, rows_h, cols].astype(f32)
            above = in_down[z, rows_h, cols].astype(f32)
            value = value + jnp.where(z > 0, below, 0.0) + jnp.where(z < planes - 1, above, 0.0)
            mixed[rows_h, cols] = value.astype(mixed.dtype)

    @pl.when(t == z)
    def _():
        for args in small_to:
            small_copy(*args).wait_send()

    @pl.when(y == 0)
    def _():
        for kind in range(2):
            halo(kind, planes - 1).wait_send()

    @pl.when(y == 1)
    def _():
        for kind in range(2):
            halo(kind, planes - 1).wait_send()

    for zz in range(planes - 1):
        for kind in range(2):
            halo(kind, zz).wait_send()

    @pl.when(y == 0)
    def _():
        for kind in range(2):
            halo_arrival(kind, planes - 1).wait_recv()

    for copy in outs:
        copy.wait_send()
    first_all(2, partner, tp, lambda copy: copy.wait_send())
    first_all(0, across_x, tx, lambda copy: copy.wait_send())
    first_all(1, diagonal, td, lambda copy: copy.wait_send())

    @pl.when(t != z)
    def _():
        for copy in second_local():
            copy.wait_send()

    for src_t in (tp, tx, td):
        @pl.when(src_t != z)
        def _():
            for copy in second_staged(src_t):
                copy.wait_send()

    for zz in range(planes):
        for copy in third(zz):
            copy.wait_send()
        for own in range(2):
            to_share(zz, own).wait_send()
    for distance in range(planes):
        for chunk in range(A_CHUNKS):
            for way in range(2):
                @pl.when(can_send(way, distance))
                def _():
                    chain(way, distance, chunk).wait_send()

                if distance:
                    @pl.when(exists(way, distance))
                    def _():
                        sideways(way, distance, chunk).wait_send()
                        for far in range(2):
                            to_partner(way, distance, chunk, far).wait_send()
    for k in range(size - 1):
        stat(k).wait_send()
    for kind in range(2):
        for r in order:
            cross(kind, r).wait_send()
            for far in range(2):
                hand(kind, r, far).wait_send()
    for distance in range(1, planes):
        for h in range(OUT_CHUNKS):
            for way in range(2):
                r = z + distance if way == 0 else z - distance

                @pl.when(r < planes if way == 0 else r >= 0)
                def _():
                    travel(way, r, h).wait_send()


def planned_per_device(
    tokens,
    norm_gain,
    w_query,
    w_key,
    w_value,
    w_glu,
    w_gate,
    sink_logit,
    conv_taps,
    conv_gain,
    out_attn,
    out_conv,
):
    planes = lax.axis_size("tp")
    block, model = tokens.shape
    rows = planes * block
    depth, cols = w_query.shape
    width = cols // planes
    columns_out = out_attn.shape[1]
    size = planes * planes
    half_width = HEAD // 2
    freq = 10000.0 ** (-jnp.arange(half_width, dtype=jnp.float32) * 2.0 / HEAD)
    freq = jnp.tile(freq, LANES // half_width)[None]
    vmem = pl.BlockSpec(memory_space=pltpu.VMEM)
    any_spec = pl.BlockSpec(memory_space=pl.ANY)
    dma = pltpu.SemaphoreType.DMA
    bf16, f32 = jnp.bfloat16, jnp.float32
    tiles = rows // LANES
    chunks = 2 * planes * A_CHUNKS
    counts = [
        chunks, chunks, 2 * chunks, 12, 4 * planes, 2 * planes, 2 * planes, 2, 3,
        2 * planes, size, 2 * planes, 4 * planes, 2 * planes * OUT_CHUNKS,
    ]
    sems = [dma((n,)) for n in counts for _ in range(2)]
    return pl.pallas_call(
        functools.partial(layer_kernel, planes, CONV),
        out_shape=jax.ShapeDtypeStruct((block, columns_out), bf16),
        in_specs=[vmem] * 8 + [any_spec] * 5,
        out_specs=vmem,
        scratch_shapes=[
            pltpu.VMEM((rows, model), bf16),
            pltpu.VMEM((2 * planes * depth, 4 * width), bf16),
            pltpu.VMEM((planes * depth, 4 * width), bf16),
            pltpu.VMEM((planes, depth // 2, 2 * HEAD), bf16),
            pltpu.VMEM((planes, 40, width), f32),
            pltpu.VMEM((40, width), f32),
            pltpu.VMEM((rows, 4 * width), f32),
            pltpu.VMEM((rows, LANES), f32),
            pltpu.VMEM((rows, LANES), f32),
            pltpu.VMEM((rows, width), bf16),
            pltpu.VMEM((rows, width), bf16),
            pltpu.VMEM((planes + 1, WINDOW, width), bf16),
            pltpu.VMEM((rows, width), bf16),
            pltpu.VMEM((planes + 1, 32, width), bf16),
            pltpu.VMEM((planes, 32 + block, width), f32),
            pltpu.VMEM((rows, width), f32),
            pltpu.VMEM((rows, 2 * planes * width), bf16),
            pltpu.VMEM((2 * planes * width, columns_out), bf16),
            pltpu.VMEM((2 * tiles, LANES), f32),
            pltpu.VMEM((size, 2 * tiles, LANES), f32),
            pltpu.VMEM((2, tiles, LANES), f32),
            pltpu.VMEM((planes, block, columns_out), bf16),
            pltpu.VMEM((planes, block, columns_out), bf16),
            pltpu.VMEM((planes, block, columns_out), bf16),
            dma((8,)),
        ]
        + sems,
        compiler_params=pltpu.CompilerParams(
            collective_id=0, has_side_effects=True, vmem_limit_bytes=60 * 2**20
        ),
    )(
        tokens,
        norm_gain[None],
        freq,
        w_key,
        w_value,
        conv_taps,
        conv_gain[None],
        sink_logit[None],
        w_query,
        w_glu,
        w_gate,
        out_attn,
        out_conv,
    )


def solution(mesh):
    planes, others = mesh.shape["tp"], mesh.shape["sp"]
    fits = others == 2 * planes and planes % 2 == 0 and HEADS == 2 * planes * planes
    return jax.shard_map(
        planned_per_device if fits else gathered_per_device,
        mesh=mesh,
        in_specs=(
            P("sp", None),
            P(),
            P("sp", "tp"),
            P("sp", "tp"),
            P("sp", "tp"),
            P("sp", "tp"),
            P("sp", "tp"),
            P("tp"),
            P(None, "tp"),
            P("tp"),
            P("sp", "tp"),
            P("sp", "tp"),
        ),
        out_specs=P("sp", "tp"),
        check_vma=False,
    )
```

```python
import functools
import math

import jax
import jax.numpy as jnp
from jax import lax
from jax.experimental import pallas as pl
from jax.experimental.pallas import tpu as pltpu
from jax.sharding import PartitionSpec as P

HEADS = 32
HEAD = 64
KV = 8
CONV = 2048
KSIZE = 31
WINDOW = 128


def passed_along(block, axis, distance):
    devices = range(lax.axis_size(axis))
    route = [(i - distance, i) for i in devices if i - distance in devices]
    return lax.ppermute(block, axis, route)


def rotate_heads(values, positions):
    half_width = values.shape[-1] // 2
    frequency = 10000.0 ** (-jnp.arange(half_width, dtype=jnp.float32) * 2.0 / values.shape[-1])
    angles = positions.astype(jnp.float32)[:, None] * frequency[None, :]
    cosine = jnp.cos(angles)[:, None, :]
    sine_part = jnp.sin(angles)[:, None, :]
    first_half = values[..., :half_width]
    second_half = values[..., half_width:]
    return jnp.concatenate(
        [
            first_half * cosine - second_half * sine_part,
            second_half * cosine + first_half * sine_part,
        ],
        axis=-1,
    )


def ring_gather_kernel(n, count, *refs):
    shards, wholes = refs[:count], refs[count : 2 * count]
    bounce = refs[2 * count : 3 * count]
    in_sem, out_sem, send_sem, recv_sem = refs[3 * count :]
    me = lax.axis_index("sp")
    half = n // 2
    odd = lax.rem(me, 2)
    place = (1 - odd) * lax.div(me, 2) + odd * (n - 1 - lax.div(me, 2))

    def device_at(position):
        spot = lax.rem(position + 2 * n, n)
        back = lax.div(spot, half)
        return (1 - back) * 2 * spot + back * (2 * (n - 1 - spot) + 1)

    ahead, behind = device_at(place + 1), device_at(place - 1)
    barrier = pltpu.get_barrier_semaphore()
    for neighbour in (ahead, behind):
        pl.semaphore_signal(
            barrier, inc=1, device_id={"sp": neighbour}, device_id_type=pl.DeviceIdType.MESH
        )
    pl.semaphore_wait(barrier, 2)

    def block(array, owner, way):
        rows = shards[array].shape[0]
        part = rows // 2
        start = pl.multiple_of(owner * rows + way * part, part)
        return wholes[array].at[pl.ds(start, part)]

    def hop(array, step, way):
        owner = device_at(place - step) if way == 0 else device_at(place + step)
        part = shards[array].shape[0] // 2
        target = block(array, owner, way)
        source = shards[array].at[pl.ds(way * part, part)] if step == 0 else target
        return pltpu.make_async_remote_copy(
            src_ref=source,
            dst_ref=target,
            send_sem=send_sem.at[way, step, array],
            recv_sem=recv_sem.at[way, step, array],
            device_id={"sp": ahead if way == 0 else behind},
            device_id_type=pl.DeviceIdType.MESH,
        )

    def arrival(array, step, way):
        owner = device_at(place - step - 1) if way == 0 else device_at(place + step + 1)
        target = block(array, owner, way)
        return pltpu.make_async_remote_copy(
            src_ref=target,
            dst_ref=target,
            send_sem=send_sem.at[way, step, array],
            recv_sem=recv_sem.at[way, step, array],
            device_id={"sp": ahead if way == 0 else behind},
            device_id_type=pl.DeviceIdType.MESH,
        )

    for array in range(count):
        for way in range(2):
            hop(array, 0, way).start()
    loads = [
        pltpu.make_async_copy(shards[a], bounce[a], in_sem.at[a]) for a in range(count)
    ]
    for load in loads:
        load.start()
    stores = []
    for a in range(count):
        loads[a].wait()
        rows = shards[a].shape[0]
        mine = wholes[a].at[pl.ds(pl.multiple_of(me * rows, rows), rows)]
        stores.append(pltpu.make_async_copy(bounce[a], mine, out_sem.at[a]))
        stores[a].start()
    for step in range(1, n - 1):
        for array in range(count):
            for way in range(2):
                arrival(array, step - 1, way).wait_recv()
                hop(array, step, way).start()
    for array in range(count):
        for way in range(2):
            arrival(array, n - 2, way).wait_recv()
    for step in range(n - 1):
        for array in range(count):
            for way in range(2):
                hop(array, step, way).wait_send()
    for store in stores:
        store.wait()


def ring_gather(arrays, collective_id):
    n = lax.axis_size("sp")
    count = len(arrays)
    return pl.pallas_call(
        functools.partial(ring_gather_kernel, n, count),
        out_shape=[
            jax.ShapeDtypeStruct((n * a.shape[0],) + a.shape[1:], a.dtype) for a in arrays
        ],
        in_specs=[pl.BlockSpec(memory_space=pl.ANY)] * count,
        out_specs=[pl.BlockSpec(memory_space=pl.ANY)] * count,
        scratch_shapes=[pltpu.VMEM(a.shape, a.dtype) for a in arrays]
        + [
            pltpu.SemaphoreType.DMA((count,)),
            pltpu.SemaphoreType.DMA((count,)),
            pltpu.SemaphoreType.DMA((2, n - 1, count)),
            pltpu.SemaphoreType.DMA((2, n - 1, count)),
        ],
        compiler_params=pltpu.CompilerParams(
            collective_id=collective_id, has_side_effects=True
        ),
    )(*arrays)


def gathered_per_device(
    tokens,
    norm_gain,
    w_query,
    w_key,
    w_value,
    w_glu,
    w_gate,
    sink_logit,
    conv_taps,
    conv_gain,
    out_attn,
    out_conv,
):
    row_count = tokens.shape[0]
    offset_rows = lax.axis_index("sp") * row_count
    positions = offset_rows + jnp.arange(row_count, dtype=jnp.int32)
    tokens_f = tokens.astype(jnp.float32)
    normed = (
        tokens_f
        * lax.rsqrt(jnp.mean(tokens_f * tokens_f, axis=1, keepdims=True) + 1e-06)
        * norm_gain
    ).astype(jnp.bfloat16)
    local_heads = w_query.shape[1] // HEAD
    local_kv = w_key.shape[1] // HEAD
    group_size = HEADS // KV
    kv_width = local_kv * HEAD
    *pieces, attn_rows, conv_rows = ring_gather(
        (w_query, w_key, w_value, w_glu, w_gate, out_attn, out_conv), 0
    )
    query_acc, key_acc, value_acc, glu_acc, gate_acc = tuple(
        (
            jnp.dot(normed, weight_piece, preferred_element_type=jnp.float32)
            for weight_piece in pieces
        )
    )
    queries = rotate_heads(query_acc.reshape(row_count, local_heads, HEAD), positions).astype(
        jnp.bfloat16
    )
    keys_rot = rotate_heads(key_acc.reshape(row_count, local_kv, HEAD), positions).astype(
        jnp.bfloat16
    )
    keys_rot = keys_rot.reshape(row_count, kv_width)
    values_bf = value_acc.astype(jnp.bfloat16)
    kv_tail = jnp.concatenate(
        [keys_rot[row_count - WINDOW :], values_bf[row_count - WINDOW :]], axis=1
    )
    kv_rim = passed_along(kv_tail, "sp", 1)
    gated = (glu_acc * jax.nn.sigmoid(gate_acc)).astype(jnp.bfloat16)
    conv_tail = gated[row_count - (KSIZE - 1) :]
    conv_rim = passed_along(conv_tail, "sp", 1)
    block_count = row_count // WINDOW
    keys_all = jnp.concatenate([kv_rim[:, :kv_width], keys_rot], axis=0).reshape(
        block_count + 1, WINDOW, local_kv, HEAD
    )
    vals_all = jnp.concatenate([kv_rim[:, kv_width:], values_bf], axis=0).reshape(
        block_count + 1, WINDOW, local_kv, HEAD
    )
    key_blocks = jnp.concatenate([keys_all[:-1], keys_all[1:]], axis=1)
    value_blocks = jnp.concatenate([vals_all[:-1], vals_all[1:]], axis=1)
    query_block_rows = queries.reshape(block_count, WINDOW, local_kv, group_size, HEAD)
    score_matrix = jnp.einsum(
        "bqhgd,bkhd->bhgqk", query_block_rows, key_blocks, preferred_element_type=jnp.float32
    ) * (1.0 / math.sqrt(HEAD))
    block_ids = jnp.arange(block_count, dtype=jnp.int32)[:, None, None]
    query_pos = (
        offset_rows + block_ids * WINDOW + jnp.arange(WINDOW, dtype=jnp.int32)[None, :, None]
    )
    key_pos = (
        offset_rows
        + (block_ids - 1) * WINDOW
        + jnp.arange(2 * WINDOW, dtype=jnp.int32)[None, None, :]
    )
    distance = query_pos - key_pos
    allowed = (distance >= 0) & (distance < WINDOW) & (key_pos >= 0)
    score_matrix = jnp.where(allowed[:, None, None], score_matrix, -1e30)
    sink_local = sink_logit.reshape(local_kv, group_size)[None, :, :, None, None]
    highest = jnp.maximum(jnp.max(score_matrix, axis=-1, keepdims=True), sink_local)
    weights_exp = jnp.exp(score_matrix - highest)
    denom_total = jnp.sum(weights_exp, axis=-1, keepdims=True) + jnp.exp(sink_local - highest)
    weights_bfloat_half = (weights_exp / denom_total).astype(jnp.bfloat16)
    attended_values = jnp.einsum(
        "bhgqk,bkhd->bqhgd", weights_bfloat_half, value_blocks, preferred_element_type=jnp.float32
    ).astype(jnp.bfloat16)
    attended_values = attended_values.reshape(row_count, local_heads * HEAD)
    extended = jnp.concatenate([conv_rim, gated], axis=0).astype(jnp.float32)
    filtered = lax.conv_general_dilated(
        extended[None],
        conv_taps.astype(jnp.float32)[:, None, :],
        (1,),
        "VALID",
        dimension_numbers=("NWC", "WIO", "NWC"),
        feature_group_count=extended.shape[1],
        precision=lax.Precision.HIGHEST,
    )[0]
    channel_sum, channel_square = lax.psum(
        (jnp.sum(filtered, axis=1), jnp.sum(filtered * filtered, axis=1)), "tp"
    )
    mean_value = channel_sum / CONV
    variance = channel_square / CONV - mean_value * mean_value
    scaled = (filtered - mean_value[:, None]) * lax.rsqrt(variance + 1e-05)[:, None] * conv_gain
    conv_out = jax.nn.silu(scaled).astype(jnp.bfloat16)
    pieces = (
        lax.all_gather(attended_values, "tp", axis=1, tiled=True),
        lax.all_gather(conv_out, "tp", axis=1, tiled=True),
    )
    mixed = jnp.dot(pieces[0], attn_rows, preferred_element_type=jnp.float32) + jnp.dot(
        pieces[1], conv_rows, preferred_element_type=jnp.float32
    )
    return mixed.astype(jnp.bfloat16)


MESH = pl.DeviceIdType.MESH
A_CHUNKS = 4
W_CHUNKS = 4
OUT_CHUNKS = 2
LANES = 128


def remote(src, dst, sems, index, target, send_index=None):
    send_sem, recv_sem = sems
    return pltpu.make_async_remote_copy(
        src_ref=src,
        dst_ref=dst,
        send_sem=send_sem.at[index if send_index is None else send_index],
        recv_sem=recv_sem.at[index],
        device_id=target,
        device_id_type=MESH,
    )


def layer_kernel(planes, channels, *refs):
    (tokens, norm_gain, freq, w_key, w_value, taps, conv_gain, sink) = refs[:8]
    (w_query, w_glu, w_gate, out_attn, out_conv) = refs[8:13]
    mixed = refs[13]
    (rows_all, w_all, stage, w_kv, small_src, small) = refs[14:20]
    (acc, cosine, sine, q_b, kv_b, kv_rim, gated, gated_rim, extended, filtered) = refs[20:30]
    (act, weights, stats, stats_all, moments, in_up, in_down, outgoing) = refs[30:38]
    local_sem = refs[38]
    pairs = [(refs[39 + 2 * i], refs[40 + 2 * i]) for i in range((len(refs) - 39) // 2)]
    (a_sem, ax_sem, ac_sem, w1_sem, w2_sem, w3_sem, kc_sem, o_sem, small_sem) = pairs[:9]
    (halo_sem, s_sem, x_sem, c_sem, r_sem) = pairs[9:14]

    s, t = lax.axis_index("sp"), lax.axis_index("tp")
    z, y, x, c = s // 2, s % 2, t // 2, t % 2
    block = tokens.shape[0]
    rows = planes * block
    piece = block // planes
    step = piece // A_CHUNKS
    depth = w_query.shape[0]
    width = w_query.shape[1] // planes
    three = 3 * width
    half = depth // 2
    heads = width // HEAD
    group = out_attn.shape[0]
    part = planes * width
    size = planes * planes
    f32 = jnp.float32

    def at(zz, yy, tt):
        return {"sp": zz * 2 + yy, "tp": tt}

    tx, td, tp = (1 - x) * 2 + c, (1 - x) * 2 + (1 - c), x * 2 + (1 - c)
    across_y, across_x = at(z, 1 - y, t), at(z, y, tx)
    diagonal, partner = at(z, y, td), at(z, y, tp)
    mine = z * planes + t
    peers = [lax.rem(mine + k, size) for k in range(1, size)]

    barrier = pltpu.get_barrier_semaphore()
    for target in [across_y] + [at(g // planes, y, g % planes) for g in peers]:
        pl.semaphore_signal(barrier, inc=1, device_id=target, device_id_type=MESH)

    def normalise(start, count):
        @pl.loop(0, count // 16)
        def _(i):
            here = pl.multiple_of(start + i * 16, 16)
            value = tokens[pl.ds(here, 16), :].astype(f32)
            scale = lax.rsqrt(jnp.mean(value * value, axis=1, keepdims=True) + 1e-06)
            there = pl.multiple_of(z * block + here, 16)
            rows_all[pl.ds(there, 16), :] = (value * scale * norm_gain[...]).astype(rows_all.dtype)

    normalise(t * piece, piece)

    lane = lax.broadcasted_iota(jnp.int32, (half, 2 * HEAD), 1)
    for cc in range(2):
        key = w_key[cc * half : (cc + 1) * half, :].astype(f32)
        value = w_value[cc * half : (cc + 1) * half, :].astype(f32)
        w_kv[cc] = jnp.where(lane < HEAD, key, pltpu.roll(value, HEAD, 1)).astype(w_kv.dtype)
        w_kv[2 + cc] = jnp.where(lane < HEAD, pltpu.roll(key, HEAD, 1), value).astype(w_kv.dtype)
    small_src[...] = jnp.zeros_like(small_src)
    for tt in range(planes):
        cols = slice(tt * width, (tt + 1) * width)
        small_src[tt, 0:KSIZE, :] = taps[:, cols].astype(f32)
        small_src[tt, 32:33, :] = conv_gain[:, cols]
        small_src[tt, 33:34, 0 : sink.shape[1]] = sink[...]
    pl.semaphore_wait(barrier, size)

    def rows_of(zz, tt, chunk):
        start = pl.multiple_of(zz * block + tt * piece + chunk * step, step)
        return rows_all.at[pl.ds(start, step)]

    def origin(way, distance):
        return z - distance if way == 0 else z + distance

    def chain(way, distance, chunk):
        ref = rows_of(origin(way, distance), t, chunk)
        index = (way * planes + distance) * A_CHUNKS + chunk
        return remote(ref, ref, a_sem, index, at(z + 1 if way == 0 else z - 1, y, t))

    def chain_arrival(way, distance, chunk):
        ref = rows_of(origin(way, distance), t, chunk)
        index = (way * planes + distance - 1) * A_CHUNKS + chunk
        return remote(ref, ref, a_sem, index, across_x)

    def can_send(way, distance):
        if way == 0:
            return jnp.logical_and(z - distance >= 0, z + 1 < planes)
        return jnp.logical_and(z + distance < planes, z - 1 >= 0)

    def exists(way, distance):
        return z - distance >= 0 if way == 0 else z + distance < planes

    def sideways(way, distance, chunk, arrival=False):
        ref = rows_of(origin(way, distance), tx if arrival else t, chunk)
        index = (way * planes + distance) * A_CHUNKS + chunk
        return remote(ref, ref, ax_sem, index, across_x)

    def to_partner(way, distance, chunk, far, arrival=False):
        tt = (td if far else tp) if arrival else (tx if far else t)
        ref = rows_of(origin(way, distance), tt, chunk)
        index = ((way * planes + distance) * A_CHUNKS + chunk) * 2 + far
        return remote(ref, ref, ac_sem, index, partner)

    def home(zz, yy):
        return pl.multiple_of((zz * 2 + yy) * depth, depth)

    fine, fine_kv = depth // W_CHUNKS, half // W_CHUNKS

    def pieces(ref, start, cc, j):
        low = pl.multiple_of(start + j * fine, fine)
        low_kv = pl.multiple_of(start + cc * half + j * fine_kv, fine_kv)
        return [
            ref.at[pl.ds(low, fine), pl.ds(0, three)],
            ref.at[pl.ds(low_kv, fine_kv), pl.ds(three, width)],
        ]

    def narrow(ref, start, cc):
        return ref.at[pl.ds(pl.multiple_of(start + cc * half, half), half), pl.ds(three, width)]

    def w_sources(tt):
        cols = pl.ds(pl.multiple_of(tt * width, width), width)
        return [w_query.at[:, cols], w_glu.at[:, cols], w_gate.at[:, cols], w_kv.at[tt]]

    def w_targets(ref, start, cc):
        here = pl.ds(start, depth)
        return [ref.at[here, pl.ds(g * width, width)] for g in range(3)] + [narrow(ref, start, cc)]

    def first_all(kind, target, tt, what):
        for here, ref, start in (
            (t == z, w_all, home(z, y)),
            (t != z, stage, pl.multiple_of(t * depth, depth)),
        ):
            @pl.when(here)
            def _():
                for i, (a, b) in enumerate(zip(w_sources(tt), w_targets(ref, start, tt % 2))):
                    what(remote(a, b, w1_sem, kind * 4 + i, target))

    def first_arrival(kind, src_t):
        for here, ref, start in (
            (src_t == z, w_all, home(z, y)),
            (src_t != z, stage, pl.multiple_of(src_t * depth, depth)),
        ):
            @pl.when(here)
            def _():
                for i, b in enumerate(w_targets(ref, start, c)):
                    remote(b, b, w1_sem, kind * 4 + i, across_x).wait_recv()

    def staged(src_t):
        return pl.multiple_of(src_t * depth, depth)

    def second(src_t, j):
        return [
            remote(a, b, w2_sem, (z * W_CHUNKS + j) * 2 + i, at(src_t, y, t), (src_t * W_CHUNKS + j) * 2 + i)
            for i, (a, b) in enumerate(
                zip(pieces(stage, staged(src_t), c, j), pieces(w_all, home(z, y), c, j))
            )
        ]

    def second_arrival(from_z, j):
        for i, ref in enumerate(pieces(w_all, home(from_z, y), c, j)):
            remote(ref, ref, w2_sem, (from_z * W_CHUNKS + j) * 2 + i, across_x).wait_recv()

    def third(from_z, j, i, arrival=False):
        ref = pieces(w_all, home(from_z, 1 - y if arrival else y), c, j)[i]
        return remote(ref, ref, w3_sem, (from_z * W_CHUNKS + j) * 2 + i, across_y)

    def to_share(from_z, own, arrival=False):
        ref = narrow(w_all, home(from_z, y if own else 1 - y), 1 - c if arrival else c)
        return remote(ref, ref, kc_sem, from_z * 2 + own, partner)

    def out_copies(yy):
        low = pl.multiple_of(yy * group, group)
        high = pl.multiple_of(part + yy * group, group)
        return [weights.at[pl.ds(low, group)], weights.at[pl.ds(high, group)]]

    outs = [
        remote(a, b, o_sem, i, across_y)
        for i, (a, b) in enumerate(zip((out_attn, out_conv), out_copies(y)))
    ]
    out_loads = [
        pltpu.make_async_copy(a, b, local_sem.at[4 + i])
        for i, (a, b) in enumerate(zip((out_attn, out_conv), out_copies(y)))
    ]

    def own_loads(ref, start):
        return [
            pltpu.make_async_copy(a, b, local_sem.at[i])
            for i, (a, b) in enumerate(zip(w_sources(t)[:3], w_targets(ref, start, c)))
        ]


    for chunk in range(A_CHUNKS):
        for way in range(2):
            @pl.when(can_send(way, 0))
            def _():
                chain(way, 0, chunk).start()
    small_to = [(partner, tp, 0), (across_x, tx, 1), (diagonal, td, 2)]

    def small_copy(target, tt, i):
        return pltpu.make_async_remote_copy(
            src_ref=small_src.at[tt],
            dst_ref=small,
            send_sem=small_sem[0].at[i],
            recv_sem=small_sem[1].at[0],
            device_id=target,
            device_id_type=MESH,
        )

    @pl.when(t == z)
    def _():
        for args in small_to:
            small_copy(*args).start()
        small[...] = small_src[t]

    for here, ref, start in ((t == z, w_all, home(z, y)), (t != z, stage, staged(t))):
        @pl.when(here)
        def _():
            for copy in own_loads(ref, start):
                copy.start()
            ref[pl.ds(pl.multiple_of(start + c * half, half), half), three : three + width] = w_kv[t]

    first_all(2, partner, tp, lambda copy: copy.start())
    first_all(0, across_x, tx, lambda copy: copy.start())
    first_all(1, diagonal, td, lambda copy: copy.start())
    for copy in outs + out_loads:
        copy.start()
    for here, ref, start in ((t == z, w_all, home(z, y)), (t != z, stage, staged(t))):
        @pl.when(here)
        def _():
            for copy in own_loads(ref, start):
                copy.wait()

    def toward(target, way):
        return target > z if way == 0 else target < z

    def next_to(target, way):
        return target == (z + 1 if way == 0 else z - 1)

    def send_second(way, sources, near):
        for j in range(W_CHUNKS):
            for src_t in sources:
                beside = next_to(src_t, way)
                beyond = jnp.logical_and(toward(src_t, way), jnp.logical_not(beside))

                @pl.when(beside if near else beyond)
                def _():
                    for copy in second(src_t, j):
                        copy.start()

    def chain_step(distance, chunks=range(A_CHUNKS)):
        for chunk in chunks:
            for way in range(2):
                @pl.when(exists(way, distance))
                def _():
                    chain_arrival(way, distance, chunk).wait_recv()

                    @pl.when(can_send(way, distance))
                    def _():
                        chain(way, distance, chunk).start()

                    sideways(way, distance, chunk).start()
                    to_partner(way, distance, chunk, 0).start()

    def sideways_step(distance):
        for chunk in range(A_CHUNKS):
            for way in range(2):
                @pl.when(exists(way, distance))
                def _():
                    sideways(way, distance, chunk, True).wait_recv()
                    to_partner(way, distance, chunk, 1).start()

    def settle(from_z, j):
        for i in range(2):
            third(from_z, j, i).start()
        if j == W_CHUNKS - 1:
            to_share(from_z, 1).start()

    def block_step(from_z, j):
        second_arrival(from_z, j)
        settle(from_z, j)

    ends = jnp.logical_or(z == 0, z == planes - 1)

    for k in range(1, planes):
        normalise(lax.rem(t + k, planes) * piece, piece)
    first_arrival(2, tp)
    chain_step(1)
    for way in range(2):
        send_second(way, (t, tp), True)

    first_arrival(0, tx)
    first_arrival(1, td)
    for way in range(2):
        send_second(way, (tx, td), True)
        send_second(way, (t, tp, tx, td), False)

    for j in range(W_CHUNKS):
        settle(z, j)
    for distance in range(2, planes - 1):
        chain_step(distance)

    row = lax.broadcasted_iota(jnp.int32, (block, LANES), 0)
    for zz in range(planes):
        angle = ((2 * zz + y) * block + row).astype(f32) * freq[...]
        here = slice(zz * block, (zz + 1) * block)
        cosine[here, :] = jnp.cos(angle)
        sine[here, :] = jnp.sin(angle)

    ahead = 1 - 2 * (z // (planes // 2))
    end = (z // (planes // 2)) * (planes - 1)
    middle = jnp.logical_not(ends)

    blocks_from = [
        z,
        jnp.where(middle, end, z + ahead),
        jnp.where(middle, planes - 1 - z, z + 2 * ahead),
        jnp.where(middle, planes - 1 - end, z + 3 * ahead),
    ]

    def tokens_here(distance):
        for chunk in range(A_CHUNKS):
            for way in range(2):
                @pl.when(exists(way, distance))
                def _():
                    for far in range(2):
                        to_partner(way, distance, chunk, far, True).wait_recv()

    first_row = (z // (planes // 2)) * block
    last_row = (planes - 1) * block - end * block

    def multiply(from_z, yy, fresh):
        cols = pl.ds(home(from_z, yy), depth)

        @pl.loop(0, planes - 1)
        def _(i):
            here = pl.ds(pl.multiple_of(first_row + i * block, block), block)
            value = jnp.dot(rows_all[here, cols], w_all[cols, :], preferred_element_type=f32)
            if fresh:
                acc[here, :] = value
            else:
                acc[here, :] += value

    def multiply_own(pair):
        for k in pair:
            to_share(blocks_from[k], 1, True).wait_recv()
            if k == 0:
                multiply(blocks_from[0], y, True)
        if 0 not in pair:
            multiply(blocks_from[pair[0]], y, False)
        multiply(blocks_from[pair[1]], y, False)

    def share_other(pair):
        for k in pair:
            for j in range(W_CHUNKS):
                third(blocks_from[k], j, 1, True).wait_recv()
            to_share(blocks_from[k], 0).start()

    def multiply_other(pair):
        for k in pair:
            for j in range(W_CHUNKS):
                third(blocks_from[k], j, 0, True).wait_recv()
            to_share(blocks_from[k], 0, True).wait_recv()

        @pl.loop(0, 2)
        def _(i):
            multiply(jnp.where(i == 0, blocks_from[pair[0]], blocks_from[pair[1]]), 1 - y, False)

    for j in range(W_CHUNKS):
        block_step(blocks_from[1], j)
    sideways_step(1)
    for j in range(W_CHUNKS):
        block_step(blocks_from[2], j)
        block_step(blocks_from[3], j)
        if j == 1:
            sideways_step(2)
        if j == 2:
            chain_step(planes - 1, range(A_CHUNKS // 4))
            share_other((0, 1))
            for distance in range(1, planes - 1):
                tokens_here(distance)
            multiply_own((0, 1))
            multiply_other((0, 1))
            chain_step(planes - 1, range(A_CHUNKS // 4, A_CHUNKS // 2))
    chain_step(planes - 1, range(A_CHUNKS // 2, A_CHUNKS))
    multiply_own((2, 3))
    share_other((2, 3))
    sideways_step(planes - 1)
    multiply_other((2, 3))

    tokens_here(planes - 1)
    here = pl.ds(pl.multiple_of(last_row, block), block)

    @pl.loop(0, 2)
    def _(i):
        cols = pl.ds(pl.multiple_of(i * 2 * width, 2 * width), 2 * width)
        acc[here, cols] = jnp.dot(rows_all[here, :], w_all[:, cols], preferred_element_type=f32)

    lane = lax.broadcasted_iota(jnp.int32, (block, LANES), 1)
    low = lax.rem(lane, HEAD) < HEAD // 2

    def turned(value, here):
        other = jnp.where(low, -pltpu.roll(value, LANES - HEAD // 2, 1), pltpu.roll(value, HEAD // 2, 1))
        return value * cosine[here, :] + other * sine[here, :]

    def halo(kind, zz):
        if kind == 0:
            ref = kv_b.at[pl.ds((zz + 1) * block - WINDOW, WINDOW)]
            return remote(ref, kv_rim.at[zz + y], halo_sem, zz, across_y)
        ref = gated.at[pl.ds((zz + 1) * block - 32, 32)]
        return remote(ref, gated_rim.at[zz + y], halo_sem, planes + zz, across_y)

    def halo_arrival(kind, zz):
        ref = (kv_rim if kind == 0 else gated_rim).at[zz + 1 - y]
        return remote(ref, ref, halo_sem, kind * planes + zz, across_y)

    for zz in range(planes):
        here = slice(zz * block, (zz + 1) * block)
        value = acc[here, three:]
        kv_b[here, :] = jnp.where(lane < HEAD, turned(value, here), value).astype(kv_b.dtype)
        halo(0, zz).start()
    for zz in range(planes):
        here = slice(zz * block, (zz + 1) * block)
        gate = acc[here, 2 * width : three]
        value = (acc[here, width : 2 * width] * (1.0 / (1.0 + jnp.exp(-gate)))).astype(gated.dtype)
        gated[here, :] = value
        extended[zz, 32:, :] = value.astype(f32)
        halo(1, zz).start()

    @pl.when(y == 0)
    def _():
        kv_rim[0] = jnp.zeros_like(kv_rim[0])
        gated_rim[0] = jnp.zeros_like(gated_rim[0])

    for zz in range(planes):
        here = slice(zz * block, (zz + 1) * block)
        q_b[here, :] = (turned(acc[here, :width], here) * (1.0 / math.sqrt(HEAD))).astype(q_b.dtype)

    @pl.when(t != z)
    def _():
        small_copy(partner, tp, 0).wait_recv()

    lane_q = lax.broadcasted_iota(jnp.int32, (WINDOW, LANES), 1)
    lane_k = lax.broadcasted_iota(jnp.int32, (2 * WINDOW, LANES), 1)
    row_s = lax.rem(lax.broadcasted_iota(jnp.int32, (heads * WINDOW, 2 * WINDOW), 0), WINDOW)
    col_s = lax.broadcasted_iota(jnp.int32, (heads * WINDOW, 2 * WINDOW), 1)
    distance_s = row_s + WINDOW - col_s
    inside = jnp.logical_and(distance_s >= 0, distance_s < WINDOW)
    sink_row = small[33:34, :]
    lane_1 = lax.broadcasted_iota(jnp.int32, (1, LANES), 1)
    sinks = [
        jnp.sum(jnp.where(lane_1 == t * heads + h, sink_row, 0.0), axis=1, keepdims=True)
        for h in range(heads)
    ]
    sink_col = jnp.concatenate([jnp.broadcast_to(v, (WINDOW, 1)) for v in sinks], axis=0)

    def attend(first_row, keys, mask):
        query = q_b[pl.ds(first_row, WINDOW), :]
        keys_f = keys.astype(f32)
        swapped = pltpu.roll(keys_f, HEAD, 1)
        key_two = jnp.where(lane_k < HEAD, keys_f, swapped).astype(jnp.bfloat16)
        value_two = jnp.where(lane_k < HEAD, swapped, keys_f).astype(jnp.bfloat16)
        zero = jnp.zeros_like(query)
        stacked = jnp.concatenate(
            [jnp.where(lane_q // HEAD == h, query, zero) for h in range(heads)], axis=0
        )
        scores = lax.dot_general(
            stacked, key_two, (((1,), (1,)), ((), ())), preferred_element_type=f32
        )
        scores = jnp.where(mask, scores, -1e30)
        top = jnp.maximum(jnp.max(scores, axis=1, keepdims=True), sink_col)
        grown = jnp.exp(scores - top)
        total = jnp.sum(grown, axis=1, keepdims=True) + jnp.exp(sink_col - top)
        probs = (grown / total).astype(jnp.bfloat16)
        mixed_values = jnp.dot(probs, value_two, preferred_element_type=f32)
        result = mixed_values[:WINDOW]
        for h in range(1, heads):
            result = jnp.where(lane_q // HEAD == h, mixed_values[h * WINDOW : (h + 1) * WINDOW], result)
        act[pl.ds(first_row, WINDOW), columns(0, t)] = result.astype(act.dtype)

    def columns(kind, tt):
        return pl.ds(pl.multiple_of(kind * part + tt * width, width), width)

    blocks = block // WINDOW

    @pl.loop(0, planes)
    def _(zz):
        for b in range(1, blocks):
            start = pl.multiple_of(zz * block + b * WINDOW, WINDOW)
            before = pl.multiple_of(zz * block + (b - 1) * WINDOW, WINDOW)
            attend(start, kv_b[pl.ds(before, 2 * WINDOW), :], inside)

    def attend_first(zz):
        start = pl.multiple_of(zz * block, block)
        keys = jnp.concatenate([kv_rim[zz], kv_b[pl.ds(start, WINDOW), :]], axis=0)
        began = jnp.logical_or(zz * 2 + y > 0, col_s >= WINDOW)
        attend(start, keys, jnp.logical_and(inside, began))

    for zz in range(planes):
        if zz < planes - 1:
            halo_arrival(1, zz).wait_recv()

        @pl.when(y == 1)
        def _():
            if zz == planes - 1:
                halo_arrival(1, zz).wait_recv()

    for zz in range(planes):
        extended[zz, 0:32, :] = gated_rim[zz].astype(f32)
    strip = 64

    @pl.loop(0, planes)
    def _(zz):
        @pl.loop(0, block // strip)
        def _(i):
            base = pl.multiple_of(i * strip, strip)
            window = extended[zz, pl.ds(base, strip + 32), :]
            total = window[2 : 2 + strip] * small[0:1, :]
            for k in range(1, KSIZE):
                total = total + window[2 + k : 2 + k + strip] * small[k : k + 1, :]
            filtered[pl.ds(pl.multiple_of(zz * block + base, strip), strip), :] = total

    tiles = rows // LANES
    for k in range(tiles):
        value = filtered[k * LANES : (k + 1) * LANES, :]
        total = jnp.sum(value, axis=1, keepdims=True)
        square = jnp.sum(value * value, axis=1, keepdims=True)
        stats[k : k + 1, :] = jnp.transpose(jnp.broadcast_to(total, (LANES, LANES)))[0:1]
        stats[tiles + k : tiles + k + 1, :] = jnp.transpose(jnp.broadcast_to(square, (LANES, LANES)))[0:1]

    def stat(k):
        g = peers[k]
        return pltpu.make_async_remote_copy(
            src_ref=stats,
            dst_ref=stats_all.at[mine],
            send_sem=s_sem[0].at[k],
            recv_sem=s_sem[1].at[mine],
            device_id=at(g // planes, y, g % planes),
            device_id_type=MESH,
        )

    for k in range(size - 1):
        stat(k).start()
    stats_all[mine] = stats[...]

    for zz in range(planes):
        if zz < planes - 1:
            halo_arrival(0, zz).wait_recv()

        @pl.when(y == 1)
        def _():
            if zz == planes - 1:
                halo_arrival(0, zz).wait_recv()

    def region(kind, r, tt):
        start = pl.multiple_of(r * block, block)
        return act.at[pl.ds(start, block), columns(kind, tt)]

    def cross(kind, r, arrival=False):
        ref = region(kind, r, tx if arrival else t)
        return remote(ref, ref, x_sem, kind * planes + r, across_x)

    def hand(kind, r, far, arrival=False):
        tt = (td if far else tp) if arrival else (tx if far else t)
        ref = region(kind, r, tt)
        return remote(ref, ref, c_sem, (kind * planes + r) * 2 + far, partner)

    near = z // (planes // 2)
    order = [(1 - near) * (planes - 1 - j) + near * j for j in range(planes)]
    def send_out(kind, r):
        cross(kind, r).start()
        hand(kind, r, 0).start()

    for r in order:
        attend_first(r)
        if r is order[0]:
            send_out(0, r)
    for g in peers:
        ref = stats_all.at[g]
        pltpu.make_async_remote_copy(
            src_ref=ref,
            dst_ref=ref,
            send_sem=s_sem[0].at[0],
            recv_sem=s_sem[1].at[g],
            device_id=partner,
            device_id_type=MESH,
        ).wait_recv()
    total = stats_all[0]
    for g in range(1, size):
        total = total + stats_all[g]
    mean = total[:tiles] / channels
    variance = total[tiles:] / channels - mean * mean
    moments[0] = mean
    moments[1] = lax.rsqrt(variance + 1e-05)
    per = block // LANES

    def normed_out(r):
        for k in range(per):
            tile = r * per + k
            mean_col = jnp.transpose(jnp.broadcast_to(moments[0, pl.ds(tile, 1), :], (LANES, LANES)))
            rate_col = jnp.transpose(jnp.broadcast_to(moments[1, pl.ds(tile, 1), :], (LANES, LANES)))
            here = pl.ds(pl.multiple_of(tile * LANES, LANES), LANES)
            scaled = (filtered[here, :] - mean_col) * rate_col * small[32:33, :]
            act[here, columns(1, t)] = (scaled / (1.0 + jnp.exp(-scaled))).astype(act.dtype)

    out_step = block // OUT_CHUNKS
    columns_out = mixed.shape[1]
    tile_out = min(256, columns_out)

    def partial(r, h, tile):
        start = pl.multiple_of(r * block + h * out_step, out_step)
        cols = pl.ds(pl.multiple_of(tile * tile_out, tile_out), tile_out)
        value = jnp.dot(act[pl.ds(start, out_step), :], weights[:, cols], preferred_element_type=f32)
        return value, cols

    def travel(way, r, h, arrival=False):
        rows_h = pl.ds(h * out_step, out_step)
        into = (in_up if way == 0 else in_down).at[r, rows_h]
        index = (way * planes + r) * OUT_CHUNKS + h
        source = into if arrival else outgoing.at[r, rows_h]
        return remote(source, into, r_sem, index, across_y if arrival else at(z + 1 if way == 0 else z - 1, y, t))

    def pass_sums(distance):
        for h in range(OUT_CHUNKS):
            rows_h = pl.ds(h * out_step, out_step)
            for way in range(2):
                r = z + distance if way == 0 else z - distance
                there = r < planes if way == 0 else r >= 0
                more = z > 0 if way == 0 else z < planes - 1
                into = in_up if way == 0 else in_down

                @pl.when(jnp.logical_and(there, jnp.logical_not(more)))
                def _():
                    @pl.loop(0, columns_out // tile_out)
                    def _(tile):
                        value, cols = partial(r, h, tile)
                        outgoing[r, rows_h, cols] = value.astype(outgoing.dtype)

                    travel(way, r, h).start()

                @pl.when(jnp.logical_and(there, more))
                def _():
                    travel(way, r, h, True).wait_recv()

                    @pl.loop(0, columns_out // tile_out)
                    def _(tile):
                        value, cols = partial(r, h, tile)
                        outgoing[r, rows_h, cols] = (value + into[r, rows_h, cols].astype(f32)).astype(
                            outgoing.dtype
                        )

                    travel(way, r, h).start()

    def gathered(js):
        for j in js:
            for kind in range(2):
                cross(kind, order[j], True).wait_recv()
                hand(kind, order[j], 1).start()
        for j in js:
            for kind in range(2):
                for far in range(2):
                    hand(kind, order[j], far, True).wait_recv()

    for r in order:
        normed_out(r)
        send_out(1, r)
        if r is not order[0]:
            send_out(0, r)
    for copy in out_loads:
        copy.wait()
    for copy in outs:
        copy.wait_recv()
    gathered([0])
    pass_sums(planes - 1)
    gathered(range(1, planes))
    for distance in range(planes - 2, 0, -1):
        pass_sums(distance)

    for h in range(OUT_CHUNKS):
        rows_h = pl.ds(h * out_step, out_step)

        @pl.when(z > 0)
        def _():
            travel(0, z, h, True).wait_recv()

        @pl.when(z < planes - 1)
        def _():
            travel(1, z, h, True).wait_recv()

        @pl.loop(0, columns_out // tile_out)
        def _(tile):
            value, cols = partial(z, h, tile)
            below = in_up[z, rows_h, cols].astype(f32)
            above = in_down[z, rows_h, cols].astype(f32)
            value = value + jnp.where(z > 0, below, 0.0) + jnp.where(z < planes - 1, above, 0.0)
            mixed[rows_h, cols] = value.astype(mixed.dtype)

    @pl.when(t == z)
    def _():
        for args in small_to:
            small_copy(*args).wait_send()

    @pl.when(y == 0)
    def _():
        for kind in range(2):
            halo(kind, planes - 1).wait_send()

    @pl.when(y == 1)
    def _():
        for kind in range(2):
            halo(kind, planes - 1).wait_send()

    for zz in range(planes - 1):
        for kind in range(2):
            halo(kind, zz).wait_send()

    @pl.when(y == 0)
    def _():
        for kind in range(2):
            halo_arrival(kind, planes - 1).wait_recv()

    for copy in outs:
        copy.wait_send()
    first_all(2, partner, tp, lambda copy: copy.wait_send())
    first_all(0, across_x, tx, lambda copy: copy.wait_send())
    first_all(1, diagonal, td, lambda copy: copy.wait_send())

    for src_t in (t, tp, tx, td):
        @pl.when(src_t != z)
        def _():
            for j in range(W_CHUNKS):
                for copy in second(src_t, j):
                    copy.wait_send()

    for zz in range(planes):
        for j in range(W_CHUNKS):
            for i in range(2):
                third(zz, j, i).wait_send()
        for own in range(2):
            to_share(zz, own).wait_send()
    for distance in range(planes):
        for chunk in range(A_CHUNKS):
            for way in range(2):
                @pl.when(can_send(way, distance))
                def _():
                    chain(way, distance, chunk).wait_send()

                if distance:
                    @pl.when(exists(way, distance))
                    def _():
                        sideways(way, distance, chunk).wait_send()
                        for far in range(2):
                            to_partner(way, distance, chunk, far).wait_send()
    for k in range(size - 1):
        stat(k).wait_send()
    for kind in range(2):
        for r in order:
            cross(kind, r).wait_send()
            for far in range(2):
                hand(kind, r, far).wait_send()
    for distance in range(1, planes):
        for h in range(OUT_CHUNKS):
            for way in range(2):
                r = z + distance if way == 0 else z - distance

                @pl.when(r < planes if way == 0 else r >= 0)
                def _():
                    travel(way, r, h).wait_send()


def planned_per_device(
    tokens,
    norm_gain,
    w_query,
    w_key,
    w_value,
    w_glu,
    w_gate,
    sink_logit,
    conv_taps,
    conv_gain,
    out_attn,
    out_conv,
):
    planes = lax.axis_size("tp")
    block, model = tokens.shape
    rows = planes * block
    depth, cols = w_query.shape
    width = cols // planes
    columns_out = out_attn.shape[1]
    size = planes * planes
    half_width = HEAD // 2
    freq = 10000.0 ** (-jnp.arange(half_width, dtype=jnp.float32) * 2.0 / HEAD)
    freq = jnp.tile(freq, LANES // half_width)[None]
    vmem = pl.BlockSpec(memory_space=pltpu.VMEM)
    any_spec = pl.BlockSpec(memory_space=pl.ANY)
    dma = pltpu.SemaphoreType.DMA
    bf16, f32 = jnp.bfloat16, jnp.float32
    tiles = rows // LANES
    chunks = 2 * planes * A_CHUNKS
    counts = [
        chunks, chunks, 2 * chunks, 12, 2 * planes * W_CHUNKS, 2 * planes * W_CHUNKS, 2 * planes, 2, 3,
        2 * planes, size, 2 * planes, 4 * planes, 2 * planes * OUT_CHUNKS,
    ]
    sems = [dma((n,)) for n in counts for _ in range(2)]
    return pl.pallas_call(
        functools.partial(layer_kernel, planes, CONV),
        out_shape=jax.ShapeDtypeStruct((block, columns_out), bf16),
        in_specs=[vmem] * 8 + [any_spec] * 5,
        out_specs=vmem,
        scratch_shapes=[
            pltpu.VMEM((rows, model), bf16),
            pltpu.VMEM((2 * planes * depth, 4 * width), bf16),
            pltpu.VMEM((planes * depth, 4 * width), bf16),
            pltpu.VMEM((planes, depth // 2, 2 * HEAD), bf16),
            pltpu.VMEM((planes, 40, width), f32),
            pltpu.VMEM((40, width), f32),
            pltpu.VMEM((rows, 4 * width), f32),
            pltpu.VMEM((rows, LANES), f32),
            pltpu.VMEM((rows, LANES), f32),
            pltpu.VMEM((rows, width), bf16),
            pltpu.VMEM((rows, width), bf16),
            pltpu.VMEM((planes + 1, WINDOW, width), bf16),
            pltpu.VMEM((rows, width), bf16),
            pltpu.VMEM((planes + 1, 32, width), bf16),
            pltpu.VMEM((planes, 32 + block, width), f32),
            pltpu.VMEM((rows, width), f32),
            pltpu.VMEM((rows, 2 * planes * width), bf16),
            pltpu.VMEM((2 * planes * width, columns_out), bf16),
            pltpu.VMEM((2 * tiles, LANES), f32),
            pltpu.VMEM((size, 2 * tiles, LANES), f32),
            pltpu.VMEM((2, tiles, LANES), f32),
            pltpu.VMEM((planes, block, columns_out), bf16),
            pltpu.VMEM((planes, block, columns_out), bf16),
            pltpu.VMEM((planes, block, columns_out), bf16),
            dma((8,)),
        ]
        + sems,
        compiler_params=pltpu.CompilerParams(
            collective_id=0, has_side_effects=True, vmem_limit_bytes=60 * 2**20
        ),
    )(
        tokens,
        norm_gain[None],
        freq,
        w_key,
        w_value,
        conv_taps,
        conv_gain[None],
        sink_logit[None],
        w_query,
        w_glu,
        w_gate,
        out_attn,
        out_conv,
    )


def solution(mesh):
    planes, others = mesh.shape["tp"], mesh.shape["sp"]
    fits = others == 2 * planes and planes % 2 == 0 and HEADS == 2 * planes * planes
    return jax.shard_map(
        planned_per_device if fits else gathered_per_device,
        mesh=mesh,
        in_specs=(
            P("sp", None),
            P(),
            P("sp", "tp"),
            P("sp", "tp"),
            P("sp", "tp"),
            P("sp", "tp"),
            P("sp", "tp"),
            P("tp"),
            P(None, "tp"),
            P("tp"),
            P("sp", "tp"),
            P("sp", "tp"),
        ),
        out_specs=P("sp", "tp"),
        check_vma=False,
    )
```

```python
import functools
import math

import jax
import jax.numpy as jnp
from jax import lax
from jax.experimental import pallas as pl
from jax.experimental.pallas import tpu as pltpu
from jax.sharding import PartitionSpec as P

HEADS = 32
HEAD = 64
KV = 8
CONV = 2048
KSIZE = 31
WINDOW = 128


def passed_along(block, axis, distance):
    devices = range(lax.axis_size(axis))
    route = [(i - distance, i) for i in devices if i - distance in devices]
    return lax.ppermute(block, axis, route)


def rotate_heads(values, positions):
    half_width = values.shape[-1] // 2
    frequency = 10000.0 ** (-jnp.arange(half_width, dtype=jnp.float32) * 2.0 / values.shape[-1])
    angles = positions.astype(jnp.float32)[:, None] * frequency[None, :]
    cosine = jnp.cos(angles)[:, None, :]
    sine_part = jnp.sin(angles)[:, None, :]
    first_half = values[..., :half_width]
    second_half = values[..., half_width:]
    return jnp.concatenate(
        [
            first_half * cosine - second_half * sine_part,
            second_half * cosine + first_half * sine_part,
        ],
        axis=-1,
    )


def ring_gather_kernel(n, count, *refs):
    shards, wholes = refs[:count], refs[count : 2 * count]
    bounce = refs[2 * count : 3 * count]
    in_sem, out_sem, send_sem, recv_sem = refs[3 * count :]
    me = lax.axis_index("sp")
    half = n // 2
    odd = lax.rem(me, 2)
    place = (1 - odd) * lax.div(me, 2) + odd * (n - 1 - lax.div(me, 2))

    def device_at(position):
        spot = lax.rem(position + 2 * n, n)
        back = lax.div(spot, half)
        return (1 - back) * 2 * spot + back * (2 * (n - 1 - spot) + 1)

    ahead, behind = device_at(place + 1), device_at(place - 1)
    barrier = pltpu.get_barrier_semaphore()
    for neighbour in (ahead, behind):
        pl.semaphore_signal(
            barrier, inc=1, device_id={"sp": neighbour}, device_id_type=pl.DeviceIdType.MESH
        )
    pl.semaphore_wait(barrier, 2)

    def block(array, owner, way):
        rows = shards[array].shape[0]
        part = rows // 2
        start = pl.multiple_of(owner * rows + way * part, part)
        return wholes[array].at[pl.ds(start, part)]

    def hop(array, step, way):
        owner = device_at(place - step) if way == 0 else device_at(place + step)
        part = shards[array].shape[0] // 2
        target = block(array, owner, way)
        source = shards[array].at[pl.ds(way * part, part)] if step == 0 else target
        return pltpu.make_async_remote_copy(
            src_ref=source,
            dst_ref=target,
            send_sem=send_sem.at[way, step, array],
            recv_sem=recv_sem.at[way, step, array],
            device_id={"sp": ahead if way == 0 else behind},
            device_id_type=pl.DeviceIdType.MESH,
        )

    def arrival(array, step, way):
        owner = device_at(place - step - 1) if way == 0 else device_at(place + step + 1)
        target = block(array, owner, way)
        return pltpu.make_async_remote_copy(
            src_ref=target,
            dst_ref=target,
            send_sem=send_sem.at[way, step, array],
            recv_sem=recv_sem.at[way, step, array],
            device_id={"sp": ahead if way == 0 else behind},
            device_id_type=pl.DeviceIdType.MESH,
        )

    for array in range(count):
        for way in range(2):
            hop(array, 0, way).start()
    loads = [
        pltpu.make_async_copy(shards[a], bounce[a], in_sem.at[a]) for a in range(count)
    ]
    for load in loads:
        load.start()
    stores = []
    for a in range(count):
        loads[a].wait()
        rows = shards[a].shape[0]
        mine = wholes[a].at[pl.ds(pl.multiple_of(me * rows, rows), rows)]
        stores.append(pltpu.make_async_copy(bounce[a], mine, out_sem.at[a]))
        stores[a].start()
    for step in range(1, n - 1):
        for array in range(count):
            for way in range(2):
                arrival(array, step - 1, way).wait_recv()
                hop(array, step, way).start()
    for array in range(count):
        for way in range(2):
            arrival(array, n - 2, way).wait_recv()
    for step in range(n - 1):
        for array in range(count):
            for way in range(2):
                hop(array, step, way).wait_send()
    for store in stores:
        store.wait()


def ring_gather(arrays, collective_id):
    n = lax.axis_size("sp")
    count = len(arrays)
    return pl.pallas_call(
        functools.partial(ring_gather_kernel, n, count),
        out_shape=[
            jax.ShapeDtypeStruct((n * a.shape[0],) + a.shape[1:], a.dtype) for a in arrays
        ],
        in_specs=[pl.BlockSpec(memory_space=pl.ANY)] * count,
        out_specs=[pl.BlockSpec(memory_space=pl.ANY)] * count,
        scratch_shapes=[pltpu.VMEM(a.shape, a.dtype) for a in arrays]
        + [
            pltpu.SemaphoreType.DMA((count,)),
            pltpu.SemaphoreType.DMA((count,)),
            pltpu.SemaphoreType.DMA((2, n - 1, count)),
            pltpu.SemaphoreType.DMA((2, n - 1, count)),
        ],
        compiler_params=pltpu.CompilerParams(
            collective_id=collective_id, has_side_effects=True
        ),
    )(*arrays)


def gathered_per_device(
    tokens,
    norm_gain,
    w_query,
    w_key,
    w_value,
    w_glu,
    w_gate,
    sink_logit,
    conv_taps,
    conv_gain,
    out_attn,
    out_conv,
):
    row_count = tokens.shape[0]
    offset_rows = lax.axis_index("sp") * row_count
    positions = offset_rows + jnp.arange(row_count, dtype=jnp.int32)
    tokens_f = tokens.astype(jnp.float32)
    normed = (
        tokens_f
        * lax.rsqrt(jnp.mean(tokens_f * tokens_f, axis=1, keepdims=True) + 1e-06)
        * norm_gain
    ).astype(jnp.bfloat16)
    local_heads = w_query.shape[1] // HEAD
    local_kv = w_key.shape[1] // HEAD
    group_size = HEADS // KV
    kv_width = local_kv * HEAD
    *pieces, attn_rows, conv_rows = ring_gather(
        (w_query, w_key, w_value, w_glu, w_gate, out_attn, out_conv), 0
    )
    query_acc, key_acc, value_acc, glu_acc, gate_acc = tuple(
        (
            jnp.dot(normed, weight_piece, preferred_element_type=jnp.float32)
            for weight_piece in pieces
        )
    )
    queries = rotate_heads(query_acc.reshape(row_count, local_heads, HEAD), positions).astype(
        jnp.bfloat16
    )
    keys_rot = rotate_heads(key_acc.reshape(row_count, local_kv, HEAD), positions).astype(
        jnp.bfloat16
    )
    keys_rot = keys_rot.reshape(row_count, kv_width)
    values_bf = value_acc.astype(jnp.bfloat16)
    kv_tail = jnp.concatenate(
        [keys_rot[row_count - WINDOW :], values_bf[row_count - WINDOW :]], axis=1
    )
    kv_rim = passed_along(kv_tail, "sp", 1)
    gated = (glu_acc * jax.nn.sigmoid(gate_acc)).astype(jnp.bfloat16)
    conv_tail = gated[row_count - (KSIZE - 1) :]
    conv_rim = passed_along(conv_tail, "sp", 1)
    block_count = row_count // WINDOW
    keys_all = jnp.concatenate([kv_rim[:, :kv_width], keys_rot], axis=0).reshape(
        block_count + 1, WINDOW, local_kv, HEAD
    )
    vals_all = jnp.concatenate([kv_rim[:, kv_width:], values_bf], axis=0).reshape(
        block_count + 1, WINDOW, local_kv, HEAD
    )
    key_blocks = jnp.concatenate([keys_all[:-1], keys_all[1:]], axis=1)
    value_blocks = jnp.concatenate([vals_all[:-1], vals_all[1:]], axis=1)
    query_block_rows = queries.reshape(block_count, WINDOW, local_kv, group_size, HEAD)
    score_matrix = jnp.einsum(
        "bqhgd,bkhd->bhgqk", query_block_rows, key_blocks, preferred_element_type=jnp.float32
    ) * (1.0 / math.sqrt(HEAD))
    block_ids = jnp.arange(block_count, dtype=jnp.int32)[:, None, None]
    query_pos = (
        offset_rows + block_ids * WINDOW + jnp.arange(WINDOW, dtype=jnp.int32)[None, :, None]
    )
    key_pos = (
        offset_rows
        + (block_ids - 1) * WINDOW
        + jnp.arange(2 * WINDOW, dtype=jnp.int32)[None, None, :]
    )
    distance = query_pos - key_pos
    allowed = (distance >= 0) & (distance < WINDOW) & (key_pos >= 0)
    score_matrix = jnp.where(allowed[:, None, None], score_matrix, -1e30)
    sink_local = sink_logit.reshape(local_kv, group_size)[None, :, :, None, None]
    highest = jnp.maximum(jnp.max(score_matrix, axis=-1, keepdims=True), sink_local)
    weights_exp = jnp.exp(score_matrix - highest)
    denom_total = jnp.sum(weights_exp, axis=-1, keepdims=True) + jnp.exp(sink_local - highest)
    weights_bfloat_half = (weights_exp / denom_total).astype(jnp.bfloat16)
    attended_values = jnp.einsum(
        "bhgqk,bkhd->bqhgd", weights_bfloat_half, value_blocks, preferred_element_type=jnp.float32
    ).astype(jnp.bfloat16)
    attended_values = attended_values.reshape(row_count, local_heads * HEAD)
    extended = jnp.concatenate([conv_rim, gated], axis=0).astype(jnp.float32)
    filtered = lax.conv_general_dilated(
        extended[None],
        conv_taps.astype(jnp.float32)[:, None, :],
        (1,),
        "VALID",
        dimension_numbers=("NWC", "WIO", "NWC"),
        feature_group_count=extended.shape[1],
        precision=lax.Precision.HIGHEST,
    )[0]
    channel_sum, channel_square = lax.psum(
        (jnp.sum(filtered, axis=1), jnp.sum(filtered * filtered, axis=1)), "tp"
    )
    mean_value = channel_sum / CONV
    variance = channel_square / CONV - mean_value * mean_value
    scaled = (filtered - mean_value[:, None]) * lax.rsqrt(variance + 1e-05)[:, None] * conv_gain
    conv_out = jax.nn.silu(scaled).astype(jnp.bfloat16)
    pieces = (
        lax.all_gather(attended_values, "tp", axis=1, tiled=True),
        lax.all_gather(conv_out, "tp", axis=1, tiled=True),
    )
    mixed = jnp.dot(pieces[0], attn_rows, preferred_element_type=jnp.float32) + jnp.dot(
        pieces[1], conv_rows, preferred_element_type=jnp.float32
    )
    return mixed.astype(jnp.bfloat16)


MESH = pl.DeviceIdType.MESH
A_CHUNKS = 4
W_CHUNKS = 4
OUT_CHUNKS = 4
LANES = 128


def remote(src, dst, sems, index, target):
    send_sem, recv_sem = sems
    return pltpu.make_async_remote_copy(
        src_ref=src,
        dst_ref=dst,
        send_sem=send_sem.at[0],
        recv_sem=recv_sem.at[index],
        device_id=target,
        device_id_type=MESH,
    )


def all_sent(ref, sems, target):
    remote(ref, ref, sems, 0, target).wait_send()


def all_here(ref, sems, index, target):
    remote(ref, ref, sems, index, target).wait_recv()


def layer_kernel(planes, channels, *refs):
    (tokens, norm_gain, freq, w_key, w_value, taps, conv_gain, sink) = refs[:8]
    (w_query, w_glu, w_gate, out_attn, out_conv) = refs[8:13]
    mixed = refs[13]
    (rows_all, w_all, stage, w_kv, small_src, small) = refs[14:20]
    (acc, cosine, sine, q_b, kv_b, kv_rim, gated, gated_rim, extended, filtered) = refs[20:30]
    (act, weights, stats, stats_all, moments, incoming, outgoing) = refs[30:37]
    local_sem = refs[37]
    pairs = [(refs[38 + 2 * i], refs[39 + 2 * i]) for i in range((len(refs) - 38) // 2)]
    (a_sem, ax_sem, ac_sem, w1_sem, w2_sem, w3_sem, kc_sem, o_sem, small_sem) = pairs[:9]
    (halo_sem, s_sem, e_sem, x_sem, c_sem, r_sem) = pairs[9:15]

    s, t = lax.axis_index("sp"), lax.axis_index("tp")
    z, y, x, c = s // 2, s % 2, t // 2, t % 2
    block = tokens.shape[0]
    rows = planes * block
    piece = block // planes
    step = piece // A_CHUNKS
    depth = w_query.shape[0]
    width = w_query.shape[1] // planes
    three = 3 * width
    half = depth // 2
    heads = width // HEAD
    group = out_attn.shape[0]
    part = planes * width
    size = planes * planes
    f32 = jnp.float32

    def at(zz, yy, tt):
        return {"sp": zz * 2 + yy, "tp": tt}

    tx, td, tp = (1 - x) * 2 + c, (1 - x) * 2 + (1 - c), x * 2 + (1 - c)
    across_y, across_x = at(z, 1 - y, t), at(z, y, tx)
    diagonal, partner = at(z, y, td), at(z, y, tp)
    mine = z * planes + t
    peers = [lax.rem(mine + k, size) for k in range(1, size)]

    barrier = pltpu.get_barrier_semaphore()
    for target in [across_y] + [at(g // planes, y, g % planes) for g in peers]:
        pl.semaphore_signal(barrier, inc=1, device_id=target, device_id_type=MESH)

    def normalise(start, count):
        @pl.loop(0, count // 16)
        def _(i):
            here = pl.multiple_of(start + i * 16, 16)
            value = tokens[pl.ds(here, 16), :].astype(f32)
            scale = lax.rsqrt(jnp.mean(value * value, axis=1, keepdims=True) + 1e-06)
            there = pl.multiple_of(z * block + here, 16)
            rows_all[pl.ds(there, 16), :] = (value * scale * norm_gain[...]).astype(rows_all.dtype)

    normalise(t * piece, piece)

    lane = lax.broadcasted_iota(jnp.int32, (half, 2 * HEAD), 1)
    for cc in range(2):
        key = w_key[cc * half : (cc + 1) * half, :].astype(f32)
        value = w_value[cc * half : (cc + 1) * half, :].astype(f32)
        w_kv[cc] = jnp.where(lane < HEAD, key, pltpu.roll(value, HEAD, 1)).astype(w_kv.dtype)
        w_kv[2 + cc] = jnp.where(lane < HEAD, pltpu.roll(key, HEAD, 1), value).astype(w_kv.dtype)
    small_src[...] = jnp.zeros_like(small_src)
    for tt in range(planes):
        cols = slice(tt * width, (tt + 1) * width)
        small_src[tt, 0:KSIZE, :] = taps[:, cols].astype(f32)
        small_src[tt, 32:33, :] = conv_gain[:, cols]
        small_src[tt, 33:34, 0 : sink.shape[1]] = sink[...]
    pl.semaphore_wait(barrier, size)

    def rows_of(zz, tt, chunk):
        start = pl.multiple_of(zz * block + tt * piece + chunk * step, step)
        return rows_all.at[pl.ds(start, step)]

    def origin(way, distance):
        return z - distance if way == 0 else z + distance

    def chain(way, distance, chunk):
        ref = rows_of(origin(way, distance), t, chunk)
        index = (way * planes + distance) * A_CHUNKS + chunk
        return remote(ref, ref, a_sem, index, at(z + 1 if way == 0 else z - 1, y, t))

    def chain_arrival(way, distance, chunk):
        ref = rows_of(origin(way, distance), t, chunk)
        index = (way * planes + distance - 1) * A_CHUNKS + chunk
        return remote(ref, ref, a_sem, index, across_x)

    def can_send(way, distance):
        if way == 0:
            return jnp.logical_and(z - distance >= 0, z + 1 < planes)
        return jnp.logical_and(z + distance < planes, z - 1 >= 0)

    def exists(way, distance):
        return z - distance >= 0 if way == 0 else z + distance < planes

    def sideways(way, distance, chunk, arrival=False):
        ref = rows_of(origin(way, distance), tx if arrival else t, chunk)
        index = (way * planes + distance) * A_CHUNKS + chunk
        return remote(ref, ref, ax_sem, index, across_x)

    def to_partner(way, distance, chunk, far):
        tt = tx if far else t
        ref = rows_of(origin(way, distance), tt, chunk)
        return remote(ref, ref, ac_sem, way * planes + distance, partner)

    def home(zz, yy):
        return pl.multiple_of((zz * 2 + yy) * depth, depth)

    fine, fine_kv = depth // W_CHUNKS, half // W_CHUNKS

    def pieces(ref, start, cc, j):
        low = pl.multiple_of(start + j * fine, fine)
        low_kv = pl.multiple_of(start + cc * half + j * fine_kv, fine_kv)
        return [
            ref.at[pl.ds(low, fine), pl.ds(0, three)],
            ref.at[pl.ds(low_kv, fine_kv), pl.ds(three, width)],
        ]

    def narrow(ref, start, cc):
        return ref.at[pl.ds(pl.multiple_of(start + cc * half, half), half), pl.ds(three, width)]

    def w_sources(tt):
        cols = pl.ds(pl.multiple_of(tt * width, width), width)
        return [w_query.at[:, cols], w_glu.at[:, cols], w_gate.at[:, cols], w_kv.at[tt]]

    def w_targets(ref, start, cc):
        here = pl.ds(start, depth)
        return [ref.at[here, pl.ds(g * width, width)] for g in range(3)] + [narrow(ref, start, cc)]

    def first_all(kind, target, tt, what):
        for here, ref, start in (
            (t == z, w_all, home(z, y)),
            (t != z, stage, pl.multiple_of(t * depth, depth)),
        ):
            @pl.when(here)
            def _():
                for a, b in zip(w_sources(tt), w_targets(ref, start, tt % 2)):
                    what(remote(a, b, w1_sem, kind, target))

    block_rows = 3 * depth // 4 + half // 4

    def first_arrival(kind):
        all_here(w_all.at[pl.ds(0, block_rows)], w1_sem, kind, across_x)

    def staged(src_t):
        return pl.multiple_of(src_t * depth, depth)

    def second(src_t, j):
        return [
            remote(a, b, w2_sem, z * W_CHUNKS + j, at(src_t, y, t))
            for a, b in zip(pieces(stage, staged(src_t), c, j), pieces(w_all, home(z, y), c, j))
        ]

    def second_arrival(from_z, j):
        all_here(w_all.at[pl.ds(0, block_rows // W_CHUNKS)], w2_sem, from_z * W_CHUNKS + j, across_x)

    def third(from_z, j, i):
        ref = pieces(w_all, home(from_z, y), c, j)[i]
        return remote(ref, ref, w3_sem, from_z * 2 + i, across_y)

    def to_share(from_z, own, arrival=False):
        ref = narrow(w_all, home(from_z, y if own else 1 - y), 1 - c if arrival else c)
        return remote(ref, ref, kc_sem, from_z * 2 + own, partner)

    ahead = 1 - 2 * (z // (planes // 2))
    end = (z // (planes // 2)) * (planes - 1)
    ends = jnp.logical_or(z == 0, z == planes - 1)
    middle = jnp.logical_not(ends)

    def out_copies(yy, side=0):
        return [
            weights.at[pl.ds(pl.multiple_of((2 * side + kind) * part + yy * group, group), group)]
            for kind in range(2)
        ]

    end_outs = [
        remote(a, b, o_sem, 2 + i, at(z + ahead, y, t))
        for i, (a, b) in enumerate(zip((out_attn, out_conv), out_copies(y, 1)))
    ]
    half_group = group // 2

    def end_across(i, arrival=False):
        start = (2 + i // 2) * part + (1 - y if arrival else y) * group + (i % 2) * half_group
        ref = weights.at[pl.ds(pl.multiple_of(start, half_group), half_group)]
        return remote(ref, ref, o_sem, 4 + i, across_y)

    outs = [
        remote(a, b, o_sem, i, across_y)
        for i, (a, b) in enumerate(zip((out_attn, out_conv), out_copies(y)))
    ]
    out_loads = [
        pltpu.make_async_copy(a, b, local_sem.at[4 + i])
        for i, (a, b) in enumerate(zip((out_attn, out_conv), out_copies(y)))
    ]

    def own_loads(ref, start):
        return [
            pltpu.make_async_copy(a, b, local_sem.at[i])
            for i, (a, b) in enumerate(zip(w_sources(t)[:3], w_targets(ref, start, c)))
        ]


    for chunk in range(A_CHUNKS):
        for way in range(2):
            @pl.when(can_send(way, 0))
            def _():
                chain(way, 0, chunk).start()

    @pl.when(ends)
    def _():
        for copy in end_outs:
            copy.start()

    small_to = [(partner, tp, 0), (across_x, tx, 1), (diagonal, td, 2)]

    def small_copy(target, tt, i):
        return pltpu.make_async_remote_copy(
            src_ref=small_src.at[tt],
            dst_ref=small,
            send_sem=small_sem[0].at[0],
            recv_sem=small_sem[1].at[0],
            device_id=target,
            device_id_type=MESH,
        )

    @pl.when(t == z)
    def _():
        for args in small_to:
            small_copy(*args).start()
        small[...] = small_src[t]

    for here, ref, start in ((t == z, w_all, home(z, y)), (t != z, stage, staged(t))):
        @pl.when(here)
        def _():
            for copy in own_loads(ref, start):
                copy.start()
            ref[pl.ds(pl.multiple_of(start + c * half, half), half), three : three + width] = w_kv[t]

    first_all(2, partner, tp, lambda copy: copy.start())
    first_all(0, across_x, tx, lambda copy: copy.start())
    first_all(1, diagonal, td, lambda copy: copy.start())
    for copy in outs + out_loads:
        copy.start()
    for here, ref, start in ((t == z, w_all, home(z, y)), (t != z, stage, staged(t))):
        @pl.when(here)
        def _():
            for copy in own_loads(ref, start):
                copy.wait()

    def toward(target, way):
        return target > z if way == 0 else target < z

    def next_to(target, way):
        return target == (z + 1 if way == 0 else z - 1)

    def send_second(way, sources, near):
        for j in range(W_CHUNKS):
            for src_t in sources:
                beside = next_to(src_t, way)
                beyond = jnp.logical_and(toward(src_t, way), jnp.logical_not(beside))

                @pl.when(beside if near else beyond)
                def _():
                    for copy in second(src_t, j):
                        copy.start()

    def chain_step(distance, chunks=range(A_CHUNKS)):
        for chunk in chunks:
            for way in range(2):
                @pl.when(exists(way, distance))
                def _():
                    chain_arrival(way, distance, chunk).wait_recv()

                    @pl.when(can_send(way, distance))
                    def _():
                        chain(way, distance, chunk).start()

                    sideways(way, distance, chunk).start()
                    to_partner(way, distance, chunk, 0).start()

    def sideways_step(distance):
        for chunk in range(A_CHUNKS):
            for way in range(2):
                @pl.when(exists(way, distance))
                def _():
                    sideways(way, distance, chunk, True).wait_recv()
                    to_partner(way, distance, chunk, 1).start()

    def settle(from_z, j):
        for i in (1, 0):
            third(from_z, j, i).start()
        if j == W_CHUNKS - 1:
            to_share(from_z, 1).start()

    def block_step(from_z, j):
        second_arrival(from_z, j)
        settle(from_z, j)

    for k in range(1, planes):
        normalise(lax.rem(t + k, planes) * piece, piece)
    first_arrival(2)
    chain_step(1)
    for way in range(2):
        send_second(way, (t, tp), True)

    first_arrival(0)
    first_arrival(1)
    for way in range(2):
        send_second(way, (tx, td), True)
        send_second(way, (t, tp, tx, td), False)


    for j in range(W_CHUNKS):
        settle(z, j)
    for distance in range(2, planes - 1):
        chain_step(distance)

    row = lax.broadcasted_iota(jnp.int32, (block, LANES), 0)
    for zz in range(planes):
        angle = ((2 * zz + y) * block + row).astype(f32) * freq[...]
        here = slice(zz * block, (zz + 1) * block)
        cosine[here, :] = jnp.cos(angle)
        sine[here, :] = jnp.sin(angle)

    @pl.when(middle)
    def _():
        end_outs[0].wait_recv()
        for i in range(2):
            end_across(i).start()

    blocks_from = [
        z,
        jnp.where(middle, end, z + ahead),
        jnp.where(middle, planes - 1 - z, z + 2 * ahead),
        jnp.where(middle, planes - 1 - end, z + 3 * ahead),
    ]

    def tokens_here(distance):
        for way in range(2):
            @pl.when(exists(way, distance))
            def _():
                all_here(rows_all.at[pl.ds(0, 2 * piece)], ac_sem, way * planes + distance, partner)

    first_row = (z // (planes // 2)) * block
    last_row = (planes - 1) * block - end * block

    def multiply(from_z, yy, fresh):
        cols = pl.ds(home(from_z, yy), depth)

        @pl.loop(0, planes - 1)
        def _(i):
            here = pl.ds(pl.multiple_of(first_row + i * block, block), block)
            value = jnp.dot(rows_all[here, cols], w_all[cols, :], preferred_element_type=f32)
            if fresh:
                acc[here, :] = value
            else:
                acc[here, :] += value

    def multiply_own(pair):
        for k in pair:
            to_share(blocks_from[k], 1, True).wait_recv()
            if k == 0:
                multiply(blocks_from[0], y, True)
        if 0 not in pair:
            multiply(blocks_from[pair[0]], y, False)
        multiply(blocks_from[pair[1]], y, False)

    def share_other(pair):
        for k in pair:
            all_here(narrow(w_all, 0, 0), w3_sem, blocks_from[k] * 2 + 1, across_y)
            to_share(blocks_from[k], 0).start()

    def multiply_other(pair):
        for k in pair:
            all_here(w_all.at[pl.ds(0, depth), pl.ds(0, three)], w3_sem, blocks_from[k] * 2, across_y)
            to_share(blocks_from[k], 0, True).wait_recv()

        @pl.loop(0, 2)
        def _(i):
            multiply(jnp.where(i == 0, blocks_from[pair[0]], blocks_from[pair[1]]), 1 - y, False)

    for j in range(W_CHUNKS):
        block_step(blocks_from[1], j)
    sideways_step(1)
    for j in range(W_CHUNKS):
        block_step(blocks_from[2], j)
        block_step(blocks_from[3], j)
        if j == 1:
            sideways_step(2)
        if j == 2:
            chain_step(planes - 1, range(A_CHUNKS // 4))
            share_other((0, 1))
            for distance in range(1, planes - 1):
                tokens_here(distance)
            multiply_own((0, 1))
            multiply_other((0, 1))
            chain_step(planes - 1, range(A_CHUNKS // 4, A_CHUNKS // 2))
    chain_step(planes - 1, range(A_CHUNKS // 2, A_CHUNKS))
    @pl.when(middle)
    def _():
        end_outs[1].wait_recv()
        end_across(2).start()

    multiply_own((2, 3))
    share_other((2, 3))
    sideways_step(planes - 1)
    multiply_other((2, 3))

    tokens_here(planes - 1)
    here = pl.ds(pl.multiple_of(last_row, block), block)

    @pl.loop(0, 2)
    def _(i):
        cols = pl.ds(pl.multiple_of(i * 2 * width, 2 * width), 2 * width)
        acc[here, cols] = jnp.dot(rows_all[here, :], w_all[:, cols], preferred_element_type=f32)

    lane = lax.broadcasted_iota(jnp.int32, (block, LANES), 1)
    low = lax.rem(lane, HEAD) < HEAD // 2

    def turned(value, here):
        other = jnp.where(low, -pltpu.roll(value, LANES - HEAD // 2, 1), pltpu.roll(value, HEAD // 2, 1))
        return value * cosine[here, :] + other * sine[here, :]

    def halo(kind, zz):
        if kind == 0:
            ref = kv_b.at[pl.ds((zz + 1) * block - WINDOW, WINDOW)]
            return remote(ref, kv_rim.at[zz + y], halo_sem, zz, across_y)
        ref = gated.at[pl.ds((zz + 1) * block - 32, 32)]
        return remote(ref, gated_rim.at[zz + y], halo_sem, planes + zz, across_y)

    def halo_arrival(kind, zz):
        ref = (kv_rim if kind == 0 else gated_rim).at[zz + 1 - y]
        return remote(ref, ref, halo_sem, kind * planes + zz, across_y)

    for zz in range(planes):
        here = slice(zz * block, (zz + 1) * block)
        value = acc[here, three:]
        kv_b[here, :] = jnp.where(lane < HEAD, turned(value, here), value).astype(kv_b.dtype)
        halo(0, zz).start()
    for zz in range(planes):
        here = slice(zz * block, (zz + 1) * block)
        gate = acc[here, 2 * width : three]
        value = (acc[here, width : 2 * width] * (1.0 / (1.0 + jnp.exp(-gate)))).astype(gated.dtype)
        gated[here, :] = value
        extended[zz, 32:, :] = value.astype(f32)
        halo(1, zz).start()

    @pl.when(y == 0)
    def _():
        kv_rim[0] = jnp.zeros_like(kv_rim[0])
        gated_rim[0] = jnp.zeros_like(gated_rim[0])

    for zz in range(planes):
        here = slice(zz * block, (zz + 1) * block)
        q_b[here, :] = (turned(acc[here, :width], here) * (1.0 / math.sqrt(HEAD))).astype(q_b.dtype)

    @pl.when(t != z)
    def _():
        small_copy(partner, tp, 0).wait_recv()

    @pl.when(middle)
    def _():
        end_across(3).start()

    lane_q = lax.broadcasted_iota(jnp.int32, (WINDOW, LANES), 1)
    lane_k = lax.broadcasted_iota(jnp.int32, (2 * WINDOW, LANES), 1)
    row_s = lax.rem(lax.broadcasted_iota(jnp.int32, (heads * WINDOW, 2 * WINDOW), 0), WINDOW)
    col_s = lax.broadcasted_iota(jnp.int32, (heads * WINDOW, 2 * WINDOW), 1)
    distance_s = row_s + WINDOW - col_s
    inside = jnp.logical_and(distance_s >= 0, distance_s < WINDOW)
    sink_row = small[33:34, :]
    lane_1 = lax.broadcasted_iota(jnp.int32, (1, LANES), 1)
    sinks = [
        jnp.sum(jnp.where(lane_1 == t * heads + h, sink_row, 0.0), axis=1, keepdims=True)
        for h in range(heads)
    ]
    sink_col = jnp.concatenate([jnp.broadcast_to(v, (WINDOW, 1)) for v in sinks], axis=0)

    def attend(first_row, keys, mask):
        query = q_b[pl.ds(first_row, WINDOW), :]
        keys_f = keys.astype(f32)
        swapped = pltpu.roll(keys_f, HEAD, 1)
        key_two = jnp.where(lane_k < HEAD, keys_f, swapped).astype(jnp.bfloat16)
        value_two = jnp.where(lane_k < HEAD, swapped, keys_f).astype(jnp.bfloat16)
        zero = jnp.zeros_like(query)
        stacked = jnp.concatenate(
            [jnp.where(lane_q // HEAD == h, query, zero) for h in range(heads)], axis=0
        )
        scores = lax.dot_general(
            stacked, key_two, (((1,), (1,)), ((), ())), preferred_element_type=f32
        )
        scores = jnp.where(mask, scores, -1e30)
        top = jnp.maximum(jnp.max(scores, axis=1, keepdims=True), sink_col)
        grown = jnp.exp(scores - top)
        total = jnp.sum(grown, axis=1, keepdims=True) + jnp.exp(sink_col - top)
        probs = (grown / total).astype(jnp.bfloat16)
        mixed_values = jnp.dot(probs, value_two, preferred_element_type=f32)
        result = mixed_values[:WINDOW]
        for h in range(1, heads):
            result = jnp.where(lane_q // HEAD == h, mixed_values[h * WINDOW : (h + 1) * WINDOW], result)
        act[pl.ds(first_row, WINDOW), columns(0, t)] = result.astype(act.dtype)

    def columns(kind, tt, side=0):
        return pl.ds(pl.multiple_of((2 * side + kind) * part + tt * width, width), width)

    blocks = block // WINDOW

    for zz in range(planes):
        for b in range(1, blocks):
            start = zz * block + b * WINDOW
            attend(start, kv_b[pl.ds(start - WINDOW, 2 * WINDOW), :], inside)

    def attend_first(zz):
        start = pl.multiple_of(zz * block, block)
        keys = jnp.concatenate([kv_rim[zz], kv_b[pl.ds(start, WINDOW), :]], axis=0)
        began = jnp.logical_or(zz * 2 + y > 0, col_s >= WINDOW)
        attend(start, keys, jnp.logical_and(inside, began))

    for zz in range(planes):
        if zz < planes - 1:
            halo_arrival(1, zz).wait_recv()

        @pl.when(y == 1)
        def _():
            if zz == planes - 1:
                halo_arrival(1, zz).wait_recv()

    for zz in range(planes):
        extended[zz, 0:32, :] = gated_rim[zz].astype(f32)
    strip = 64

    @pl.loop(0, planes)
    def _(zz):
        @pl.loop(0, block // strip)
        def _(i):
            base = pl.multiple_of(i * strip, strip)
            window = extended[zz, pl.ds(base, strip + 32), :]
            total = jnp.zeros((strip, width), f32)
            for shift in range(8):
                moved = window[shift : shift + strip + 24] if shift else window
                for k in range((shift - 2) % 8, KSIZE, 8):
                    low = 2 + k - shift
                    total = total + moved[low : low + strip] * small[k : k + 1, :]
            filtered[pl.ds(pl.multiple_of(zz * block + base, strip), strip), :] = total

    tiles = rows // LANES
    for k in range(tiles):
        value = filtered[k * LANES : (k + 1) * LANES, :]
        total = jnp.sum(value, axis=1, keepdims=True)
        square = jnp.sum(value * value, axis=1, keepdims=True)
        stats[k : k + 1, :] = jnp.transpose(jnp.broadcast_to(total, (LANES, LANES)))[0:1]
        stats[tiles + k : tiles + k + 1, :] = jnp.transpose(jnp.broadcast_to(square, (LANES, LANES)))[0:1]

    def stat(k):
        g = peers[k]
        return pltpu.make_async_remote_copy(
            src_ref=stats,
            dst_ref=stats_all.at[mine],
            send_sem=s_sem[0].at[0],
            recv_sem=s_sem[1].at[0],
            device_id=at(g // planes, y, g % planes),
            device_id_type=MESH,
        )

    for k in range(size - 1):
        stat(k).start()
    stats_all[mine] = stats[...]

    for zz in range(planes):
        if zz < planes - 1:
            halo_arrival(0, zz).wait_recv()

        @pl.when(y == 1)
        def _():
            if zz == planes - 1:
                halo_arrival(0, zz).wait_recv()

    def region(kind, r, tt, side):
        start = pl.multiple_of(r * block, block)
        return act.at[pl.ds(start, block), columns(kind, tt, side)]

    def cross(kind, r, side, arrival=False):
        ref = region(kind, r, tx if arrival else t, side)
        return remote(ref, ref, x_sem, (side * 2 + kind) * planes + r, across_x)

    def hand(kind, r, side, far):
        ref = region(kind, r, tx if far else t, side)
        return remote(ref, ref, c_sem, side * planes + r, partner)

    def send_out(kind, r, side=0):
        cross(kind, r, side).start()
        hand(kind, r, side, 0).start()

    near = z // (planes // 2)
    order = [(1 - near) * (planes - 1 - j) + near * j for j in range(planes)]

    def inward(kind, j):
        source = region(kind, order[j], t, 0)
        return remote(source, region(kind, order[j], t, 1), e_sem, kind * planes + j, at(z + ahead, y, t))

    def pass_in(kind, j):
        inward(kind, j).wait_recv()
        send_out(kind, order[j], 1)

    for pair in ((0, 1), (2, 3)):
        for j in pair:
            attend_first(order[j])

        @pl.when(ends)
        def _():
            for j in pair:
                if j < planes - 1:
                    inward(0, j).start()

        @pl.when(middle)
        def _():
            for j in pair:
                if j < 2:
                    send_out(0, order[j])

    @pl.when(middle)
    def _():
        pass_in(0, 0)
        pass_in(0, 1)

    all_here(stats_all.at[pl.ds(0, size - 1)], s_sem, 0, partner)
    total = stats_all[0]
    for g in range(1, size):
        total = total + stats_all[g]
    mean = total[:tiles] / channels
    variance = total[tiles:] / channels - mean * mean
    moments[0] = mean
    moments[1] = lax.rsqrt(variance + 1e-05)
    per = block // LANES

    def normed_out(r):
        for k in range(per):
            tile = r * per + k
            mean_col = jnp.transpose(jnp.broadcast_to(moments[0, pl.ds(tile, 1), :], (LANES, LANES)))
            rate_col = jnp.transpose(jnp.broadcast_to(moments[1, pl.ds(tile, 1), :], (LANES, LANES)))
            here = pl.ds(pl.multiple_of(tile * LANES, LANES), LANES)
            scaled = (filtered[here, :] - mean_col) * rate_col * small[32:33, :]
            act[here, columns(1, t)] = (scaled / (1.0 + jnp.exp(-scaled))).astype(act.dtype)

    out_step = mixed.shape[1] // OUT_CHUNKS

    def gathered(j, sides):
        for side in sides:
            for kind in range(2):
                cross(kind, order[j], side, True).wait_recv()
                hand(kind, order[j], side, 1).start()
        for side in sides:
            ref = act.at[pl.ds(0, block), pl.ds(0, 4 * width)]
            all_here(ref, c_sem, side * planes + order[j], partner)

    def out_columns(h):
        return pl.ds(pl.multiple_of(h * out_step, out_step), out_step)

    def travel(slot, h, toward_z):
        return remote(
            outgoing.at[slot, :, out_columns(h)],
            incoming.at[slot, :, out_columns(h)],
            r_sem,
            slot * OUT_CHUNKS + h,
            at(toward_z, y, t),
        )

    def outputs(j, h, deep):
        start = pl.multiple_of(order[j] * block, block)
        deep_rows = slice(0, (4 if deep else 2) * part)
        return jnp.dot(
            act[pl.ds(start, block), deep_rows], weights[deep_rows, out_columns(h)], preferred_element_type=f32
        )

    def send_sums(j, deep, came, slot, toward_z):
        @pl.loop(0, OUT_CHUNKS)
        def _(h):
            value = outputs(j, h, deep)
            if came is not None:
                travel(came, h, across_z).wait_recv()
                value = value + incoming[came, :, out_columns(h)].astype(f32)
            outgoing[slot, :, out_columns(h)] = value.astype(outgoing.dtype)
            travel(slot, h, toward_z).start()

    def finish(j, deep, came):
        @pl.loop(0, OUT_CHUNKS)
        def _(h):
            value = outputs(j, h, deep)
            travel(came, h, across_z).wait_recv()
            mixed[:, out_columns(h)] = value + incoming[came, :, out_columns(h)].astype(f32)

    across_z = z + ahead

    for j, r in enumerate(order):
        normed_out(r)

        @pl.when(ends)
        def _():
            if j < planes - 1:
                inward(1, j).start()
            else:
                send_out(0, r)
                send_out(1, r)

        if j == 0:
            @pl.when(middle)
            def _():
                send_out(1, r)

    for copy in out_loads:
        copy.wait()
    for copy in outs:
        copy.wait_recv()

    @pl.when(middle)
    def _():
        for i in range(4):
            end_across(i, True).wait_recv()

    @pl.when(middle)
    def _():
        pass_in(1, 0)
        send_out(1, order[1])
        gathered(0, (0, 1))
        send_sums(0, True, None, 0, across_z)

    @pl.when(middle)
    def _():
        pass_in(1, 1)
        for kind in range(2):
            send_out(kind, order[3])
        gathered(1, (0, 1))
        send_sums(1, True, None, 1, across_z)

    @pl.when(middle)
    def _():
        for kind in range(2):
            send_out(kind, order[2])
            pass_in(kind, 2)
        gathered(3, (0,))
        send_sums(3, False, 0, 2, z - ahead)

    @pl.when(middle)
    def _():
        gathered(2, (0, 1))
        finish(2, True, 1)

    @pl.when(ends)
    def _():
        gathered(3, (0,))
        finish(3, False, 2)

    @pl.when(t == z)
    def _():
        all_sent(small_src.at[pl.ds(0, 3)], small_sem, partner)

    @pl.when(y == 0)
    def _():
        for kind in range(2):
            halo_arrival(kind, planes - 1).wait_recv()

    all_sent(kv_b.at[pl.ds(0, planes * (WINDOW + 32))], halo_sem, across_y)
    all_sent(w_all.at[pl.ds(0, 3 * block_rows)], w1_sem, partner)
    all_sent(w_all.at[pl.ds(0, 3 * block_rows)], w2_sem, partner)
    all_sent(w_all.at[pl.ds(0, planes * block_rows)], w3_sem, across_y)
    all_sent(w_all.at[pl.ds(0, 2 * planes * half), pl.ds(0, width)], kc_sem, partner)
    all_sent(rows_all.at[pl.ds(0, (planes - 1) * piece)], ax_sem, across_x)
    all_sent(rows_all.at[pl.ds(0, 2 * (planes - 1) * piece)], ac_sem, partner)
    all_sent(stats_all.at[pl.ds(0, size - 1)], s_sem, partner)

    def sent_regions(count, sems):
        all_sent(act.at[pl.ds(0, 2 * block), pl.ds(0, count * width // 2)], sems, partner)

    @pl.when(ends)
    def _():
        all_sent(rows_all.at[pl.ds(0, piece)], a_sem, partner)
        sent_regions(2 * (planes - 1), e_sem)
        sent_regions(2, x_sem)
        sent_regions(4, c_sem)
        all_sent(weights.at[pl.ds(0, 4 * group)], o_sem, partner)

    @pl.when(middle)
    def _():
        all_sent(rows_all.at[pl.ds(0, (planes + 1) * piece)], a_sem, partner)
        sent_regions(2 * planes + 2 * (planes - 1), x_sem)
        sent_regions(4 * planes + 4 * (planes - 1), c_sem)
        all_sent(weights.at[pl.ds(0, 4 * group)], o_sem, partner)
        all_sent(outgoing, r_sem, partner)


def planned_per_device(
    tokens,
    norm_gain,
    w_query,
    w_key,
    w_value,
    w_glu,
    w_gate,
    sink_logit,
    conv_taps,
    conv_gain,
    out_attn,
    out_conv,
):
    planes = lax.axis_size("tp")
    block, model = tokens.shape
    rows = planes * block
    depth, cols = w_query.shape
    width = cols // planes
    columns_out = out_attn.shape[1]
    size = planes * planes
    half_width = HEAD // 2
    freq = 10000.0 ** (-jnp.arange(half_width, dtype=jnp.float32) * 2.0 / HEAD)
    freq = jnp.tile(freq, LANES // half_width)[None]
    vmem = pl.BlockSpec(memory_space=pltpu.VMEM)
    any_spec = pl.BlockSpec(memory_space=pl.ANY)
    dma = pltpu.SemaphoreType.DMA
    bf16, f32 = jnp.bfloat16, jnp.float32
    tiles = rows // LANES
    chunks = 2 * planes * A_CHUNKS
    counts = [
        chunks, chunks, 2 * planes, 3, planes * W_CHUNKS, 2 * planes, 2 * planes, 8, 1,
        2 * planes, 1, 2 * planes, 4 * planes, 2 * planes, 3 * OUT_CHUNKS,
    ]
    sems = [dma((n,)) for count in counts for n in (1, count)]
    return pl.pallas_call(
        functools.partial(layer_kernel, planes, CONV),
        out_shape=jax.ShapeDtypeStruct((block, columns_out), f32),
        in_specs=[vmem] * 8 + [any_spec] * 5,
        out_specs=vmem,
        scratch_shapes=[
            pltpu.VMEM((rows, model), bf16),
            pltpu.VMEM((2 * planes * depth, 4 * width), bf16),
            pltpu.VMEM((planes * depth, 4 * width), bf16),
            pltpu.VMEM((planes, depth // 2, 2 * HEAD), bf16),
            pltpu.VMEM((planes, 40, width), f32),
            pltpu.VMEM((40, width), f32),
            pltpu.VMEM((rows, 4 * width), f32),
            pltpu.VMEM((rows, LANES), f32),
            pltpu.VMEM((rows, LANES), f32),
            pltpu.VMEM((rows, width), bf16),
            pltpu.VMEM((rows, width), bf16),
            pltpu.VMEM((planes + 1, WINDOW, width), bf16),
            pltpu.VMEM((rows, width), bf16),
            pltpu.VMEM((planes + 1, 32, width), bf16),
            pltpu.VMEM((planes, 32 + block, width), f32),
            pltpu.VMEM((rows, width), f32),
            pltpu.VMEM((rows, 4 * planes * width), bf16),
            pltpu.VMEM((4 * planes * width, columns_out), bf16),
            pltpu.VMEM((2 * tiles, LANES), f32),
            pltpu.VMEM((size, 2 * tiles, LANES), f32),
            pltpu.VMEM((2, tiles, LANES), f32),
            pltpu.VMEM((3, block, columns_out), bf16),
            pltpu.VMEM((3, block, columns_out), bf16),
            dma((8,)),
        ]
        + sems,
        compiler_params=pltpu.CompilerParams(
            collective_id=0, has_side_effects=True, vmem_limit_bytes=60 * 2**20
        ),
    )(
        tokens,
        norm_gain[None],
        freq,
        w_key,
        w_value,
        conv_taps,
        conv_gain[None],
        sink_logit[None],
        w_query,
        w_glu,
        w_gate,
        out_attn,
        out_conv,
    ).astype(bf16)


def solution(mesh):
    planes, others = mesh.shape["tp"], mesh.shape["sp"]
    fits = others == 2 * planes and planes == 4 and HEADS == 2 * planes * planes
    return jax.shard_map(
        planned_per_device if fits else gathered_per_device,
        mesh=mesh,
        in_specs=(
            P("sp", None),
            P(),
            P("sp", "tp"),
            P("sp", "tp"),
            P("sp", "tp"),
            P("sp", "tp"),
            P("sp", "tp"),
            P("tp"),
            P(None, "tp"),
            P("tp"),
            P("sp", "tp"),
            P("sp", "tp"),
        ),
        out_specs=P("sp", "tp"),
        check_vma=False,
    )
```

```python
import functools
import math

import jax
import jax.numpy as jnp
import numpy as np
from jax import lax
from jax.experimental import pallas as pl
from jax.experimental.pallas import tpu as pltpu
from jax.sharding import PartitionSpec as P

HEADS = 32
HEAD = 64
KV = 8
CONV = 2048
KSIZE = 31
WINDOW = 128


def passed_along(block, axis, distance):
    devices = range(lax.axis_size(axis))
    route = [(i - distance, i) for i in devices if i - distance in devices]
    return lax.ppermute(block, axis, route)


def rotate_heads(values, positions):
    half_width = values.shape[-1] // 2
    frequency = 10000.0 ** (-jnp.arange(half_width, dtype=jnp.float32) * 2.0 / values.shape[-1])
    angles = positions.astype(jnp.float32)[:, None] * frequency[None, :]
    cosine = jnp.cos(angles)[:, None, :]
    sine_part = jnp.sin(angles)[:, None, :]
    first_half = values[..., :half_width]
    second_half = values[..., half_width:]
    return jnp.concatenate(
        [
            first_half * cosine - second_half * sine_part,
            second_half * cosine + first_half * sine_part,
        ],
        axis=-1,
    )


def ring_gather_kernel(n, count, *refs):
    shards, wholes = refs[:count], refs[count : 2 * count]
    bounce = refs[2 * count : 3 * count]
    in_sem, out_sem, send_sem, recv_sem = refs[3 * count :]
    me = lax.axis_index("sp")
    half = n // 2
    odd = lax.rem(me, 2)
    place = (1 - odd) * lax.div(me, 2) + odd * (n - 1 - lax.div(me, 2))

    def device_at(position):
        spot = lax.rem(position + 2 * n, n)
        back = lax.div(spot, half)
        return (1 - back) * 2 * spot + back * (2 * (n - 1 - spot) + 1)

    ahead, behind = device_at(place + 1), device_at(place - 1)
    barrier = pltpu.get_barrier_semaphore()
    for neighbour in (ahead, behind):
        pl.semaphore_signal(
            barrier, inc=1, device_id={"sp": neighbour}, device_id_type=pl.DeviceIdType.MESH
        )
    pl.semaphore_wait(barrier, 2)

    def block(array, owner, way):
        rows = shards[array].shape[0]
        part = rows // 2
        start = pl.multiple_of(owner * rows + way * part, part)
        return wholes[array].at[pl.ds(start, part)]

    def hop(array, step, way):
        owner = device_at(place - step) if way == 0 else device_at(place + step)
        part = shards[array].shape[0] // 2
        target = block(array, owner, way)
        source = shards[array].at[pl.ds(way * part, part)] if step == 0 else target
        return pltpu.make_async_remote_copy(
            src_ref=source,
            dst_ref=target,
            send_sem=send_sem.at[way, step, array],
            recv_sem=recv_sem.at[way, step, array],
            device_id={"sp": ahead if way == 0 else behind},
            device_id_type=pl.DeviceIdType.MESH,
        )

    def arrival(array, step, way):
        owner = device_at(place - step - 1) if way == 0 else device_at(place + step + 1)
        target = block(array, owner, way)
        return pltpu.make_async_remote_copy(
            src_ref=target,
            dst_ref=target,
            send_sem=send_sem.at[way, step, array],
            recv_sem=recv_sem.at[way, step, array],
            device_id={"sp": ahead if way == 0 else behind},
            device_id_type=pl.DeviceIdType.MESH,
        )

    for array in range(count):
        for way in range(2):
            hop(array, 0, way).start()
    loads = [
        pltpu.make_async_copy(shards[a], bounce[a], in_sem.at[a]) for a in range(count)
    ]
    for load in loads:
        load.start()
    stores = []
    for a in range(count):
        loads[a].wait()
        rows = shards[a].shape[0]
        mine = wholes[a].at[pl.ds(pl.multiple_of(me * rows, rows), rows)]
        stores.append(pltpu.make_async_copy(bounce[a], mine, out_sem.at[a]))
        stores[a].start()
    for step in range(1, n - 1):
        for array in range(count):
            for way in range(2):
                arrival(array, step - 1, way).wait_recv()
                hop(array, step, way).start()
    for array in range(count):
        for way in range(2):
            arrival(array, n - 2, way).wait_recv()
    for step in range(n - 1):
        for array in range(count):
            for way in range(2):
                hop(array, step, way).wait_send()
    for store in stores:
        store.wait()


def ring_gather(arrays, collective_id):
    n = lax.axis_size("sp")
    count = len(arrays)
    return pl.pallas_call(
        functools.partial(ring_gather_kernel, n, count),
        out_shape=[
            jax.ShapeDtypeStruct((n * a.shape[0],) + a.shape[1:], a.dtype) for a in arrays
        ],
        in_specs=[pl.BlockSpec(memory_space=pl.ANY)] * count,
        out_specs=[pl.BlockSpec(memory_space=pl.ANY)] * count,
        scratch_shapes=[pltpu.VMEM(a.shape, a.dtype) for a in arrays]
        + [
            pltpu.SemaphoreType.DMA((count,)),
            pltpu.SemaphoreType.DMA((count,)),
            pltpu.SemaphoreType.DMA((2, n - 1, count)),
            pltpu.SemaphoreType.DMA((2, n - 1, count)),
        ],
        compiler_params=pltpu.CompilerParams(
            collective_id=collective_id, has_side_effects=True
        ),
    )(*arrays)


def gathered_per_device(
    tokens,
    norm_gain,
    w_query,
    w_key,
    w_value,
    w_glu,
    w_gate,
    sink_logit,
    conv_taps,
    conv_gain,
    out_attn,
    out_conv,
):
    row_count = tokens.shape[0]
    offset_rows = lax.axis_index("sp") * row_count
    positions = offset_rows + jnp.arange(row_count, dtype=jnp.int32)
    tokens_f = tokens.astype(jnp.float32)
    normed = (
        tokens_f
        * lax.rsqrt(jnp.mean(tokens_f * tokens_f, axis=1, keepdims=True) + 1e-06)
        * norm_gain
    ).astype(jnp.bfloat16)
    local_heads = w_query.shape[1] // HEAD
    local_kv = w_key.shape[1] // HEAD
    group_size = HEADS // KV
    kv_width = local_kv * HEAD
    *pieces, attn_rows, conv_rows = ring_gather(
        (w_query, w_key, w_value, w_glu, w_gate, out_attn, out_conv), 0
    )
    query_acc, key_acc, value_acc, glu_acc, gate_acc = tuple(
        (
            jnp.dot(normed, weight_piece, preferred_element_type=jnp.float32)
            for weight_piece in pieces
        )
    )
    queries = rotate_heads(query_acc.reshape(row_count, local_heads, HEAD), positions).astype(
        jnp.bfloat16
    )
    keys_rot = rotate_heads(key_acc.reshape(row_count, local_kv, HEAD), positions).astype(
        jnp.bfloat16
    )
    keys_rot = keys_rot.reshape(row_count, kv_width)
    values_bf = value_acc.astype(jnp.bfloat16)
    kv_tail = jnp.concatenate(
        [keys_rot[row_count - WINDOW :], values_bf[row_count - WINDOW :]], axis=1
    )
    kv_rim = passed_along(kv_tail, "sp", 1)
    gated = (glu_acc * jax.nn.sigmoid(gate_acc)).astype(jnp.bfloat16)
    conv_tail = gated[row_count - (KSIZE - 1) :]
    conv_rim = passed_along(conv_tail, "sp", 1)
    block_count = row_count // WINDOW
    keys_all = jnp.concatenate([kv_rim[:, :kv_width], keys_rot], axis=0).reshape(
        block_count + 1, WINDOW, local_kv, HEAD
    )
    vals_all = jnp.concatenate([kv_rim[:, kv_width:], values_bf], axis=0).reshape(
        block_count + 1, WINDOW, local_kv, HEAD
    )
    key_blocks = jnp.concatenate([keys_all[:-1], keys_all[1:]], axis=1)
    value_blocks = jnp.concatenate([vals_all[:-1], vals_all[1:]], axis=1)
    query_block_rows = queries.reshape(block_count, WINDOW, local_kv, group_size, HEAD)
    score_matrix = jnp.einsum(
        "bqhgd,bkhd->bhgqk", query_block_rows, key_blocks, preferred_element_type=jnp.float32
    ) * (1.0 / math.sqrt(HEAD))
    block_ids = jnp.arange(block_count, dtype=jnp.int32)[:, None, None]
    query_pos = (
        offset_rows + block_ids * WINDOW + jnp.arange(WINDOW, dtype=jnp.int32)[None, :, None]
    )
    key_pos = (
        offset_rows
        + (block_ids - 1) * WINDOW
        + jnp.arange(2 * WINDOW, dtype=jnp.int32)[None, None, :]
    )
    distance = query_pos - key_pos
    allowed = (distance >= 0) & (distance < WINDOW) & (key_pos >= 0)
    score_matrix = jnp.where(allowed[:, None, None], score_matrix, -1e30)
    sink_local = sink_logit.reshape(local_kv, group_size)[None, :, :, None, None]
    highest = jnp.maximum(jnp.max(score_matrix, axis=-1, keepdims=True), sink_local)
    weights_exp = jnp.exp(score_matrix - highest)
    denom_total = jnp.sum(weights_exp, axis=-1, keepdims=True) + jnp.exp(sink_local - highest)
    weights_bfloat_half = (weights_exp / denom_total).astype(jnp.bfloat16)
    attended_values = jnp.einsum(
        "bhgqk,bkhd->bqhgd", weights_bfloat_half, value_blocks, preferred_element_type=jnp.float32
    ).astype(jnp.bfloat16)
    attended_values = attended_values.reshape(row_count, local_heads * HEAD)
    extended = jnp.concatenate([conv_rim, gated], axis=0).astype(jnp.float32)
    filtered = lax.conv_general_dilated(
        extended[None],
        conv_taps.astype(jnp.float32)[:, None, :],
        (1,),
        "VALID",
        dimension_numbers=("NWC", "WIO", "NWC"),
        feature_group_count=extended.shape[1],
        precision=lax.Precision.HIGHEST,
    )[0]
    channel_sum, channel_square = lax.psum(
        (jnp.sum(filtered, axis=1), jnp.sum(filtered * filtered, axis=1)), "tp"
    )
    mean_value = channel_sum / CONV
    variance = channel_square / CONV - mean_value * mean_value
    scaled = (filtered - mean_value[:, None]) * lax.rsqrt(variance + 1e-05)[:, None] * conv_gain
    conv_out = jax.nn.silu(scaled).astype(jnp.bfloat16)
    pieces = (
        lax.all_gather(attended_values, "tp", axis=1, tiled=True),
        lax.all_gather(conv_out, "tp", axis=1, tiled=True),
    )
    mixed = jnp.dot(pieces[0], attn_rows, preferred_element_type=jnp.float32) + jnp.dot(
        pieces[1], conv_rows, preferred_element_type=jnp.float32
    )
    return mixed.astype(jnp.bfloat16)


MESH = pl.DeviceIdType.MESH
A_CHUNKS = 4
W_CHUNKS = 4
OUT_CHUNKS = 4
END_CHUNKS = 4
LANES = 128


def remote(src, dst, sems, index, target):
    send_sem, recv_sem = sems
    return pltpu.make_async_remote_copy(
        src_ref=src,
        dst_ref=dst,
        send_sem=send_sem.at[0],
        recv_sem=recv_sem.at[index],
        device_id=target,
        device_id_type=MESH,
    )


def all_sent(ref, sems, target):
    remote(ref, ref, sems, 0, target).wait_send()


def all_here(ref, sems, index, target):
    remote(ref, ref, sems, index, target).wait_recv()


def layer_kernel(planes, channels, *refs):
    (tokens_far, norm_gain, freq, w_key, w_value, taps, conv_gain, sink) = refs[:8]
    (w_query, w_glu, w_gate, out_attn, out_conv) = refs[8:13]
    mixed = refs[13]
    (rows_all, w_all, stage, w_kv, small_src, small) = refs[14:20]
    (acc, cosine, sine, q_b, kv_b, kv_rim, gated, gated_rim, extended, filtered) = refs[20:30]
    (act, weights, stats, stats_all, moments, incoming, outgoing, tokens) = refs[30:38]
    local_sem = refs[38]
    pairs = [(refs[39 + 2 * i], refs[40 + 2 * i]) for i in range((len(refs) - 39) // 2)]
    (a_sem, ax_sem, ac_sem, w1_sem, w2_sem, w3_sem, kc_sem, o_sem, small_sem) = pairs[:9]
    (halo_sem, s_sem, e_sem, x_sem, c_sem, r_sem) = pairs[9:15]

    s, t = lax.axis_index("sp"), lax.axis_index("tp")
    z, y, x, c = s // 2, s % 2, t // 2, t % 2
    block = tokens.shape[0]
    rows = planes * block
    piece = block // planes
    step = piece // A_CHUNKS
    depth = w_query.shape[0]
    width = w_query.shape[1] // planes
    three = 3 * width
    half = depth // 2
    heads = width // HEAD
    group = out_attn.shape[0]
    part = planes * width
    size = planes * planes
    f32 = jnp.float32

    def at(zz, yy, tt):
        return {"sp": zz * 2 + yy, "tp": tt}

    tx, td, tp = (1 - x) * 2 + c, (1 - x) * 2 + (1 - c), x * 2 + (1 - c)
    across_y, across_x = at(z, 1 - y, t), at(z, y, tx)
    diagonal, partner = at(z, y, td), at(z, y, tp)
    mine = z * planes + t
    peers = [lax.rem(mine + k, size) for k in range(1, size)]

    barrier = pltpu.get_barrier_semaphore()
    for target in [across_y] + [at(g // planes, y, g % planes) for g in peers]:
        pl.semaphore_signal(barrier, inc=1, device_id=target, device_id_type=MESH)

    def normalise(start, count):
        @pl.loop(0, count // 16)
        def _(i):
            here = pl.multiple_of(start + i * 16, 16)
            value = tokens[pl.ds(here, 16), :].astype(f32)
            scale = lax.rsqrt(jnp.mean(value * value, axis=1, keepdims=True) + 1e-06)
            there = pl.multiple_of(z * block + here, 16)
            rows_all[pl.ds(there, 16), :] = (value * scale * norm_gain[...]).astype(rows_all.dtype)

    def quarter(k):
        part_rows = pl.ds(pl.multiple_of(lax.rem(t + k, planes) * piece, piece), piece)
        return pltpu.make_async_copy(tokens_far.at[part_rows], tokens.at[part_rows], local_sem.at[6 + k])

    for k in range(planes):
        quarter(k).start()

    lane = lax.broadcasted_iota(jnp.int32, (half, 2 * HEAD), 1)
    for cc in range(2):
        key = w_key[cc * half : (cc + 1) * half, :].astype(f32)
        value = w_value[cc * half : (cc + 1) * half, :].astype(f32)
        w_kv[cc] = jnp.where(lane < HEAD, key, pltpu.roll(value, HEAD, 1)).astype(w_kv.dtype)
        w_kv[2 + cc] = jnp.where(lane < HEAD, pltpu.roll(key, HEAD, 1), value).astype(w_kv.dtype)
    small_src[...] = jnp.zeros_like(small_src)
    for tt in range(planes):
        cols = slice(tt * width, (tt + 1) * width)
        small_src[tt, 0:KSIZE, :] = taps[:, cols].astype(f32)
        small_src[tt, 32:33, :] = conv_gain[:, cols]
        small_src[tt, 33:34, 0 : sink.shape[1]] = sink[...]
    quarter(0).wait()
    normalise(t * piece, piece)
    pl.semaphore_wait(barrier, size)

    def rows_of(zz, tt, chunk):
        start = pl.multiple_of(zz * block + tt * piece + chunk * step, step)
        return rows_all.at[pl.ds(start, step)]

    def origin(way, distance):
        return z - distance if way == 0 else z + distance

    def chain(way, distance, chunk):
        ref = rows_of(origin(way, distance), t, chunk)
        index = (way * planes + distance) * A_CHUNKS + chunk
        return remote(ref, ref, a_sem, index, at(z + 1 if way == 0 else z - 1, y, t))

    def chain_arrival(way, distance, chunk):
        ref = rows_of(origin(way, distance), t, chunk)
        index = (way * planes + distance - 1) * A_CHUNKS + chunk
        return remote(ref, ref, a_sem, index, across_x)

    def can_send(way, distance):
        if way == 0:
            return jnp.logical_and(z - distance >= 0, z + 1 < planes)
        return jnp.logical_and(z + distance < planes, z - 1 >= 0)

    def exists(way, distance):
        return z - distance >= 0 if way == 0 else z + distance < planes

    def sideways(way, distance, chunk, arrival=False):
        ref = rows_of(origin(way, distance), tx if arrival else t, chunk)
        index = (way * planes + distance) * A_CHUNKS + chunk
        return remote(ref, ref, ax_sem, index, across_x)

    def to_partner(way, distance, chunk, far):
        tt = tx if far else t
        ref = rows_of(origin(way, distance), tt, chunk)
        return remote(ref, ref, ac_sem, way * planes + distance, partner)

    def home(zz, yy):
        return pl.multiple_of((zz * 2 + yy) * depth, depth)

    fine, fine_kv = depth // W_CHUNKS, half // W_CHUNKS

    def pieces(ref, start, cc, j):
        low = pl.multiple_of(start + j * fine, fine)
        low_kv = pl.multiple_of(start + cc * half + j * fine_kv, fine_kv)
        return [
            ref.at[pl.ds(low, fine), pl.ds(0, three)],
            ref.at[pl.ds(low_kv, fine_kv), pl.ds(three, width)],
        ]

    def narrow(ref, start, cc):
        return ref.at[pl.ds(pl.multiple_of(start + cc * half, half), half), pl.ds(three, width)]

    def w_sources(tt):
        cols = pl.ds(pl.multiple_of(tt * width, width), width)
        return [w_query.at[:, cols], w_glu.at[:, cols], w_gate.at[:, cols], w_kv.at[tt]]

    def w_targets(ref, start, cc):
        here = pl.ds(start, depth)
        return [ref.at[here, pl.ds(g * width, width)] for g in range(3)] + [narrow(ref, start, cc)]

    def first_all(kind, target, tt, what):
        for here, ref, start in (
            (t == z, w_all, home(z, y)),
            (t != z, stage, pl.multiple_of(t * depth, depth)),
        ):
            @pl.when(here)
            def _():
                for a, b in zip(w_sources(tt), w_targets(ref, start, tt % 2)):
                    what(remote(a, b, w1_sem, kind, target))

    block_rows = 3 * depth // 4 + half // 4

    def first_arrival(kind):
        all_here(w_all.at[pl.ds(0, block_rows)], w1_sem, kind, across_x)

    def staged(src_t):
        return pl.multiple_of(src_t * depth, depth)

    def second(src_t, j):
        return [
            remote(a, b, w2_sem, z * W_CHUNKS + j, at(src_t, y, t))
            for a, b in zip(pieces(stage, staged(src_t), c, j), pieces(w_all, home(z, y), c, j))
        ]

    def second_arrival(from_z, j):
        all_here(w_all.at[pl.ds(0, block_rows // W_CHUNKS)], w2_sem, from_z * W_CHUNKS + j, across_x)

    def third(from_z, j, i):
        ref = pieces(w_all, home(from_z, y), c, j)[i]
        return remote(ref, ref, w3_sem, from_z * 2 + i, across_y)

    def to_share(from_z, own, arrival=False):
        ref = narrow(w_all, home(from_z, y if own else 1 - y), 1 - c if arrival else c)
        return remote(ref, ref, kc_sem, from_z * 2 + own, partner)

    ahead = 1 - 2 * (z // (planes // 2))
    end = (z // (planes // 2)) * (planes - 1)
    ends = jnp.logical_or(z == 0, z == planes - 1)
    middle = jnp.logical_not(ends)

    def out_copies(yy, side=0):
        return [
            weights.at[pl.ds(pl.multiple_of((2 * side + kind) * part + yy * group, group), group)]
            for kind in range(2)
        ]

    end_outs = [
        remote(a, b, o_sem, 2 + i, at(z + ahead, y, t))
        for i, (a, b) in enumerate(zip((out_attn, out_conv), out_copies(y, 1)))
    ]
    small_group = group // END_CHUNKS

    def end_across(i, arrival=False):
        kind, k = i // END_CHUNKS, i % END_CHUNKS
        start = (2 + kind) * part + (1 - y if arrival else y) * group + k * small_group
        ref = weights.at[pl.ds(pl.multiple_of(start, small_group), small_group)]
        return remote(ref, ref, o_sem, 4 + i, across_y)

    outs = [
        remote(a, b, o_sem, i, across_y)
        for i, (a, b) in enumerate(zip((out_attn, out_conv), out_copies(y)))
    ]
    out_loads = [
        pltpu.make_async_copy(a, b, local_sem.at[4 + i])
        for i, (a, b) in enumerate(zip((out_attn, out_conv), out_copies(y)))
    ]

    def own_loads(ref, start):
        return [
            pltpu.make_async_copy(a, b, local_sem.at[i])
            for i, (a, b) in enumerate(zip(w_sources(t)[:3], w_targets(ref, start, c)))
        ]


    for chunk in range(A_CHUNKS):
        for way in range(2):
            @pl.when(can_send(way, 0))
            def _():
                chain(way, 0, chunk).start()

    @pl.when(ends)
    def _():
        for copy in end_outs:
            copy.start()

    small_to = [(partner, tp, 0), (across_x, tx, 1), (diagonal, td, 2)]

    def small_copy(target, tt, i):
        return pltpu.make_async_remote_copy(
            src_ref=small_src.at[tt],
            dst_ref=small,
            send_sem=small_sem[0].at[0],
            recv_sem=small_sem[1].at[0],
            device_id=target,
            device_id_type=MESH,
        )

    @pl.when(t == z)
    def _():
        for args in small_to:
            small_copy(*args).start()
        small[...] = small_src[t]

    for here, ref, start in ((t == z, w_all, home(z, y)), (t != z, stage, staged(t))):
        @pl.when(here)
        def _():
            for copy in own_loads(ref, start):
                copy.start()
            ref[pl.ds(pl.multiple_of(start + c * half, half), half), three : three + width] = w_kv[t]

    first_all(2, partner, tp, lambda copy: copy.start())
    first_all(0, across_x, tx, lambda copy: copy.start())
    first_all(1, diagonal, td, lambda copy: copy.start())
    for copy in outs + out_loads:
        copy.start()
    for here, ref, start in ((t == z, w_all, home(z, y)), (t != z, stage, staged(t))):
        @pl.when(here)
        def _():
            for copy in own_loads(ref, start):
                copy.wait()

    def toward(target, way):
        return target > z if way == 0 else target < z

    def next_to(target, way):
        return target == (z + 1 if way == 0 else z - 1)

    def send_second(way, sources, near):
        for j in range(W_CHUNKS):
            for src_t in sources:
                beside = next_to(src_t, way)
                beyond = jnp.logical_and(toward(src_t, way), jnp.logical_not(beside))

                @pl.when(beside if near else beyond)
                def _():
                    for copy in second(src_t, j):
                        copy.start()

    def chain_step(distance, chunks=range(A_CHUNKS)):
        for chunk in chunks:
            for way in range(2):
                @pl.when(exists(way, distance))
                def _():
                    chain_arrival(way, distance, chunk).wait_recv()

                    @pl.when(can_send(way, distance))
                    def _():
                        chain(way, distance, chunk).start()

                    sideways(way, distance, chunk).start()
                    to_partner(way, distance, chunk, 0).start()

    def sideways_step(distance):
        for chunk in range(A_CHUNKS):
            for way in range(2):
                @pl.when(exists(way, distance))
                def _():
                    sideways(way, distance, chunk, True).wait_recv()
                    to_partner(way, distance, chunk, 1).start()

    def settle(from_z, j):
        for i in (1, 0):
            third(from_z, j, i).start()
        if j == W_CHUNKS - 1:
            to_share(from_z, 1).start()

    def block_step(from_z, j):
        second_arrival(from_z, j)
        settle(from_z, j)

    for k in range(1, planes):
        quarter(k).wait()
        normalise(lax.rem(t + k, planes) * piece, piece)
    first_arrival(2)
    chain_step(1)
    for way in range(2):
        send_second(way, (t, tp), True)

    first_arrival(0)
    first_arrival(1)
    for way in range(2):
        send_second(way, (tx, td), True)
        send_second(way, (t, tp, tx, td), False)


    for j in range(W_CHUNKS):
        settle(z, j)
    for distance in range(2, planes - 1):
        chain_step(distance)

    row = lax.broadcasted_iota(jnp.int32, (block, LANES), 0)
    for zz in range(planes):
        angle = ((2 * zz + y) * block + row).astype(f32) * freq[...]
        here = slice(zz * block, (zz + 1) * block)
        cosine[here, :] = jnp.cos(angle)
        sine[here, :] = jnp.sin(angle)

    @pl.when(middle)
    def _():
        end_outs[0].wait_recv()
        for i in range(END_CHUNKS // 2):
            end_across(i).start()

    blocks_from = [
        z,
        jnp.where(middle, end, z + ahead),
        jnp.where(middle, planes - 1 - z, z + 2 * ahead),
        jnp.where(middle, planes - 1 - end, z + 3 * ahead),
    ]

    def tokens_here(distance):
        for way in range(2):
            @pl.when(exists(way, distance))
            def _():
                all_here(rows_all.at[pl.ds(0, 2 * piece)], ac_sem, way * planes + distance, partner)

    first_row = (z // (planes // 2)) * block
    last_row = (planes - 1) * block - end * block

    def multiply(from_z, yy, fresh):
        cols = pl.ds(home(from_z, yy), depth)

        @pl.loop(0, planes - 1)
        def _(i):
            here = pl.ds(pl.multiple_of(first_row + i * block, block), block)
            value = jnp.dot(rows_all[here, cols], w_all[cols, :], preferred_element_type=f32)
            if fresh:
                acc[here, :] = value
            else:
                acc[here, :] += value

    def multiply_own(pair):
        for k in pair:
            to_share(blocks_from[k], 1, True).wait_recv()
            if k == 0:
                multiply(blocks_from[0], y, True)
        if 0 not in pair:
            multiply(blocks_from[pair[0]], y, False)
        multiply(blocks_from[pair[1]], y, False)

    def share_other(pair):
        for k in pair:
            all_here(narrow(w_all, 0, 0), w3_sem, blocks_from[k] * 2 + 1, across_y)
            to_share(blocks_from[k], 0).start()

    def multiply_other(pair):
        for k in pair:
            all_here(w_all.at[pl.ds(0, depth), pl.ds(0, three)], w3_sem, blocks_from[k] * 2, across_y)
            to_share(blocks_from[k], 0, True).wait_recv()

        @pl.loop(0, 2)
        def _(i):
            multiply(jnp.where(i == 0, blocks_from[pair[0]], blocks_from[pair[1]]), 1 - y, False)

    for j in range(W_CHUNKS):
        block_step(blocks_from[1], j)
    sideways_step(1)
    for j in range(W_CHUNKS):
        block_step(blocks_from[2], j)
        block_step(blocks_from[3], j)
        chain_step(planes - 1, range(j * A_CHUNKS // W_CHUNKS, (j + 1) * A_CHUNKS // W_CHUNKS))
        if j == 1:
            sideways_step(2)
        if j == 2:
            share_other((0, 1))
            for distance in range(1, planes - 1):
                tokens_here(distance)
            multiply_own((0, 1))
            multiply_other((0, 1))
    @pl.when(middle)
    def _():
        end_outs[1].wait_recv()
        for i in range(END_CHUNKS // 2, END_CHUNKS):
            end_across(i).start()

    multiply_own((2, 3))
    share_other((2, 3))
    sideways_step(planes - 1)
    multiply_other((2, 3))

    tokens_here(planes - 1)
    here = pl.ds(pl.multiple_of(last_row, block), block)

    @pl.loop(0, 2)
    def _(i):
        cols = pl.ds(pl.multiple_of(i * 2 * width, 2 * width), 2 * width)
        acc[here, cols] = jnp.dot(rows_all[here, :], w_all[:, cols], preferred_element_type=f32)

    lane = lax.broadcasted_iota(jnp.int32, (block, LANES), 1)
    low = lax.rem(lane, HEAD) < HEAD // 2

    def turned(value, here):
        other = jnp.where(low, -pltpu.roll(value, LANES - HEAD // 2, 1), pltpu.roll(value, HEAD // 2, 1))
        return value * cosine[here, :] + other * sine[here, :]

    def halo(kind, zz):
        if kind == 0:
            ref = kv_b.at[pl.ds((zz + 1) * block - WINDOW, WINDOW)]
            return remote(ref, kv_rim.at[zz + y], halo_sem, zz, across_y)
        ref = gated.at[pl.ds((zz + 1) * block - 32, 32)]
        return remote(ref, gated_rim.at[zz + y], halo_sem, planes + zz, across_y)

    def halo_arrival(kind, zz):
        ref = (kv_rim if kind == 0 else gated_rim).at[zz + 1 - y]
        return remote(ref, ref, halo_sem, kind * planes + zz, across_y)

    for zz in range(planes):
        here = slice(zz * block, (zz + 1) * block)
        value = acc[here, three:]
        kv_b[here, :] = jnp.where(lane < HEAD, turned(value, here), value).astype(kv_b.dtype)
        halo(0, zz).start()
    for zz in range(planes):
        here = slice(zz * block, (zz + 1) * block)
        gate = acc[here, 2 * width : three]
        value = (acc[here, width : 2 * width] * (1.0 / (1.0 + jnp.exp(-gate)))).astype(gated.dtype)
        gated[here, :] = value
        extended[zz, 32:, :] = value.astype(f32)
        halo(1, zz).start()

    @pl.when(y == 0)
    def _():
        kv_rim[0] = jnp.zeros_like(kv_rim[0])
        gated_rim[0] = jnp.zeros_like(gated_rim[0])

    for zz in range(planes):
        here = slice(zz * block, (zz + 1) * block)
        q_b[here, :] = (turned(acc[here, :width], here) * (1.0 / math.sqrt(HEAD))).astype(q_b.dtype)

    @pl.when(t != z)
    def _():
        small_copy(partner, tp, 0).wait_recv()

    @pl.when(middle)
    def _():
        for i in range(END_CHUNKS, 2 * END_CHUNKS):
            end_across(i).start()

    lane_q = lax.broadcasted_iota(jnp.int32, (WINDOW, LANES), 1)
    lane_k = lax.broadcasted_iota(jnp.int32, (2 * WINDOW, LANES), 1)
    row_s = lax.rem(lax.broadcasted_iota(jnp.int32, (heads * WINDOW, 2 * WINDOW), 0), WINDOW)
    col_s = lax.broadcasted_iota(jnp.int32, (heads * WINDOW, 2 * WINDOW), 1)
    distance_s = row_s + WINDOW - col_s
    inside = jnp.logical_and(distance_s >= 0, distance_s < WINDOW)
    sink_row = small[33:34, :]
    lane_1 = lax.broadcasted_iota(jnp.int32, (1, LANES), 1)
    sinks = [
        jnp.sum(jnp.where(lane_1 == t * heads + h, sink_row, 0.0), axis=1, keepdims=True)
        for h in range(heads)
    ]
    sink_col = jnp.concatenate([jnp.broadcast_to(v, (WINDOW, 1)) for v in sinks], axis=0)

    def attend(first_row, keys, mask):
        query = q_b[pl.ds(first_row, WINDOW), :]
        keys_f = keys.astype(f32)
        swapped = pltpu.roll(keys_f, HEAD, 1)
        key_two = jnp.where(lane_k < HEAD, keys_f, swapped).astype(jnp.bfloat16)
        value_two = jnp.where(lane_k < HEAD, swapped, keys_f).astype(jnp.bfloat16)
        zero = jnp.zeros_like(query)
        stacked = jnp.concatenate(
            [jnp.where(lane_q // HEAD == h, query, zero) for h in range(heads)], axis=0
        )
        scores = lax.dot_general(
            stacked, key_two, (((1,), (1,)), ((), ())), preferred_element_type=f32
        )
        scores = jnp.where(mask, scores, -1e30)
        top = jnp.maximum(jnp.max(scores, axis=1, keepdims=True), sink_col)
        grown = jnp.exp(scores - top)
        total = jnp.sum(grown, axis=1, keepdims=True) + jnp.exp(sink_col - top)
        probs = (grown / total).astype(jnp.bfloat16)
        mixed_values = jnp.dot(probs, value_two, preferred_element_type=f32)
        result = mixed_values[:WINDOW]
        for h in range(1, heads):
            result = jnp.where(lane_q // HEAD == h, mixed_values[h * WINDOW : (h + 1) * WINDOW], result)
        act[pl.ds(first_row, WINDOW), columns(0, t)] = result.astype(act.dtype)

    def columns(kind, tt, side=0):
        return pl.ds(pl.multiple_of((2 * side + kind) * part + tt * width, width), width)

    blocks = block // WINDOW

    for zz in range(planes):
        for b in range(1, blocks):
            start = zz * block + b * WINDOW
            attend(start, kv_b[pl.ds(start - WINDOW, 2 * WINDOW), :], inside)

    def attend_first(zz):
        start = pl.multiple_of(zz * block, block)
        keys = jnp.concatenate([kv_rim[zz], kv_b[pl.ds(start, WINDOW), :]], axis=0)
        began = jnp.logical_or(zz * 2 + y > 0, col_s >= WINDOW)
        attend(start, keys, jnp.logical_and(inside, began))

    for zz in range(planes):
        if zz < planes - 1:
            halo_arrival(1, zz).wait_recv()

        @pl.when(y == 1)
        def _():
            if zz == planes - 1:
                halo_arrival(1, zz).wait_recv()

    for zz in range(planes):
        extended[zz, 0:32, :] = gated_rim[zz].astype(f32)
    strip = 64

    @pl.loop(0, planes)
    def _(zz):
        @pl.loop(0, block // strip)
        def _(i):
            base = pl.multiple_of(i * strip, strip)
            window = extended[zz, pl.ds(base, strip + 32), :]
            total = jnp.zeros((strip, width), f32)
            for shift in range(8):
                moved = extended[zz, pl.ds(base + shift, strip + 24), :] if shift else window
                for k in range((shift - 2) % 8, KSIZE, 8):
                    low = 2 + k - shift
                    total = total + moved[low : low + strip] * small[k : k + 1, :]
            filtered[pl.ds(pl.multiple_of(zz * block + base, strip), strip), :] = total

    tiles = rows // LANES
    for k in range(tiles):
        value = filtered[k * LANES : (k + 1) * LANES, :]
        total = jnp.sum(value, axis=1, keepdims=True)
        square = jnp.sum(value * value, axis=1, keepdims=True)
        stats[k : k + 1, :] = jnp.transpose(jnp.broadcast_to(total, (LANES, LANES)))[0:1]
        stats[tiles + k : tiles + k + 1, :] = jnp.transpose(jnp.broadcast_to(square, (LANES, LANES)))[0:1]

    def stat(k):
        g = peers[k]
        return pltpu.make_async_remote_copy(
            src_ref=stats,
            dst_ref=stats_all.at[mine],
            send_sem=s_sem[0].at[0],
            recv_sem=s_sem[1].at[0],
            device_id=at(g // planes, y, g % planes),
            device_id_type=MESH,
        )

    for k in range(size - 1):
        stat(k).start()
    stats_all[mine] = stats[...]

    for zz in range(planes):
        if zz < planes - 1:
            halo_arrival(0, zz).wait_recv()

        @pl.when(y == 1)
        def _():
            if zz == planes - 1:
                halo_arrival(0, zz).wait_recv()

    def region(kind, r, tt, side):
        start = pl.multiple_of(r * block, block)
        return act.at[pl.ds(start, block), columns(kind, tt, side)]

    def cross(kind, r, side, arrival=False):
        ref = region(kind, r, tx if arrival else t, side)
        return remote(ref, ref, x_sem, (side * 2 + kind) * planes + r, across_x)

    def hand(kind, r, side, far):
        ref = region(kind, r, tx if far else t, side)
        return remote(ref, ref, c_sem, side * planes + r, partner)

    def send_out(kind, r, side=0):
        cross(kind, r, side).start()
        hand(kind, r, side, 0).start()

    near = z // (planes // 2)
    order = [(1 - near) * (planes - 1 - j) + near * j for j in range(planes)]

    def inward(kind, j):
        source = region(kind, order[j], t, 0)
        return remote(source, region(kind, order[j], t, 1), e_sem, kind * planes + j, at(z + ahead, y, t))

    def pass_in(kind, j):
        inward(kind, j).wait_recv()
        send_out(kind, order[j], 1)

    for pair in ((0, 1), (2, 3)):
        for j in pair:
            attend_first(order[j])

        @pl.when(ends)
        def _():
            for j in pair:
                if j < planes - 1:
                    inward(0, j).start()

        @pl.when(middle)
        def _():
            for j in pair:
                if j < 2:
                    send_out(0, order[j])

    @pl.when(middle)
    def _():
        pass_in(0, 0)

    all_here(stats_all.at[pl.ds(0, size - 1)], s_sem, 0, partner)
    total = stats_all[0]
    for g in range(1, size):
        total = total + stats_all[g]
    mean = total[:tiles] / channels
    variance = total[tiles:] / channels - mean * mean
    moments[0] = mean
    moments[1] = lax.rsqrt(variance + 1e-05)
    per = block // LANES

    def normed_out(r):
        for k in range(per):
            tile = r * per + k
            mean_col = jnp.transpose(jnp.broadcast_to(moments[0, pl.ds(tile, 1), :], (LANES, LANES)))
            rate_col = jnp.transpose(jnp.broadcast_to(moments[1, pl.ds(tile, 1), :], (LANES, LANES)))
            here = pl.ds(pl.multiple_of(tile * LANES, LANES), LANES)
            scaled = (filtered[here, :] - mean_col) * rate_col * small[32:33, :]
            act[here, columns(1, t)] = (scaled / (1.0 + jnp.exp(-scaled))).astype(act.dtype)

    out_step = mixed.shape[1] // OUT_CHUNKS

    def gathered(j, sides):
        for side in sides:
            for kind in range(2):
                cross(kind, order[j], side, True).wait_recv()
                hand(kind, order[j], side, 1).start()
        for side in sides:
            ref = act.at[pl.ds(0, block), pl.ds(0, 4 * width)]
            all_here(ref, c_sem, side * planes + order[j], partner)

    def out_columns(h):
        return pl.ds(pl.multiple_of(h * out_step, out_step), out_step)

    def travel(slot, h, toward_z):
        return remote(
            outgoing.at[slot, :, out_columns(h)],
            incoming.at[slot, :, out_columns(h)],
            r_sem,
            slot * OUT_CHUNKS + h,
            at(toward_z, y, t),
        )

    def outputs(j, h, deep):
        start = pl.multiple_of(order[j] * block, block)
        deep_rows = slice(0, (4 if deep else 2) * part)
        return jnp.dot(
            act[pl.ds(start, block), deep_rows], weights[deep_rows, out_columns(h)], preferred_element_type=f32
        )

    def send_sums(j, deep, came, slot, toward_z):
        @pl.loop(0, OUT_CHUNKS)
        def _(h):
            value = outputs(j, h, deep)
            if came is not None:
                travel(came, h, across_z).wait_recv()
                value = value + incoming[came, :, out_columns(h)].astype(f32)
            outgoing[slot, :, out_columns(h)] = value.astype(outgoing.dtype)
            travel(slot, h, toward_z).start()

    def finish(j, deep, came):
        @pl.loop(0, OUT_CHUNKS)
        def _(h):
            value = outputs(j, h, deep)
            travel(came, h, across_z).wait_recv()
            mixed[:, out_columns(h)] = value + incoming[came, :, out_columns(h)].astype(f32)

    across_z = z + ahead

    for j, r in enumerate(order):
        normed_out(r)

        @pl.when(ends)
        def _():
            if j < planes - 1:
                inward(1, j).start()
            else:
                send_out(0, r)
                send_out(1, r)

        if j == 0:
            @pl.when(middle)
            def _():
                send_out(1, r)

    for copy in out_loads:
        copy.wait()
    for copy in outs:
        copy.wait_recv()

    @pl.when(middle)
    def _():
        for i in range(2 * END_CHUNKS):
            end_across(i, True).wait_recv()

    @pl.when(middle)
    def _():
        pass_in(1, 0)
        send_out(1, order[1])
        pass_in(0, 1)
        gathered(0, (0, 1))
        send_sums(0, True, None, 0, across_z)

    @pl.when(middle)
    def _():
        pass_in(1, 1)
        for kind in range(2):
            send_out(kind, order[3])
        gathered(1, (0, 1))
        send_sums(1, True, None, 1, across_z)

    @pl.when(middle)
    def _():
        for kind in range(2):
            send_out(kind, order[2])
            pass_in(kind, 2)
        gathered(3, (0,))
        send_sums(3, False, 0, 2, z - ahead)

    @pl.when(middle)
    def _():
        gathered(2, (0, 1))
        finish(2, True, 1)

    @pl.when(ends)
    def _():
        gathered(3, (0,))
        finish(3, False, 2)

    @pl.when(t == z)
    def _():
        all_sent(small_src.at[pl.ds(0, 3)], small_sem, partner)

    @pl.when(y == 0)
    def _():
        for kind in range(2):
            halo_arrival(kind, planes - 1).wait_recv()

    all_sent(kv_b.at[pl.ds(0, planes * (WINDOW + 32))], halo_sem, across_y)
    all_sent(w_all.at[pl.ds(0, 3 * block_rows)], w1_sem, partner)
    all_sent(w_all.at[pl.ds(0, 3 * block_rows)], w2_sem, partner)
    all_sent(w_all.at[pl.ds(0, planes * block_rows)], w3_sem, across_y)
    all_sent(w_all.at[pl.ds(0, 2 * planes * half), pl.ds(0, width)], kc_sem, partner)
    all_sent(rows_all.at[pl.ds(0, (planes - 1) * piece)], ax_sem, across_x)
    all_sent(rows_all.at[pl.ds(0, 2 * (planes - 1) * piece)], ac_sem, partner)
    all_sent(stats_all.at[pl.ds(0, size - 1)], s_sem, partner)

    def sent_regions(count, sems):
        all_sent(act.at[pl.ds(0, 2 * block), pl.ds(0, count * width // 2)], sems, partner)

    @pl.when(ends)
    def _():
        all_sent(rows_all.at[pl.ds(0, piece)], a_sem, partner)
        sent_regions(2 * (planes - 1), e_sem)
        sent_regions(2, x_sem)
        sent_regions(4, c_sem)
        all_sent(weights.at[pl.ds(0, 4 * group)], o_sem, partner)

    @pl.when(middle)
    def _():
        all_sent(rows_all.at[pl.ds(0, (planes + 1) * piece)], a_sem, partner)
        sent_regions(2 * planes + 2 * (planes - 1), x_sem)
        sent_regions(4 * planes + 4 * (planes - 1), c_sem)
        all_sent(weights.at[pl.ds(0, 4 * group)], o_sem, partner)
        all_sent(outgoing, r_sem, partner)


def planned_per_device(
    tokens,
    norm_gain,
    w_query,
    w_key,
    w_value,
    w_glu,
    w_gate,
    sink_logit,
    conv_taps,
    conv_gain,
    out_attn,
    out_conv,
):
    planes = lax.axis_size("tp")
    block, model = tokens.shape
    rows = planes * block
    depth, cols = w_query.shape
    width = cols // planes
    columns_out = out_attn.shape[1]
    size = planes * planes
    half_width = HEAD // 2
    freq = 10000.0 ** (-np.arange(half_width, dtype=np.float64) * 2.0 / HEAD)
    freq = jnp.asarray(np.tile(freq, LANES // half_width)[None], dtype=jnp.float32)
    vmem = pl.BlockSpec(memory_space=pltpu.VMEM)
    any_spec = pl.BlockSpec(memory_space=pl.ANY)
    dma = pltpu.SemaphoreType.DMA
    bf16, f32 = jnp.bfloat16, jnp.float32
    tiles = rows // LANES
    chunks = 2 * planes * A_CHUNKS
    counts = [
        chunks, chunks, 2 * planes, 3, planes * W_CHUNKS, 2 * planes, 2 * planes, 4 + 2 * END_CHUNKS, 1,
        2 * planes, 1, 2 * planes, 4 * planes, 2 * planes, 3 * OUT_CHUNKS,
    ]
    sems = [dma((n,)) for count in counts for n in (1, count)]
    return pl.pallas_call(
        functools.partial(layer_kernel, planes, CONV),
        out_shape=pltpu.VMEM((block, columns_out), f32),
        in_specs=[any_spec] + [vmem] * 7 + [any_spec] * 5,
        out_specs=vmem,
        scratch_shapes=[
            pltpu.VMEM((rows, model), bf16),
            pltpu.VMEM((2 * planes * depth, 4 * width), bf16),
            pltpu.VMEM((planes * depth, 4 * width), bf16),
            pltpu.VMEM((planes, depth // 2, 2 * HEAD), bf16),
            pltpu.VMEM((planes, 40, width), f32),
            pltpu.VMEM((40, width), f32),
            pltpu.VMEM((rows, 4 * width), f32),
            pltpu.VMEM((rows, LANES), f32),
            pltpu.VMEM((rows, LANES), f32),
            pltpu.VMEM((rows, width), bf16),
            pltpu.VMEM((rows, width), bf16),
            pltpu.VMEM((planes + 1, WINDOW, width), bf16),
            pltpu.VMEM((rows, width), bf16),
            pltpu.VMEM((planes + 1, 32, width), bf16),
            pltpu.VMEM((planes, 32 + block, width), f32),
            pltpu.VMEM((rows, width), f32),
            pltpu.VMEM((rows, 4 * planes * width), bf16),
            pltpu.VMEM((4 * planes * width, columns_out), bf16),
            pltpu.VMEM((2 * tiles, LANES), f32),
            pltpu.VMEM((size, 2 * tiles, LANES), f32),
            pltpu.VMEM((2, tiles, LANES), f32),
            pltpu.VMEM((3, block, columns_out), bf16),
            pltpu.VMEM((3, block, columns_out), bf16),
            pltpu.VMEM((block, model), bf16),
            dma((6 + planes,)),
        ]
        + sems,
        compiler_params=pltpu.CompilerParams(
            collective_id=0, has_side_effects=True, vmem_limit_bytes=58 * 2**20
        ),
    )(
        tokens,
        norm_gain[None],
        freq,
        w_key,
        w_value,
        conv_taps,
        conv_gain[None],
        sink_logit[None],
        w_query,
        w_glu,
        w_gate,
        out_attn,
        out_conv,
    ).astype(bf16)


def solution(mesh):
    planes, others = mesh.shape["tp"], mesh.shape["sp"]
    fits = others == 2 * planes and planes == 4 and HEADS == 2 * planes * planes
    return jax.shard_map(
        planned_per_device if fits else gathered_per_device,
        mesh=mesh,
        in_specs=(
            P("sp", None),
            P(),
            P("sp", "tp"),
            P("sp", "tp"),
            P("sp", "tp"),
            P("sp", "tp"),
            P("sp", "tp"),
            P("tp"),
            P(None, "tp"),
            P("tp"),
            P("sp", "tp"),
            P("sp", "tp"),
        ),
        out_specs=P("sp", "tp"),
        check_vma=False,
    )
```
